256 devices in a mesh: sp: 64 (over z, y, core), tp: 4 (over x).
Axes of the slice: x: 4, y: 4, z: 8, core: 2. Of those that a mesh axis runs over, the one named last changes fastest.
Arguments:
- queries: bfloat16 [32768, 1024], P('sp', 'tp'), may hold values from -6 to 6
- keys: bfloat16 [32768, 1024], P('sp', 'tp'), may hold values from -6 to 6
- values: bfloat16 [32768, 1024], P('sp', 'tp'), may hold values from -6 to 6
- output_gate_logits: bfloat16 [32768, 1024], P('sp', 'tp'), may hold values from -6 to 6
- input_gate_log: float32 [32768, 8], P('sp', 'tp'), may hold values from -5 to 125
- forget_gate_logits: float32 [32768, 8], P('sp', 'tp')
- extra_decay_log: float32 [32768, 8], P('sp', 'tp'), may hold values from -1 to 0
- document: int32 [32768], P('sp'), may hold values from 0 to 31, never falling along the last dimension, each value on 1 to 2048 neighbouring positions
- residual: bfloat16 [32768, 2048], P('sp', 'tp'), may hold values from -16 to 16
- cell_norm_gain: bfloat16 [1024], P('tp'), may hold values from 0.099609375 to 1.8984375
- output_weight: bfloat16 [1024, 2048], P('tp'), may hold values from -0.1875 to 0.1875
- mixer_norm_gain: bfloat16 [2048], P('tp'), may hold values from 0.099609375 to 1.8984375
- up_weight: bfloat16 [2048, 8192], P('sp', 'tp'), may hold values from -0.125 to 0.125
- down_weight: bfloat16 [8192, 2048], P('tp', 'sp'), may hold values from -0.0625 to 0.0625
Outputs:
- layer_out: bfloat16 [32768, 2048], P('sp', 'tp')
The draws below stay inside these ranges and needn't reach their ends.
All inputs are finite; a program needn't handle non-finite values.
Results may differ from the reference program's by a relative error of at most 0.015.
Values may be sent and summed in bfloat16 or wider, within the bound.
A program may use at most 128 MiB of HBM per device.

```python
import math
import jax
import jax.numpy as jnp
import numpy as np
from jax import lax

D = 2048
FF = 8192
HM = 8
DH = 128
BLOCK = 128
TOK_DEV = 512
TOKENS = 32768
DOCS = 32
MOST = 2048
N_SP = 64
N_TP = 4


def draw_input_gate_log(key, part):
    key_base = jax.random.fold_in(key, 0)
    return jnp.clip(jax.random.normal(key_base, (TOKENS, HM), jnp.float32), -4.0, 4.0)


def draw_forget_gate_logits(key, part):
    key_kind, key_device, key_noise = jax.random.split(key, 3)
    fast_heads = jax.random.randint(key_kind, (HM,), 0, 2) == 1
    device_rate = jax.random.uniform(key_device, (TOKENS // TOK_DEV, 1, 1), jnp.float32, 0.0, math.log(4.0))
    jitter = jax.random.uniform(key_noise, (TOKENS // TOK_DEV, TOK_DEV, HM), jnp.float32, -0.7, 0.7)
    slow_pre = math.log(8.0 * MOST) - device_rate + jitter
    fast_pre = math.log(40.0) + jitter
    result = jnp.where(fast_heads[None, None, :], fast_pre, slow_pre)
    return result.reshape(TOKENS, HM)


def draw_extra_decay_log(key, part):
    key_spot, key_head, key_depth = jax.random.split(key, 3)
    places = max(TOKENS // TOK_DEV * 2, 4)
    spots = jax.random.randint(key_spot, (places,), 0, TOKENS)
    heads_hit = jax.random.randint(key_head, (places,), 0, HM)
    depths = jax.random.uniform(key_depth, (places,), jnp.float32, math.log(0.5), math.log(0.8))
    return jnp.zeros((TOKENS, HM), jnp.float32).at[spots, heads_hit].min(depths)


def draw_residual(key, part):
    key_values = jax.random.fold_in(key, 0)
    ramp = jnp.exp(jnp.linspace(0.0, math.log(3.0), D)).astype(jnp.float32)
    entries = jnp.clip(jax.random.normal(key_values, (TOKENS, D), jnp.float32), -4.0, 4.0)
    return (entries * ramp[None, :] / 1.7).astype(jnp.bfloat16)


def shard_levels(rng, dims, cuts, smallest, high):
    loudness = 1.0
    for axis_at, parts in cuts:
        draws = jax.random.uniform(jax.random.fold_in(jax.random.fold_in(rng, 6), axis_at), (parts,), jnp.float32, smallest / len(cuts), high / len(cuts))
        loudness = loudness * jnp.repeat(jnp.exp(draws), dims[axis_at] // parts).reshape((-1,) + (1,) * (len(dims) - 1 - axis_at))
    return loudness


def split_up(amount, total, most, slope):
    portions = [(1 << 20) // math.isqrt(grade ** slope) + 1 for grade in range(2, amount + 1)]
    surplus, counts = total - most - (amount - 1), [1] * (amount - 1)
    while surplus > 0:
        free = [i for i in range(amount - 1) if counts[i] < most]
        mass, budget = sum([portions[i] for i in free]), surplus
        for i in free:
            more = min(most - counts[i], max(1, budget * portions[i] // mass), surplus)
            counts[i] = counts[i] + more
            surplus = surplus - more
    return np.array([most] + counts)


def ragged_sizes(stream_key, count, total, limit, lean):
    if count == 2:
        one = jax.random.randint(stream_key, (), max(1, total - limit), min(limit, total - 1) + 1)
        return jnp.stack([one, total - one])
    lengths = jnp.asarray(split_up(count, total, limit, lean), jnp.int32)
    couples = (count - 1) // 2
    source_of, receiver = lengths[1:1 + 2 * couples:2], lengths[2:2 + 2 * couples:2]
    slack = jnp.minimum(source_of - 1, limit - receiver)
    passed = jax.random.randint(jax.random.fold_in(stream_key, 1), (couples,), 0, 1 << 20) % (slack + 1)
    lengths = lengths.at[1:1 + 2 * couples:2].set(source_of - passed).at[2:2 + 2 * couples:2].set(receiver + passed)
    return lengths[jax.random.permutation(jax.random.fold_in(stream_key, 2), count)]


def gaussian(key, extent, scale, bound, cuts=(), dtype=jnp.bfloat16):
    values = jax.random.normal(key, extent, jnp.float32) * scale
    if len(cuts) > 0:
        values = shard_levels(key, extent, cuts, -0.22, 0.18) * values
    return jnp.clip(values, min=-bound, max=bound).astype(dtype)


def setup_inputs(seed: int = 0) -> dict:
    streams_of = jax.random.split(jax.random.key(seed), 15)
    queries = gaussian(streams_of[0], (TOKENS, HM * DH), 1.0, 6.0, ((0, 64), (1, 4)))
    keys = gaussian(streams_of[1], (TOKENS, HM * DH), 1.0, 6.0, ((0, 64), (1, 4)))
    values = gaussian(streams_of[2], (TOKENS, HM * DH), 1.0, 6.0, ((0, 64), (1, 4)))
    output_gate_logits = gaussian(streams_of[3], (TOKENS, HM * DH), 1.0, 6.0, ((0, 64), (1, 4)))
    input_gate_log = draw_input_gate_log(jax.random.fold_in(streams_of[14], 71), 0)
    forget_gate_logits = draw_forget_gate_logits(jax.random.fold_in(streams_of[14], 71), 0)
    extra_decay_log = draw_extra_decay_log(jax.random.fold_in(streams_of[14], 71), 0)
    document = jnp.searchsorted(jnp.cumsum(ragged_sizes(streams_of[7], DOCS, TOKENS, MOST, 0)), jnp.arange(TOKENS), side="right").astype(jnp.int32)
    residual = draw_residual(jax.random.fold_in(streams_of[14], 71), 0)
    cell_norm_gain = jnp.clip(1.0 + 0.18 * jax.random.normal(streams_of[9], (HM * DH,), jnp.float32), 0.099609375, 1.8984375).astype(jnp.bfloat16)
    output_weight = gaussian(streams_of[10], (HM * DH, D), (HM * DH) ** -0.5, 0.1875, ((0, 4),))
    mixer_norm_gain = jnp.clip(1.0 + 0.18 * jax.random.normal(streams_of[11], (D,), jnp.float32), 0.099609375, 1.8984375).astype(jnp.bfloat16)
    up_weight = gaussian(streams_of[12], (D, FF), D ** -0.5, 0.125, ((0, 64), (1, 4)))
    down_weight = gaussian(streams_of[13], (FF, D), FF ** -0.5, 0.0625, ((0, 4), (1, 64)))
    return dict(queries=queries, keys=keys, values=values, output_gate_logits=output_gate_logits, input_gate_log=input_gate_log, forget_gate_logits=forget_gate_logits, extra_decay_log=extra_decay_log, document=document, residual=residual, cell_norm_gain=cell_norm_gain, output_weight=output_weight, mixer_norm_gain=mixer_norm_gain, up_weight=up_weight, down_weight=down_weight)


NEG = -1e+30
EPS = 1e-06
HIGH = lax.Precision.HIGHEST

def block_terms(carry, inputs):
    memory, normer, stabil, last_doc = carry
    q_blk, k_blk, v_blk, gate_in, gate_log, doc_blk = inputs
    length = doc_blk.shape[0]
    causal = jnp.arange(length)[:, None] >= jnp.arange(length)[None, :]
    cumulative = jnp.cumsum(gate_log, axis=-1)
    same_doc = (doc_blk[:, None] == doc_blk[None, :]) & causal
    pair_log = cumulative[:, :, None] - cumulative[:, None, :] + gate_in[:, None, :]
    pair_log = jnp.where(same_doc[None], pair_log, NEG)
    live_rows = doc_blk == last_doc
    carried_log = jnp.where(live_rows[None, :], cumulative + stabil[:, None], NEG)
    peak_log = jnp.maximum(carried_log, lax.optimization_barrier(jnp.max(pair_log, axis=-1)))
    weights = jnp.exp(pair_log - peak_log[:, :, None])
    carried = jnp.exp(carried_log - peak_log)
    scores = jnp.einsum('htd,hsd->hts', q_blk, k_blk, precision=HIGH) * weights
    numerator = carried[:, :, None] * jnp.einsum('htd,hde->hte', q_blk, memory, precision=HIGH)
    numerator = numerator + jnp.einsum('hts,hse->hte', scores, v_blk, precision=HIGH)
    denominator = carried * jnp.einsum('htd,hd->ht', q_blk, normer, precision=HIGH) + lax.optimization_barrier(jnp.sum(scores, axis=-1))
    end_doc = doc_blk[-1]
    end_cum = cumulative[:, -1]
    keep_log = jnp.where((doc_blk == end_doc)[None, :], end_cum[:, None] - cumulative + gate_in, NEG)
    old_log = jnp.where(last_doc == end_doc, end_cum + stabil, NEG)
    new_stab = jnp.maximum(old_log, lax.optimization_barrier(jnp.max(keep_log, axis=-1)))
    scaled = jnp.exp(keep_log - new_stab[:, None])
    decayed = jnp.exp(old_log - new_stab)
    memory = decayed[:, None, None] * memory + jnp.einsum('hs,hsd,hse->hde', scaled, k_blk, v_blk, precision=HIGH)
    normer = decayed[:, None] * normer + jnp.einsum('hs,hsd->hd', scaled, k_blk, precision=HIGH)
    return ((memory, normer, new_stab, end_doc), (numerator, denominator, peak_log, cumulative))

def split_heads(source, blocks):
    return source.astype(jnp.float32).reshape(blocks, BLOCK, -1, DH).transpose(0, 2, 1, 3)

def split_gates(source, blocks):
    return source.reshape(blocks, BLOCK, -1).transpose(0, 2, 1)

def within_block_pass(queries, keys, values, input_gate_log, forget_gate_logits, extra_decay_log, document):
    blocks = queries.shape[0] // BLOCK
    head_count = queries.shape[1] // DH
    query_heads = split_heads(queries, blocks) * DH ** (-0.5)
    forget_log_values = jax.nn.log_sigmoid(forget_gate_logits) + extra_decay_log
    inputs = (query_heads, split_heads(keys, blocks), split_heads(values, blocks), split_gates(input_gate_log, blocks), split_gates(forget_log_values, blocks), document.reshape(blocks, BLOCK))
    initial = (jnp.zeros((head_count, DH, DH), jnp.float32), jnp.zeros((head_count, DH), jnp.float32), jnp.full((head_count,), NEG, jnp.float32), jnp.array(-1, jnp.int32))
    final_state, output_rows = lax.scan(block_terms, initial, inputs)
    return (query_heads, final_state, output_rows)

def head_mix(cell_out, output_gate_logits, cell_norm_gain):
    row_count = output_gate_logits.shape[0]
    head_count = cell_out.shape[1]
    hidden = cell_out.transpose(0, 2, 1, 3).reshape(row_count, head_count * DH)
    inverse = lax.rsqrt(lax.optimization_barrier(jnp.mean(hidden * hidden, axis=1, keepdims=True)) + EPS)
    gated = jax.nn.sigmoid(output_gate_logits.astype(jnp.float32))
    gains = cell_norm_gain.astype(jnp.float32)
    return (gated * hidden * inverse * gains[None, :]).astype(jnp.bfloat16)

def reference(queries, keys, values, output_gate_logits, input_gate_log, forget_gate_logits, extra_decay_log, document, residual, cell_norm_gain, output_weight, mixer_norm_gain, up_weight, down_weight):
    query_heads, final_state, output_rows = within_block_pass(queries, keys, values, input_gate_log, forget_gate_logits, extra_decay_log, document)
    numerator, denominator, peak_log, cumulative = output_rows
    cell_out = numerator / jnp.maximum(jnp.abs(denominator), 1.0)[..., None]
    mixed = head_mix(cell_out, output_gate_logits, cell_norm_gain)
    out_groups = output_weight.reshape(N_TP, -1, D).astype(jnp.float32)
    down_groups = down_weight.reshape(N_TP, -1, D).astype(jnp.float32)
    gain_wide = mixer_norm_gain.astype(jnp.float32)

    def rows_step(row_args):
        mixed_rows, resid_rows = row_args
        row_count = mixed_rows.shape[0]
        group_parts = jnp.einsum('rgk,gkd->grd', mixed_rows.reshape(row_count, N_TP, -1).astype(jnp.float32), out_groups)
        group_parts = lax.optimization_barrier(group_parts.astype(jnp.bfloat16)).astype(jnp.float32)
        first_sum = (resid_rows.astype(jnp.float32) + lax.optimization_barrier(jnp.sum(group_parts, axis=0))).astype(jnp.bfloat16)
        first_wide = lax.optimization_barrier(first_sum).astype(jnp.float32)
        inverse = lax.rsqrt(lax.optimization_barrier(jnp.mean(first_wide * first_wide, axis=1, keepdims=True)) + EPS)
        normed = (first_wide * inverse * gain_wide).astype(jnp.bfloat16)
        hidden = jnp.dot(normed, up_weight, preferred_element_type=jnp.float32)
        squared = jnp.square(jax.nn.relu(hidden)).astype(jnp.bfloat16)
        channel_parts = jnp.einsum('rgf,gfd->grd', squared.reshape(row_count, N_TP, -1).astype(jnp.float32), down_groups)
        channel_parts = lax.optimization_barrier(channel_parts.astype(jnp.bfloat16)).astype(jnp.float32)
        return (first_wide + lax.optimization_barrier(jnp.sum(channel_parts, axis=0))).astype(jnp.bfloat16)
    layer = lax.map(rows_step, (mixed.reshape(N_SP, -1, mixed.shape[1]), residual.reshape(N_SP, -1, D)))
    return layer.reshape(-1, D)
```

```python
import jax
import jax.numpy as jnp
from jax import lax
from jax.experimental import pallas as pl
from jax.experimental.pallas import tpu as pltpu
from jax.sharding import Mesh
from jax.sharding import PartitionSpec as P

MESH = pl.DeviceIdType.MESH
SP = ("z", "y", "c")
NZ, NY, NC, NX = 8, 4, 2, 4
ROWS, DH, BLK = 512, 128, 128
HW = 256
DM = 2048
OWN = 512
NB = ROWS // BLK
BACK = 4
NEG = -1e30
EPS = 1e-6
F32, BF16 = jnp.float32, jnp.bfloat16


def rcopy(src, dst, sems, i, dev):
    return pltpu.make_async_remote_copy(
        src_ref=src, dst_ref=dst, send_sem=sems[0].at[i], recv_sem=sems[1].at[i],
        device_id=dev, device_id_type=MESH,
    )


def across(row):
    return jnp.transpose(jnp.broadcast_to(row, (BLK, BLK)))


def rows_of(values):
    return lax.dot_general(
        jnp.ones((8, BLK), F32), values, (((1,), (1,)), ((), ())),
        precision=lax.Precision.HIGHEST, preferred_element_type=F32,
    )


class Gather:
    def __init__(self, view, sems, base, x):
        self.view, self.sems, self.base, self.x = view, sems, base, x
        self.right, self.left = lax.rem(x + 1, NX), lax.rem(x + NX - 1, NX)

    def start(self):
        own = self.view(self.x, None)
        self.r = rcopy(own, own, self.sems, self.base, {"x": self.right})
        self.l = rcopy(own, own, self.sems, self.base + 1, {"x": self.left})
        self.r.start()
        self.l.start()

    def forward(self):
        self.r.wait_recv()
        a = self.view(self.left, 0)
        self.fr = rcopy(a, a, self.sems, self.base + 2, {"x": self.right})
        self.fr.start()
        self.l.wait_recv()
        b = self.view(self.right, 1)
        self.fl = rcopy(b, b, self.sems, self.base + 3, {"x": self.left})
        self.fl.start()

    def finish(self):
        self.fr.wait_recv()
        self.fl.wait_recv()
        for d in (self.r, self.l, self.fr, self.fl):
            d.wait_send()


def kernel(
    small_h, q_h, k_h, v_h, og_h, res_h, wout_h,
    normed, first_own,
    small, q, k, v, og, res, wc, nd, top, stout, auxout, stin, auxin,
    u, line1, line1in, full, line2, line2in,
    lsem, wss, wrs, wds, wdr, sts, strv, gss, grs, lns, lnr,
):
    z, y, c, x = (lax.axis_index(a) for a in ("z", "y", "c", "x"))
    sp = (z * NY + y) * NC + c
    right, left = lax.rem(x + 1, NX), lax.rem(x + NX - 1, NX)

    def at_sp(s):
        s = lax.rem(s + 64, 64)
        return {"z": s // 8, "y": lax.rem(s // 2, NY), "c": lax.rem(s, 2)}

    own_cols = pl.ds(pl.multiple_of(x * OWN, OWN), OWN)
    loads = {}
    for i, (name, src, dst) in enumerate((
        ("small", small_h, small), ("k", k_h, k), ("v", v_h, v), ("q", q_h, q),
        ("og", og_h, og), ("res", res_h, res),
        ("w", wout_h.at[:, own_cols], wc.at[pl.ds(pl.multiple_of(x * HW, HW), HW), :]),
    )):
        loads[name] = pltpu.make_async_copy(src, dst, lsem.at[i])
        loads[name].start()

    barrier = pltpu.get_barrier_semaphore()
    peers = [{"x": lax.rem(x + r, NX)} for r in range(1, NX)]
    peers.append({"c": 1 - c})
    for j in range(1, BACK + 1):
        peers.append(at_sp(sp + j))
        peers.append(at_sp(sp - j))
    for peer in peers:
        pl.semaphore_signal(barrier, inc=1, device_id=peer, device_id_type=MESH)
    pl.semaphore_wait(barrier, len(peers))

    wsend = []
    for r in range(1, NX):
        to = lax.rem(x + r, NX)
        d = rcopy(
            wout_h.at[pl.ds(pl.multiple_of(c * 128, 128), 128), pl.ds(pl.multiple_of(to * OWN, OWN), OWN)],
            wc.at[pl.ds(pl.multiple_of(x * HW + c * 128, 128), 128), :],
            (wss, wrs), r - 1, {"x": to},
        )
        d.start()
        wsend.append(d)

    loads["small"].wait()
    ga = [small[0:8, a * BLK:(a + 1) * BLK] for a in range(NB)]
    lf = jnp.concatenate([small[8:16, a * BLK:(a + 1) * BLK] for a in range(NB)], axis=0)
    ri = lax.broadcasted_iota(jnp.int32, (BLK, BLK), 0)
    ci = lax.broadcasted_iota(jnp.int32, (BLK, BLK), 1)
    upper = (ri <= ci).astype(F32)
    cum = jnp.dot(lf, upper, precision=lax.Precision.HIGHEST, preferred_element_type=F32)
    cm = [cum[8 * a:8 * a + 8] for a in range(NB)]
    tot = [jnp.broadcast_to(cm[a][:, BLK - 1:BLK], (8, BLK)) for a in range(NB)]

    def between(b, a):
        s = jnp.zeros((8, BLK), F32)
        for i in range(b, a):
            s = s + tot[i]
        return s

    ex = [[ga[b] - cm[b] + between(b, a) if a == b else ga[b] + ((tot[b] - cm[b]) + between(b + 1, a))
           for b in range(min(a + 1, NB))] for a in range(NB + 1)]
    doc_last = jnp.broadcast_to(ga[NB - 1][2:3, BLK - 1:BLK], (8, BLK))
    doc_first = jnp.broadcast_to(ga[0][2:3, 0:1], (8, BLK))
    kept = [jnp.where(jnp.broadcast_to(ga[b][2:3], (8, BLK)) == doc_last, ex[NB][b], NEG) for b in range(NB)]
    peak = jnp.maximum(jnp.maximum(kept[0], kept[1]), jnp.maximum(kept[2], kept[3]))
    peak = jnp.broadcast_to(jnp.max(peak, axis=1, keepdims=True), (8, BLK))
    wt = [jnp.exp(kept[b] - peak) for b in range(NB)]
    wrow = jnp.concatenate(wt, axis=1).astype(BF16)

    loads["k"].wait()
    loads["v"].wait()
    sub = lax.broadcasted_iota(jnp.int32, (8, BLK), 0)
    nrm = jnp.zeros((8, BLK), F32)
    for h in range(2):
        hc = slice(h * DH, (h + 1) * DH)
        kh = k[:, hc]
        scaled = jnp.concatenate(
            [v[b * BLK:(b + 1) * BLK, hc].astype(F32) * across(wt[b][h:h + 1]) for b in range(NB)], axis=0
        ).astype(BF16)
        stout[h * DH:(h + 1) * DH, :] = lax.dot_general(
            kh, scaled, (((0,), (0,)), ((), ())), preferred_element_type=F32
        ).astype(BF16)
        nh = jnp.dot(wrow, kh, preferred_element_type=F32)
        nrm = jnp.where(sub == h, nh, nrm)
    auxout[0:8] = jnp.where(sub == 2, doc_last, peak)
    auxout[8:16] = between(0, NB)
    auxout[16:24] = nrm
    sent = []
    for j in range(1, BACK + 1):
        for i, (src, dst) in enumerate(((stout, stin.at[j - 1]), (auxout, auxin.at[j - 1]))):
            d = rcopy(src, dst, (sts, strv), 2 * (j - 1) + i, at_sp(sp + j))
            d.start()
            sent.append(d)

    loads["q"].wait()
    scale = DH ** (-0.5)
    ones = jnp.ones((ROWS, DH), BF16)
    dcol = [across(ga[a][2:3]) for a in range(NB)]
    for h in range(2):
        hc = slice(h * DH, (h + 1) * DH)
        vx = jnp.concatenate([v[:, hc], ones], axis=1)
        for a in range(NB):
            n = (a + 1) * BLK
            qa = q[a * BLK:n, hc]
            sc = lax.dot_general(qa, k[:n, hc], (((1,), (1,)), ((), ())), preferred_element_type=F32)
            es = []
            for b in range(a + 1):
                ok = dcol[a] == ga[b][2:3]
                if b == a:
                    ok = ok & (ci <= ri)
                es.append(jnp.where(ok, ex[a][b][h:h + 1], NEG))
            best = es[0]
            for e in es[1:]:
                best = jnp.maximum(best, e)
            best = jnp.max(best, axis=1, keepdims=True)
            p = jnp.concatenate(
                [(jnp.exp(es[b] - best) * (sc[:, b * BLK:(b + 1) * BLK] * scale)).astype(BF16) for b in range(a + 1)], axis=1
            )
            nd[h, a * BLK:n, :] = jnp.dot(p, vx[:n], preferred_element_type=F32)
            top[h, a * BLK:n, :] = jnp.broadcast_to(best, (BLK, BLK))

    wpass = []
    for r in range(1, NX):
        wsend[r - 1].wait_recv()
        rows = wc.at[pl.ds(pl.multiple_of(lax.rem(x + NX - r, NX) * HW + c * 128, 128), 128), :]
        d = rcopy(rows, rows, (wds, wdr), r - 1, {"c": 1 - c})
        d.start()
        wpass.append(d)

    for d in sent:
        d.wait_recv()
    gone = jnp.zeros((8, BLK), F32)
    logs = []
    for j in range(1, BACK + 1):
        a = auxin[j - 1, 0:8]
        live = (jnp.broadcast_to(a[2:3], (8, BLK)) == doc_first) & (sp >= j)
        logs.append(jnp.where(live, a + gone, NEG))
        gone = gone + auxin[j - 1, 8:16]
    came = jnp.maximum(jnp.maximum(logs[0], logs[1]), jnp.maximum(logs[2], logs[3]))
    part = [jnp.where(lg > 0.5 * NEG, jnp.exp(lg - came), 0.0) for lg in logs]
    nin = jnp.zeros((8, BLK), F32)
    for j in range(BACK):
        nin = nin + part[j] * auxin[j, 16:24]
    memx = []
    for h in range(2):
        m = jnp.zeros((DH, DH), F32)
        for j in range(BACK):
            m = m + part[j][h:h + 1] * stin[j, h * DH:(h + 1) * DH, :].astype(F32)
        memx.append(jnp.concatenate([m, across(nin[h:h + 1])], axis=1).astype(BF16))

    loads["og"].wait()
    ucols = lambda xi: pl.ds(pl.multiple_of(xi * HW, HW), HW)
    for a in range(NB):
        rows = slice(a * BLK, (a + 1) * BLK)
        squares = jnp.zeros((BLK, DH), F32)
        outs = []
        for h in range(2):
            hc = slice(h * DH, (h + 1) * DH)
            qm = jnp.dot(q[rows, hc], memx[h], preferred_element_type=F32) * scale
            far = jnp.where(dcol[a] == doc_first[0:1], (between(0, a) + came)[h:h + 1], NEG)
            near = top[h, rows, :]
            m = jnp.maximum(near, far)
            wn, wf = jnp.exp(near - m), jnp.exp(far - m)
            num = wn * nd[h, rows, :DH] + wf * qm[:, :DH]
            den = wn * nd[h, rows, DH:] + wf * qm[:, DH:]
            cell = num / jnp.maximum(jnp.abs(den), 1.0)
            squares = squares + cell * cell
            gate = jax.nn.sigmoid(og[rows, hc].astype(F32))
            outs.append((gate * cell * ga[h][3:4]).astype(BF16))
        u[rows, ucols(x)] = jnp.concatenate(outs, axis=1)
        line1[:, rows] = rows_of(squares)

    gu = Gather(
        lambda xi, half: u.at[:, ucols(xi)] if half is None else u.at[pl.ds(half * 256, 256), ucols(xi)],
        (gss, grs), 0, x,
    )
    gu.start()
    lsent = []
    for r in range(1, NX):
        d = rcopy(line1, line1in.at[r - 1], (lns, lnr), r - 1, {"x": lax.rem(x + r, NX)})
        d.start()
        lsent.append(d)
    gu.forward()
    for d in lsent:
        d.wait_recv()
    total = line1[...] + line1in[0] + line1in[1] + line1in[2]
    inv = lax.rsqrt(total / (DH * 8) + EPS)
    loads["w"].wait()
    loads["res"].wait()
    for d in wpass:
        d.wait_recv()
    gu.finish()
    for a in range(NB):
        rows = slice(a * BLK, (a + 1) * BLK)
        ic = across(inv[0:1, rows])
        acc = jnp.dot(u[rows, :], wc[...], preferred_element_type=F32)
        squares = jnp.zeros((BLK, BLK), F32)
        outs = []
        for b in range(OWN // BLK):
            cols = slice(b * BLK, (b + 1) * BLK)
            f = (res[rows, cols].astype(F32) + acc[:, cols] * ic).astype(BF16)
            fw = f.astype(F32)
            squares = squares + fw * fw
            outs.append(f)
        f = jnp.concatenate(outs, axis=1)
        full[rows, own_cols] = f
        first_own[rows, :] = f
        line2[:, rows] = rows_of(squares)
    line2[1:2, :] = small[4:5, :]

    fcols = lambda xi: pl.ds(pl.multiple_of(xi * OWN, OWN), OWN)
    gf = Gather(
        lambda xi, half: full.at[:, fcols(xi)] if half is None else full.at[pl.ds(half * 256, 256), fcols(xi)],
        (gss, grs), 4, x,
    )
    gf.start()
    for r in range(1, NX):
        d = rcopy(line2, line2in.at[r - 1], (lns, lnr), NX - 1 + r - 1, {"x": lax.rem(x + r, NX)})
        d.start()
        lsent.append(d)
    gf.forward()
    for d in lsent[NX - 1:]:
        d.wait_recv()
    total = line2[...] + line2in[0] + line2in[1] + line2in[2]
    inv = lax.rsqrt(total / DM + EPS)
    gf.finish()
    icol = [across(inv[0:1, a * BLK:(a + 1) * BLK]) for a in range(NB)]
    for r in range(NX):
        xi = lax.rem(x + NX - r, NX)
        gain = line2[1:2, :] if r == 0 else line2in[r - 1, 1:2, :]
        for a in range(NB):
            rows = slice(a * BLK, (a + 1) * BLK)
            fw = full[rows, fcols(xi)].astype(F32)
            outs = [
                (fw[:, b * BLK:(b + 1) * BLK] * icol[a] * gain[:, b * BLK:(b + 1) * BLK]).astype(BF16)
                for b in range(OWN // BLK)
            ]
            normed[rows, fcols(xi)] = jnp.concatenate(outs, axis=1)
    for d in wsend + wpass + sent + lsent:
        d.wait_send()


def cell_and_norm(small, q, k, v, og, res, wout):
    dma = pltpu.SemaphoreType.DMA
    return pl.pallas_call(
        kernel,
        out_shape=(
            jax.ShapeDtypeStruct((ROWS, DM), BF16),
            jax.ShapeDtypeStruct((ROWS, OWN), BF16),
        ),
        in_specs=[pl.BlockSpec(memory_space=pl.ANY)] * 7,
        out_specs=(pl.BlockSpec(memory_space=pltpu.VMEM),) * 2,
        scratch_shapes=[
            pltpu.VMEM((16, ROWS), F32),
            *[pltpu.VMEM((ROWS, HW), BF16)] * 4,
            pltpu.VMEM((ROWS, OWN), BF16),
            pltpu.VMEM((4 * HW, OWN), BF16),
            pltpu.VMEM((2, ROWS, 2 * DH), F32),
            pltpu.VMEM((2, ROWS, DH), F32),
            pltpu.VMEM((2 * DH, DH), BF16),
            pltpu.VMEM((24, BLK), F32),
            pltpu.VMEM((BACK, 2 * DH, DH), BF16),
            pltpu.VMEM((BACK, 24, BLK), F32),
            pltpu.VMEM((ROWS, 4 * HW), BF16),
            pltpu.VMEM((8, ROWS), F32),
            pltpu.VMEM((3, 8, ROWS), F32),
            pltpu.VMEM((ROWS, DM), BF16),
            pltpu.VMEM((8, ROWS), F32),
            pltpu.VMEM((3, 8, ROWS), F32),
            dma((7,)), dma((3,)), dma((3,)), dma((3,)), dma((3,)),
            dma((8,)), dma((8,)), dma((8,)), dma((8,)), dma((6,)), dma((6,)),
        ],
        compiler_params=pltpu.CompilerParams(
            collective_id=0, has_side_effects=True, vmem_limit_bytes=48 * 2**20
        ),
        cost_estimate=pl.CostEstimate(flops=40_000_000_000, bytes_accessed=2**22, transcendentals=0),
    )(small, q, k, v, og, res, wout)


def small_rows(igate, fgate, extra, document, cgain, mgain):
    f = lambda a: a.astype(F32)
    cg = f(cgain).reshape(2, DH)
    cgrow = jnp.concatenate([cg.reshape(1, 2 * DH), jnp.zeros((1, ROWS - 2 * DH), F32)], axis=1)
    top = jnp.concatenate(
        [igate.T, f(document)[None], cgrow, f(mgain)[None], jnp.zeros((3, ROWS), F32)], axis=0
    )
    lf = (jax.nn.log_sigmoid(fgate) + extra).T
    return jnp.concatenate([top, lf, jnp.zeros((6, ROWS), F32)], axis=0)


def cut_along(value, dim, count):
    lengths = value.shape
    parts = value.reshape(*lengths[:dim], count, lengths[dim] // count, *lengths[dim + 1 :])
    return jnp.moveaxis(parts, dim, 0)


def summed_on_arrival(value, axis, dim):
    parts = cut_along(value, dim, lax.axis_size(axis))
    arrived = lax.all_to_all(parts, axis, split_axis=0, concat_axis=0, tiled=True)
    return arrived.astype(jnp.float32).sum(axis=0)


def local(
    queries, keys, values, output_gate_logits, input_gate_log, forget_gate_logits, extra_decay_log,
    document, residual, cell_norm_gain, output_weight, mixer_norm_gain, up_weight, down_weight,
):
    both = jnp.concatenate([up_weight, down_weight.T], axis=1)
    whole = lax.all_gather(both, SP, axis=0, tiled=True)
    small = small_rows(
        input_gate_log, forget_gate_logits, extra_decay_log, document, cell_norm_gain, mixer_norm_gain
    )
    normed, first = cell_and_norm(
        small, queries, keys, values, output_gate_logits, residual, output_weight
    )
    hidden = jnp.dot(normed, whole[:, :DM], preferred_element_type=F32)
    squared = jnp.square(jax.nn.relu(hidden)).astype(BF16)
    channel = lax.dot_general(squared, whole[:, DM:], (((1,), (1,)), ((), ())), preferred_element_type=F32)
    own = summed_on_arrival(channel.astype(BF16), "x", 1)
    return (first.astype(F32) + own).astype(BF16)


def solution(mesh):
    split = Mesh(mesh.devices.reshape(NZ, NY, NC, NX), ("z", "y", "c", "x"))
    rows, heads = P(SP, "x"), P("x")
    return jax.shard_map(
        local,
        mesh=split,
        in_specs=(
            rows, rows, rows, rows, rows, rows, rows, P(SP), rows, heads, P("x", None), heads, rows, P("x", SP),
        ),
        out_specs=rows,
        check_vma=False,
    )
```

```python
import jax
import jax.numpy as jnp
from jax import lax
from jax.experimental import pallas as pl
from jax.experimental.pallas import tpu as pltpu
from jax.sharding import Mesh
from jax.sharding import PartitionSpec as P

MESH = pl.DeviceIdType.MESH
SP = ("z", "y", "c")
NZ, NY, NC, NX = 8, 4, 2, 4
ROWS, DH, BLK = 512, 128, 128
HW = 256
DM = 2048
OWN = 512
NB = ROWS // BLK
BACK = 4
NEG = -1e30
EPS = 1e-6
F32, BF16 = jnp.float32, jnp.bfloat16


def rcopy(src, dst, sems, i, dev):
    return pltpu.make_async_remote_copy(
        src_ref=src, dst_ref=dst, send_sem=sems[0].at[i], recv_sem=sems[1].at[i],
        device_id=dev, device_id_type=MESH,
    )


def across(row):
    return jnp.transpose(jnp.broadcast_to(row, (BLK, BLK)))


def rows_of(values):
    return lax.dot_general(
        jnp.ones((8, BLK), F32), values, (((1,), (1,)), ((), ())),
        precision=lax.Precision.HIGHEST, preferred_element_type=F32,
    )


class Gather:
    def __init__(self, view, sems, base, x):
        self.view, self.sems, self.base, self.x = view, sems, base, x
        self.right, self.left = lax.rem(x + 1, NX), lax.rem(x + NX - 1, NX)

    def start(self):
        own = self.view(self.x, None)
        self.r = rcopy(own, own, self.sems, self.base, {"x": self.right})
        self.l = rcopy(own, own, self.sems, self.base + 1, {"x": self.left})
        self.r.start()
        self.l.start()

    def forward(self):
        self.r.wait_recv()
        a = self.view(self.left, 0)
        self.fr = rcopy(a, a, self.sems, self.base + 2, {"x": self.right})
        self.fr.start()
        self.l.wait_recv()
        b = self.view(self.right, 1)
        self.fl = rcopy(b, b, self.sems, self.base + 3, {"x": self.left})
        self.fl.start()

    def finish(self):
        self.fr.wait_recv()
        self.fl.wait_recv()
        for d in (self.r, self.l, self.fr, self.fl):
            d.wait_send()


class Weights:
    RIGHT = (0, -2, 2)

    def __init__(self, wup, wdn, us, ds, z, y, c, dirs):
        self.wup, self.wdn, self.us, self.ds = wup, wdn, us, ds
        self.z, self.y, self.c = z, y, c
        self.yr, self.yl, self.zr, self.zl = dirs
        self.other = {"c": 1 - c}
        self.un = self.dn = 0
        self.all = []
        self.got = {}
        self.mates = {"up": [], "down": []}

    def zi(self, o):
        return lax.rem(self.z + NZ + o, NZ)

    def yi(self, o):
        return lax.rem(self.y + NY + o, NY)

    def send(self, kind, ref, dev, key):
        sems, i = (self.us, self.un) if kind == "up" else (self.ds, self.dn)
        if kind == "up":
            self.un += 1
        else:
            self.dn += 1
        d = rcopy(ref, ref, sems, i, dev)
        d.start()
        self.all.append(d)
        self.got[key] = d

    def up(self, zo, yo):
        return self.wup.at[self.zi(zo), self.yi(yo), self.c]

    def begin(self):
        own = self.up(0, 0)
        self.send("up", own, self.zr, ("uz", -1))
        self.send("up", own, self.zl, ("uz", 1))
        own = self.wdn.at[self.z, self.y, self.c]
        self.send("down", own, self.yr, ("dy", -1))
        self.send("down", own, self.yl, ("dy", 1))

    def up_y(self, zo):
        own = self.up(zo, 0)
        self.send("up", own, self.yr, ("uy", zo, -1))
        self.send("up", own, self.yl, ("uy", zo, 1))

    def up_z(self, zo):
        self.got["uz", zo].wait_recv()
        if -4 < zo < 0:
            self.send("up", self.up(zo, 0), self.zr, ("uz", zo - 1))
        elif 0 < zo < 3:
            self.send("up", self.up(zo, 0), self.zl, ("uz", zo + 1))
        self.up_y(zo)

    def up_pass(self, zo):
        self.got["uy", zo, -1].wait_recv()
        self.got["uy", zo, 1].wait_recv()
        if zo in self.RIGHT:
            self.send("up", self.up(zo, -1), self.yr, ("uo", zo))
        else:
            self.send("up", self.up(zo, 1), self.yl, ("uo", zo))

    def mate(self, kind, ref):
        self.send(kind, ref, self.other, (kind, "mate", len(self.mates[kind])))
        self.mates[kind].append(self.all[-1])

    def up_mate(self, yo):
        self.mate("up", self.wup.at[:, self.yi(yo), self.c])

    def down_y(self):
        lo, hi = pl.ds(0, 16), pl.ds(16, 16)
        self.got["dy", -1].wait_recv()
        self.send("down", self.wdn.at[self.z, self.yi(-1), self.c, lo], self.yr, ("do", 0))
        self.got["dy", 1].wait_recv()
        self.send("down", self.wdn.at[self.z, self.yi(1), self.c, hi], self.yl, ("do", 1))

    def block(self, zo, half):
        return self.wdn.at[self.zi(zo), pl.ds(2 * half, 2), self.c]

    def down_z(self, zo, side):
        dev = self.zr if side < 0 else self.zl
        last = zo == 3 * side
        for half in (0, 1):
            if last and half != (0 if side < 0 else 1):
                continue
            self.send("down", self.block(zo, half), dev, ("dz", zo + side, half))

    def down_start(self):
        self.got["do", 0].wait_recv()
        self.got["do", 1].wait_recv()
        self.down_z(0, -1)
        self.down_z(0, 1)
        self.mate("down", self.wdn.at[self.z, :, self.c])

    def down_step(self, n):
        for side in (-1, 1):
            zo = n * side
            for half in (0, 1):
                self.got["dz", zo, half].wait_recv()
            self.down_z(zo, side)
            self.mate("down", self.wdn.at[self.zi(zo), :, self.c])

    def down_last(self):
        self.got["dz", -4, 0].wait_recv()
        self.got["dz", 4, 1].wait_recv()
        self.mate("down", self.wdn.at[self.zi(4), :, self.c])

    def serve(self, at):
        if at == "y0":
            self.up_y(0)
            self.down_y()
            self.up_z(-1)
            self.up_z(1)
        elif at == "cell0":
            self.down_start()
            self.up_z(-2)
            self.up_z(2)
        elif at == "cell1":
            self.up_pass(0)
        elif at == "u0":
            self.up_pass(-1)
            self.up_pass(1)
            self.up_z(-3)
            self.up_z(3)
        elif at == "u1":
            self.up_pass(-2)
            self.up_pass(2)
            self.down_step(1)
        elif at == "f0":
            self.up_z(-4)
            self.up_mate(0)
            self.up_pass(-3)
            self.up_pass(3)
        elif at == "f1":
            self.down_step(2)
            self.up_pass(-4)
            self.up_mate(-1)
            self.up_mate(1)
        elif at == "up":
            for zo in range(-4, 4):
                self.got["uo", zo].wait_recv()
            self.up_mate(2)
            self.down_step(3)
            for d in self.mates["up"]:
                d.wait_recv()
        elif at == "down":
            self.down_last()
            for d in self.mates["down"]:
                d.wait_recv()

    def end(self):
        for d in self.all:
            d.wait_send()


def kernel(
    small_h, q_h, k_h, v_h, og_h, res_h, wout_h, up_h, down_h,
    out,
    small, q, k, v, og, res, wc, nd, top, stout, auxout, stin, auxin,
    u, line1, line1in, full, line2, line2in, normed, wup, wdn, squared, terms, parts,
    lsem, wss, wrs, wds, wdr, sts, strv, gss, grs, lns, lnr, uss, urs, dss, drs, rss, rrs,
):
    z, y, c, x = (lax.axis_index(a) for a in ("z", "y", "c", "x"))
    sp = (z * NY + y) * NC + c
    right, left = lax.rem(x + 1, NX), lax.rem(x + NX - 1, NX)

    def at_sp(s):
        s = lax.rem(s + 64, 64)
        return {"z": s // 8, "y": lax.rem(s // 2, NY), "c": lax.rem(s, 2)}

    own_cols = pl.ds(pl.multiple_of(x * OWN, OWN), OWN)
    loads = {}
    for i, (name, src, dst) in enumerate((
        ("up", up_h, wup.at[z, y, c]), ("down", down_h, wdn.at[z, y, c]),
        ("small", small_h, small), ("k", k_h, k), ("v", v_h, v), ("q", q_h, q),
        ("og", og_h, og), ("res", res_h, res),
        ("w", wout_h.at[:, own_cols], wc.at[pl.ds(pl.multiple_of(x * HW, HW), HW), :]),
    )):
        loads[name] = pltpu.make_async_copy(src, dst, lsem.at[i])
        loads[name].start()

    barrier = pltpu.get_barrier_semaphore()
    peers = [{"x": lax.rem(x + r, NX)} for r in range(1, NX)]
    peers.append({"c": 1 - c})
    yr, yl, zr, zl = ({"y": lax.rem(y + 1, NY)}, {"y": lax.rem(y + NY - 1, NY)},
                      {"z": lax.rem(z + 1, NZ)}, {"z": lax.rem(z + NZ - 1, NZ)})
    peers += [yr, yl, zr, zl]
    for j in range(1, BACK + 1):
        peers.append(at_sp(sp + j))
        peers.append(at_sp(sp - j))
    for peer in peers:
        pl.semaphore_signal(barrier, inc=1, device_id=peer, device_id_type=MESH)
    pl.semaphore_wait(barrier, len(peers))

    ring = Weights(wup, wdn, (uss, urs), (dss, drs), z, y, c, (yr, yl, zr, zl))
    loads["up"].wait()
    loads["down"].wait()
    ring.begin()

    wsend = []
    for r in range(1, NX):
        to = lax.rem(x + r, NX)
        d = rcopy(
            wout_h.at[pl.ds(pl.multiple_of(c * 128, 128), 128), pl.ds(pl.multiple_of(to * OWN, OWN), OWN)],
            wc.at[pl.ds(pl.multiple_of(x * HW + c * 128, 128), 128), :],
            (wss, wrs), r - 1, {"x": to},
        )
        d.start()
        wsend.append(d)

    loads["small"].wait()
    ga = [small[0:8, a * BLK:(a + 1) * BLK] for a in range(NB)]
    lf = jnp.concatenate([small[8:16, a * BLK:(a + 1) * BLK] for a in range(NB)], axis=0)
    ri = lax.broadcasted_iota(jnp.int32, (BLK, BLK), 0)
    ci = lax.broadcasted_iota(jnp.int32, (BLK, BLK), 1)
    upper = (ri <= ci).astype(F32)
    cum = jnp.dot(lf, upper, precision=lax.Precision.HIGHEST, preferred_element_type=F32)
    cm = [cum[8 * a:8 * a + 8] for a in range(NB)]
    tot = [jnp.broadcast_to(cm[a][:, BLK - 1:BLK], (8, BLK)) for a in range(NB)]

    def between(b, a):
        s = jnp.zeros((8, BLK), F32)
        for i in range(b, a):
            s = s + tot[i]
        return s

    ex = [[ga[b] - cm[b] + between(b, a) if a == b else ga[b] + ((tot[b] - cm[b]) + between(b + 1, a))
           for b in range(min(a + 1, NB))] for a in range(NB + 1)]
    doc_last = jnp.broadcast_to(ga[NB - 1][2:3, BLK - 1:BLK], (8, BLK))
    doc_first = jnp.broadcast_to(ga[0][2:3, 0:1], (8, BLK))
    kept = [jnp.where(jnp.broadcast_to(ga[b][2:3], (8, BLK)) == doc_last, ex[NB][b], NEG) for b in range(NB)]
    peak = jnp.maximum(jnp.maximum(kept[0], kept[1]), jnp.maximum(kept[2], kept[3]))
    peak = jnp.broadcast_to(jnp.max(peak, axis=1, keepdims=True), (8, BLK))
    wt = [jnp.exp(kept[b] - peak) for b in range(NB)]
    wrow = jnp.concatenate(wt, axis=1).astype(BF16)

    loads["k"].wait()
    loads["v"].wait()
    sub = lax.broadcasted_iota(jnp.int32, (8, BLK), 0)
    nrm = jnp.zeros((8, BLK), F32)
    for h in range(2):
        hc = slice(h * DH, (h + 1) * DH)
        kh = k[:, hc]
        scaled = jnp.concatenate(
            [v[b * BLK:(b + 1) * BLK, hc].astype(F32) * across(wt[b][h:h + 1]) for b in range(NB)], axis=0
        ).astype(BF16)
        stout[h * DH:(h + 1) * DH, :] = lax.dot_general(
            kh, scaled, (((0,), (0,)), ((), ())), preferred_element_type=F32
        ).astype(BF16)
        nh = jnp.dot(wrow, kh, preferred_element_type=F32)
        nrm = jnp.where(sub == h, nh, nrm)
    auxout[0:8] = jnp.where(sub == 2, doc_last, peak)
    auxout[8:16] = between(0, NB)
    auxout[16:24] = nrm
    sent = []
    for j in range(1, BACK + 1):
        for i, (src, dst) in enumerate(((stout, stin.at[j - 1]), (auxout, auxin.at[j - 1]))):
            d = rcopy(src, dst, (sts, strv), 2 * (j - 1) + i, at_sp(sp + j))
            d.start()
            sent.append(d)
    ring.serve("y0")

    loads["q"].wait()
    scale = DH ** (-0.5)
    ones = jnp.ones((ROWS, DH), BF16)
    dcol = [across(ga[a][2:3]) for a in range(NB)]
    for h in range(2):
        hc = slice(h * DH, (h + 1) * DH)
        vx = jnp.concatenate([v[:, hc], ones], axis=1)
        for a in range(NB):
            n = (a + 1) * BLK
            qa = q[a * BLK:n, hc]
            sc = lax.dot_general(qa, k[:n, hc], (((1,), (1,)), ((), ())), preferred_element_type=F32)
            es = []
            for b in range(a + 1):
                ok = dcol[a] == ga[b][2:3]
                if b == a:
                    ok = ok & (ci <= ri)
                es.append(jnp.where(ok, ex[a][b][h:h + 1], NEG))
            best = es[0]
            for e in es[1:]:
                best = jnp.maximum(best, e)
            best = jnp.max(best, axis=1, keepdims=True)
            p = jnp.concatenate(
                [(jnp.exp(es[b] - best) * (sc[:, b * BLK:(b + 1) * BLK] * scale)).astype(BF16) for b in range(a + 1)], axis=1
            )
            nd[h, a * BLK:n, :] = jnp.dot(p, vx[:n], preferred_element_type=F32)
            top[h, a * BLK:n, :] = jnp.broadcast_to(best, (BLK, BLK))
        ring.serve("cell%d" % h)

    wpass = []
    for r in range(1, NX):
        wsend[r - 1].wait_recv()
        rows = wc.at[pl.ds(pl.multiple_of(lax.rem(x + NX - r, NX) * HW + c * 128, 128), 128), :]
        d = rcopy(rows, rows, (wds, wdr), r - 1, {"c": 1 - c})
        d.start()
        wpass.append(d)

    ring.serve("pass")
    for d in sent:
        d.wait_recv()
    gone = jnp.zeros((8, BLK), F32)
    logs = []
    for j in range(1, BACK + 1):
        a = auxin[j - 1, 0:8]
        live = (jnp.broadcast_to(a[2:3], (8, BLK)) == doc_first) & (sp >= j)
        logs.append(jnp.where(live, a + gone, NEG))
        gone = gone + auxin[j - 1, 8:16]
    came = jnp.maximum(jnp.maximum(logs[0], logs[1]), jnp.maximum(logs[2], logs[3]))
    part = [jnp.where(lg > 0.5 * NEG, jnp.exp(lg - came), 0.0) for lg in logs]
    nin = jnp.zeros((8, BLK), F32)
    for j in range(BACK):
        nin = nin + part[j] * auxin[j, 16:24]
    memx = []
    for h in range(2):
        m = jnp.zeros((DH, DH), F32)
        for j in range(BACK):
            m = m + part[j][h:h + 1] * stin[j, h * DH:(h + 1) * DH, :].astype(F32)
        memx.append(jnp.concatenate([m, across(nin[h:h + 1])], axis=1).astype(BF16))

    loads["og"].wait()
    ucols = lambda xi: pl.ds(pl.multiple_of(xi * HW, HW), HW)
    for a in range(NB):
        rows = slice(a * BLK, (a + 1) * BLK)
        squares = jnp.zeros((BLK, DH), F32)
        outs = []
        for h in range(2):
            hc = slice(h * DH, (h + 1) * DH)
            qm = jnp.dot(q[rows, hc], memx[h], preferred_element_type=F32) * scale
            far = jnp.where(dcol[a] == doc_first[0:1], (between(0, a) + came)[h:h + 1], NEG)
            near = top[h, rows, :]
            m = jnp.maximum(near, far)
            wn, wf = jnp.exp(near - m), jnp.exp(far - m)
            num = wn * nd[h, rows, :DH] + wf * qm[:, :DH]
            den = wn * nd[h, rows, DH:] + wf * qm[:, DH:]
            cell = num / jnp.maximum(jnp.abs(den), 1.0)
            squares = squares + cell * cell
            gate = jax.nn.sigmoid(og[rows, hc].astype(F32))
            outs.append((gate * cell * ga[h][3:4]).astype(BF16))
        u[rows, ucols(x)] = jnp.concatenate(outs, axis=1)
        line1[:, rows] = rows_of(squares)

    gu = Gather(
        lambda xi, half: u.at[:, ucols(xi)] if half is None else u.at[pl.ds(half * 256, 256), ucols(xi)],
        (gss, grs), 0, x,
    )
    gu.start()
    lsent = []
    for r in range(1, NX):
        d = rcopy(line1, line1in.at[r - 1], (lns, lnr), r - 1, {"x": lax.rem(x + r, NX)})
        d.start()
        lsent.append(d)
    ring.serve("u0")
    gu.forward()
    ring.serve("u1")
    for d in lsent:
        d.wait_recv()
    total = line1[...] + line1in[0] + line1in[1] + line1in[2]
    inv = lax.rsqrt(total / (DH * 8) + EPS)
    loads["w"].wait()
    loads["res"].wait()
    for d in wpass:
        d.wait_recv()
    gu.finish()
    for a in range(NB):
        rows = slice(a * BLK, (a + 1) * BLK)
        ic = across(inv[0:1, rows])
        acc = jnp.dot(u[rows, :], wc[...], preferred_element_type=F32)
        squares = jnp.zeros((BLK, BLK), F32)
        outs = []
        for b in range(OWN // BLK):
            cols = slice(b * BLK, (b + 1) * BLK)
            f = (res[rows, cols].astype(F32) + acc[:, cols] * ic).astype(BF16)
            fw = f.astype(F32)
            squares = squares + fw * fw
            outs.append(f)
        f = jnp.concatenate(outs, axis=1)
        full[rows, own_cols] = f
        line2[:, rows] = rows_of(squares)
    line2[1:2, :] = small[4:5, :]

    fcols = lambda xi: pl.ds(pl.multiple_of(xi * OWN, OWN), OWN)
    gf = Gather(
        lambda xi, half: full.at[:, fcols(xi)] if half is None else full.at[pl.ds(half * 256, 256), fcols(xi)],
        (gss, grs), 4, x,
    )
    gf.start()
    for r in range(1, NX):
        d = rcopy(line2, line2in.at[r - 1], (lns, lnr), NX - 1 + r - 1, {"x": lax.rem(x + r, NX)})
        d.start()
        lsent.append(d)
    ring.serve("f0")
    gf.forward()
    ring.serve("f1")
    for d in lsent[NX - 1:]:
        d.wait_recv()
    total = line2[...] + line2in[0] + line2in[1] + line2in[2]
    inv = lax.rsqrt(total / DM + EPS)
    gf.finish()
    icol = [across(inv[0:1, a * BLK:(a + 1) * BLK]) for a in range(NB)]
    for r in range(NX):
        xi = lax.rem(x + NX - r, NX)
        gain = line2[1:2, :] if r == 0 else line2in[r - 1, 1:2, :]
        for a in range(NB):
            rows = slice(a * BLK, (a + 1) * BLK)
            fw = full[rows, fcols(xi)].astype(F32)
            outs = [
                (fw[:, b * BLK:(b + 1) * BLK] * icol[a] * gain[:, b * BLK:(b + 1) * BLK]).astype(BF16)
                for b in range(OWN // BLK)
            ]
            normed[rows, fcols(xi)] = jnp.concatenate(outs, axis=1)

    ring.serve("up")
    for t in range(4):
        cols = slice(t * 512, (t + 1) * 512)
        hid = jnp.dot(normed[...], wup[:, :, :, :, cols].reshape(DM, 512), preferred_element_type=F32)
        hid = jnp.maximum(hid, 0.0)
        squared[:, cols] = (hid * hid).astype(BF16)
        ring.serve("up%d" % t)
    ring.serve("down")

    def project(r):
        to = lax.rem(x + r, NX)
        w = wdn[pl.ds(2 * to, 2)].reshape(OWN, DM)
        return lax.dot_general(squared[...], w, (((1,), (1,)), ((), ())), preferred_element_type=F32)

    first, second = slice(0, 256), slice(256, 512)
    rsem = (rss, rrs)
    terms[2] = project(2).astype(BF16)
    i1 = rcopy(terms.at[2, first], parts.at[0], rsem, 0, {"x": right})
    i2 = rcopy(terms.at[2, second], parts.at[1], rsem, 1, {"x": left})
    i1.start()
    i2.start()
    c1 = project(1)
    terms[1] = c1.astype(BF16)
    i3 = rcopy(terms.at[1, second], parts.at[2], rsem, 2, {"x": right})
    i3.start()
    c3 = project(3)
    terms[3] = c3.astype(BF16)
    i4 = rcopy(terms.at[3, first], parts.at[3], rsem, 3, {"x": left})
    i4.start()
    i1.wait_recv()
    terms[1, first] = (terms[1, first].astype(F32) + parts[0].astype(F32)).astype(BF16)
    i5 = rcopy(terms.at[1, first], parts.at[4], rsem, 4, {"x": right})
    i5.start()
    i2.wait_recv()
    terms[3, second] = (terms[3, second].astype(F32) + parts[1].astype(F32)).astype(BF16)
    i6 = rcopy(terms.at[3, second], parts.at[5], rsem, 5, {"x": left})
    i6.start()
    mine = project(0) + full[:, own_cols].astype(F32)
    for d in (i3, i4, i5, i6):
        d.wait_recv()
    out[first] = (mine[first] + parts[3].astype(F32) + parts[4].astype(F32)).astype(BF16)
    out[second] = (mine[second] + parts[2].astype(F32) + parts[5].astype(F32)).astype(BF16)
    for d in wsend + wpass + sent + lsent + [i1, i2, i3, i4, i5, i6]:
        d.wait_send()
    ring.end()


def layer(small, q, k, v, og, res, wout, up, down):
    dma = pltpu.SemaphoreType.DMA
    return pl.pallas_call(
        kernel,
        out_shape=jax.ShapeDtypeStruct((ROWS, OWN), BF16),
        in_specs=[pl.BlockSpec(memory_space=pltpu.HBM)] * 9,
        out_specs=pl.BlockSpec(memory_space=pltpu.VMEM),
        scratch_shapes=[
            pltpu.VMEM((16, ROWS), F32),
            *[pltpu.VMEM((ROWS, HW), BF16)] * 4,
            pltpu.VMEM((ROWS, OWN), BF16),
            pltpu.VMEM((4 * HW, OWN), BF16),
            pltpu.VMEM((2, ROWS, 2 * DH), F32),
            pltpu.VMEM((2, ROWS, DH), F32),
            pltpu.VMEM((2 * DH, DH), BF16),
            pltpu.VMEM((24, BLK), F32),
            pltpu.VMEM((BACK, 2 * DH, DH), BF16),
            pltpu.VMEM((BACK, 24, BLK), F32),
            pltpu.VMEM((ROWS, 4 * HW), BF16),
            pltpu.VMEM((8, ROWS), F32),
            pltpu.VMEM((3, 8, ROWS), F32),
            pltpu.VMEM((ROWS, DM), BF16),
            pltpu.VMEM((8, ROWS), F32),
            pltpu.VMEM((3, 8, ROWS), F32),
            pltpu.VMEM((ROWS, DM), BF16),
            pltpu.VMEM((NZ, NY, NC, 32, DM), BF16),
            pltpu.VMEM((NZ, NY, NC, 32, DM), BF16),
            pltpu.VMEM((ROWS, DM), BF16),
            pltpu.VMEM((4, ROWS, OWN), BF16),
            pltpu.VMEM((6, ROWS // 2, OWN), BF16),
            dma((9,)), dma((3,)), dma((3,)), dma((3,)), dma((3,)),
            dma((8,)), dma((8,)), dma((8,)), dma((8,)), dma((6,)), dma((6,)),
            dma((35,)), dma((35,)), dma((26,)), dma((26,)), dma((6,)), dma((6,)),
        ],
        compiler_params=pltpu.CompilerParams(
            collective_id=0, has_side_effects=True, vmem_limit_bytes=62 * 2**20
        ),
    )(small, q, k, v, og, res, wout, up, down)


def small_rows(igate, fgate, extra, document, cgain, mgain):
    f = lambda a: a.astype(F32)
    cg = f(cgain).reshape(2, DH)
    cgrow = jnp.concatenate([cg.reshape(1, 2 * DH), jnp.zeros((1, ROWS - 2 * DH), F32)], axis=1)
    top = jnp.concatenate(
        [igate.T, f(document)[None], cgrow, f(mgain)[None], jnp.zeros((3, ROWS), F32)], axis=0
    )
    lf = (jax.nn.log_sigmoid(fgate) + extra).T
    return jnp.concatenate([top, lf, jnp.zeros((6, ROWS), F32)], axis=0)


def local(
    queries, keys, values, output_gate_logits, input_gate_log, forget_gate_logits, extra_decay_log,
    document, residual, cell_norm_gain, output_weight, mixer_norm_gain, up_weight, down_weight,
):
    small = small_rows(
        input_gate_log, forget_gate_logits, extra_decay_log, document, cell_norm_gain, mixer_norm_gain
    )
    return layer(
        small, queries, keys, values, output_gate_logits, residual, output_weight, up_weight, down_weight.T
    )


def solution(mesh):
    split = Mesh(mesh.devices.reshape(NZ, NY, NC, NX), ("z", "y", "c", "x"))
    rows, heads = P(SP, "x"), P("x")
    return jax.shard_map(
        local,
        mesh=split,
        in_specs=(
            rows, rows, rows, rows, rows, rows, rows, P(SP), rows, heads, P("x", None), heads, rows, P("x", SP),
        ),
        out_specs=rows,
        check_vma=False,
    )
```

```python
import jax
import jax.numpy as jnp
from jax import lax
from jax.experimental import pallas as pl
from jax.experimental.pallas import tpu as pltpu
from jax.sharding import Mesh
from jax.sharding import PartitionSpec as P

MESH = pl.DeviceIdType.MESH
SP = ("z", "y", "c")
NZ, NY, NC, NX = 8, 4, 2, 4
ROWS, DH, BLK = 512, 128, 128
HW = 256
DM = 2048
OWN = 512
NB = ROWS // BLK
NEG = -1e30
EPS = 1e-6
F32, BF16 = jnp.float32, jnp.bfloat16
OFFS = (0, -1, 1, 2)
LOADS = ("up", "down", "ig", "fg", "ex", "doc", "k", "v", "q", "cg", "og", "mg", "res", "w")

RIGHT = (0, -1, 2)

ORDER = (
    "begin", "gates", "state", "dz0,0", "wsend", "uz-1", "dy-1", "uz1", "dy1",
    "st0", "y0", "uyz-1", "dz0,-1", "intra0", "uyz1", "do", "dz0,2", "st1",
    "uz-2", "uz2", "uyz2", "intra1", "dz0,1", "cell", "dz-1,0", "ps1", "ufl",
    "ufr", "uz-3", "uz3", "dz-1,2", "wpass", "uyz-3", "uyz3", "dz1,2", "dz-1,-1",
    "dz1,1", "dz-1,1", "dm-1", "uyz-2", "dz1,-1", "outa", "dz1,0", "uz-4", "outb",
    "ps-3", "dz-2,0", "dz2,-1", "dz2,2", "uyz-4", "dz-2,-1", "ps2", "ps3", "dz-2,1",
    "ps-1", "ps0", "ps-2", "dm0", "ffr", "dz2,1", "dz-2,2", "dz2,0", "ps-4",
    "ffl", "um0", "um-1", "um1", "dm2", "dz3,2", "dz3,1", "dm-2", "dz-3,0",
    "dz-3,-1", "um2", "dz3,0", "dz3,-1", "norm", "up0", "dz4,1", "dz4,2", "dm3",
    "dz-3,1", "dz-3,2", "dm1", "dm-3", "up1", "up2", "dz-4,0", "dz-4,-1", "dm4",
    "up3", "down",
)


def across(row):
    return jnp.transpose(jnp.broadcast_to(row, (BLK, BLK)))


def rows_of(values):
    return lax.dot_general(
        jnp.ones((8, BLK), F32), values, (((1,), (1,)), ((), ())),
        precision=lax.Precision.HIGHEST, preferred_element_type=F32,
    )


def kernel(
    ig_h, fg_h, ex_h, doc_h, cg_h, mg_h, q_h, k_h, v_h, og_h, res_h, wout_h, up_h, down_h,
    out,
    ig, fg, ex, doc, cg, mg, q, k, v, og, res, wc, nd, top, stin, auxin,
    u, line1, line1in, full, line2, line2in, normed, wup, wdn, squared, terms, parts,
    lsem, xss, xrs, sts, strs, uss, urs, dss, drs,
):
    z, y, c, x = (lax.axis_index(a) for a in ("z", "y", "c", "x"))
    chip = z * NY + y

    def at_chip(i):
        i = lax.rem(i + NZ * NY, NZ * NY)
        return {"z": i // NY, "y": lax.rem(i, NY)}

    xi = lambda o: lax.rem(x + NX + o, NX)
    yi = lambda o: lax.rem(y + NY + o, NY)
    zi = lambda o: lax.rem(z + NZ + o, NZ)
    xr, xl, yr, yl, zr, zl = ({a: f(o)} for a, f in (("x", xi), ("y", yi), ("z", zi)) for o in (1, -1))
    mate = {"c": 1 - c}
    ahead, behind = at_chip(chip + 1), at_chip(chip - 1)
    sp = chip * NC + c

    own_cols = pl.ds(pl.multiple_of(x * OWN, OWN), OWN)
    sources = dict(
        up=(up_h, wup.at[z, y, c]), down=(down_h, wdn.at[z, y, c]), ig=(ig_h, ig), fg=(fg_h, fg), ex=(ex_h, ex),
        doc=(doc_h, doc), k=(k_h, k), v=(v_h, v), q=(q_h, q), cg=(cg_h, cg), og=(og_h, og), mg=(mg_h, mg),
        res=(res_h, res), w=(wout_h.at[:, own_cols], wc.at[pl.ds(pl.multiple_of(x * HW, HW), HW), :]),
    )
    loads = {}
    for i, name in enumerate(LOADS):
        loads[name] = pltpu.make_async_copy(*sources[name], lsem.at[i])
        loads[name].start()

    barrier = pltpu.get_barrier_semaphore()
    peers = [xr, xl, {"x": xi(2)}, mate, yr, yl, zr, zl, ahead, behind]
    for peer in peers:
        pl.semaphore_signal(barrier, inc=1, device_id=peer, device_id_type=MESH)
    pl.semaphore_wait(barrier, len(peers))

    pools = {"x": [xss, xrs, 0], "s": [sts, strs, 0], "u": [uss, urs, 0], "d": [dss, drs, 0]}
    copies = {}

    def send(pool, name, src, dst, dev):
        p = pools[pool]
        d = pltpu.make_async_remote_copy(
            src_ref=src, dst_ref=dst, send_sem=p[0].at[p[2]], recv_sem=p[1].at[p[2]],
            device_id=dev, device_id_type=MESH,
        )
        p[2] += 1
        d.start()
        copies[name] = d

    def arrived(*names):
        for name in names:
            copies[name].wait_recv()

    got = {}
    steps = {}

    def step(f):
        steps[f.__name__] = f
        return f

    def up_at(zo, yo):
        return wup.at[zi(zo), yi(yo), c]

    def down_at(zo, yo):
        return wdn.at[zi(zo), yi(yo), c]

    @step
    def begin():
        loads["up"].wait()
        loads["down"].wait()
        own, dn = up_at(0, 0), down_at(0, 0)
        send("u", "uz-1", own, own, zr)
        send("u", "uz1", own, own, zl)
        send("d", "dy-1", dn, dn, yr)
        send("d", "dy1", dn, dn, yl)

    def uz(zo):
        arrived("uz%d" % zo)
        ref = up_at(zo, 0)
        if -4 < zo < 0:
            send("u", "uz%d" % (zo - 1), ref, ref, zr)
        elif 0 < zo < 3:
            send("u", "uz%d" % (zo + 1), ref, ref, zl)

    def uyz(zo):
        ref = up_at(zo, 0)
        send("u", "uy%d,-1" % zo, ref, ref, yr)
        send("u", "uy%d,1" % zo, ref, ref, yl)

    def ps(zo):
        side = -1 if zo in RIGHT else 1
        arrived("uy%d,%d" % (zo, side))
        ref = up_at(zo, side)
        send("u", "uo%d" % zo, ref, ref, yr if side < 0 else yl)

    def um(yo):
        if yo in (-1, 1):
            arrived(*("uy%d,%d" % (zo, yo) for zo in range(-4, 4) if (zo in RIGHT) != (yo == -1)))
        elif yo == 2:
            arrived(*("uo%d" % zo for zo in range(-4, 4)))
        ref = wup.at[:, yi(yo), c]
        send("u", "umr%d" % yo, ref, ref, mate)

    def dy(side):
        arrived("dy%d" % side)
        ref = wdn.at[z, yi(side), c, pl.ds(0 if side < 0 else 16, 16)]
        send("d", "do%d" % side, ref, ref, yr if side < 0 else yl)

    @step
    def do():
        arrived("do-1", "do1")

    def dz(zo, yo):
        ref = down_at(zo, yo)
        if zo:
            arrived("dz%d,%d" % (zo, yo))
        for side, dev, last in ((-1, zr, (0, -1)), (1, zl, (1, 2))):
            if zo * side < 0 or abs(zo) == 4 or (abs(zo) == 3 and yo not in last):
                continue
            send("d", "dz%d,%d" % (zo + side, yo), ref, ref, dev)

    def dm(zo):
        ref = wdn.at[zi(zo), :, c]
        send("d", "dmr%d" % zo, ref, ref, mate)

    for zo in range(-4, 4):
        steps["uz%d" % zo] = lambda zo=zo: uz(zo)
        steps["uyz%d" % zo] = lambda zo=zo: uyz(zo)
        steps["ps%d" % zo] = lambda zo=zo: ps(zo)
    steps["y0"] = steps["uyz0"]
    for o in OFFS:
        steps["um%d" % o] = lambda o=o: um(o)
    for side in (-1, 1):
        steps["dy%d" % side] = lambda side=side: dy(side)
    for zo in range(-4, 5):
        steps["dm%d" % zo] = lambda zo=zo: dm(zo)
        for yo in OFFS:
            steps["dz%d,%d" % (zo, yo)] = lambda zo=zo, yo=yo: dz(zo, yo)

    half = pl.multiple_of(c * 128, 128)
    wrows = lambda o: wc.at[pl.ds(pl.multiple_of(xi(o) * HW + half, 128), 128), :]

    @step
    def wsend():
        for r in range(1, NX):
            cols = pl.ds(pl.multiple_of(xi(r) * OWN, OWN), OWN)
            send("x", "w%d" % r, wout_h.at[pl.ds(half, 128), cols], wrows(0), {"x": xi(r)})

    @step
    def wpass():
        for r in range(1, NX):
            arrived("w%d" % r)
            send("x", "wm%d" % r, wrows(-r), wrows(-r), mate)

    ri = lax.broadcasted_iota(jnp.int32, (BLK, BLK), 0)
    ci = lax.broadcasted_iota(jnp.int32, (BLK, BLK), 1)
    scale = DH ** (-0.5)
    block = lambda a: slice(a * BLK, (a + 1) * BLK)
    head = lambda h: slice(h * DH, (h + 1) * DH)

    @step
    def gates():
        for name in ("ig", "fg", "ex", "doc"):
            loads[name].wait()
        f = fg[...]
        lf = jnp.minimum(f, 0.0) - jnp.log1p(jnp.exp(-jnp.abs(f))) + ex[...]
        docs = doc[...].astype(F32)
        dr = [docs[:, block(a)] for a in range(NB)]
        ga = [ig[:, block(a)] for a in range(NB)]
        cum = jnp.dot(
            jnp.concatenate([lf[:, block(a)] for a in range(NB)], axis=0), (ri <= ci).astype(F32),
            precision=lax.Precision.HIGHEST, preferred_element_type=F32,
        )
        cm = [cum[2 * a:2 * a + 2] for a in range(NB)]
        tot = [jnp.broadcast_to(cm[a][:, BLK - 1:BLK], (2, BLK)) for a in range(NB)]

        def between(b, a):
            s = jnp.zeros((2, BLK), F32)
            for i in range(b, a):
                s = s + tot[i]
            return s

        got.update(
            between=between, dr=dr,
            ex=[[ga[b] - cm[b] if a == b else ga[b] + ((tot[b] - cm[b]) + between(b + 1, a))
                 for b in range(min(a + 1, NB))] for a in range(NB + 1)],
            first=jnp.broadcast_to(dr[0][:, 0:1], (1, BLK)), last=jnp.broadcast_to(dr[NB - 1][:, BLK - 1:BLK], (1, BLK)),
        )
        got["dcol"] = [across(d) for d in dr]

    @step
    def state():
        e = got["ex"][NB]
        kept = [jnp.where(got["dr"][b] == got["last"], e[b], NEG) for b in range(NB)]
        peak = jnp.maximum(jnp.maximum(kept[0], kept[1]), jnp.maximum(kept[2], kept[3]))
        peak = jnp.broadcast_to(jnp.max(peak, axis=1, keepdims=True), (2, BLK))
        wt = [jnp.exp(kept[b] - peak) for b in range(NB)]
        wrow = jnp.concatenate(wt, axis=1)
        loads["k"].wait()
        loads["v"].wait()
        for h in range(2):
            kh = k[:, head(h)]
            scaled = jnp.concatenate(
                [v[block(b), head(h)].astype(F32) * across(wt[b][h:h + 1]) for b in range(NB)], axis=0
            ).astype(BF16)
            stin[5, head(h), :] = lax.dot_general(
                kh, scaled, (((0,), (0,)), ((), ())), preferred_element_type=F32
            ).astype(BF16)
            w8 = jnp.broadcast_to(wrow[h:h + 1], (8, ROWS)).astype(BF16)
            auxin[5, 4 + h:5 + h] = jnp.dot(w8, kh, preferred_element_type=F32)[0:1]
        auxin[5, 0:2] = peak
        auxin[5, 2:4] = got["between"](0, NB)
        auxin[5, 6:7] = got["last"]
        auxin[5, 7:8] = got["last"]
        pass_state(5, 0, ahead)
        pass_state(5, 4, mate)

    def pass_state(slot, to, dev):
        send("s", "st%d" % to, stin.at[slot], stin.at[to], dev)
        send("s", "sx%d" % to, auxin.at[slot], auxin.at[to], dev)

    @step
    def st0():
        arrived("st0", "sx0")
        pass_state(0, 1, ahead)
        pass_state(0, 2, mate)

    @step
    def st1():
        arrived("st1", "sx1")
        pass_state(1, 3, mate)

    def intra(h):
        loads["q"].wait() if h == 0 else None
        vx = jnp.concatenate([v[:, head(h)], jnp.ones((ROWS, DH), BF16)], axis=1)
        for a in range(NB):
            n = (a + 1) * BLK
            sc = lax.dot_general(
                q[block(a), head(h)], k[:n, head(h)], (((1,), (1,)), ((), ())), preferred_element_type=F32
            )
            es = []
            for b in range(a + 1):
                ok = got["dcol"][a] == got["dr"][b]
                if b == a:
                    ok = ok & (ci <= ri)
                es.append(jnp.where(ok, got["ex"][a][b][h:h + 1], NEG))
            best = es[0]
            for e in es[1:]:
                best = jnp.maximum(best, e)
            best = jnp.max(best, axis=1, keepdims=True)
            p = jnp.concatenate(
                [(jnp.exp(es[b] - best) * (sc[:, block(b)] * scale)).astype(BF16) for b in range(a + 1)], axis=1
            )
            nd[h, block(a), :] = jnp.dot(p, vx[:n], preferred_element_type=F32)
            top[h, block(a), :] = jnp.broadcast_to(best, (BLK, BLK))

    steps["intra0"] = lambda: intra(0)
    steps["intra1"] = lambda: intra(1)

    ucols = lambda o: pl.ds(pl.multiple_of(xi(o) * HW, HW), HW)
    uview = lambda o, s: u.at[pl.ds(256 * s, 256), ucols(o)]
    fcols = lambda o: pl.ds(pl.multiple_of(xi(o) * OWN, OWN), OWN)
    fview = lambda o, s: full.at[pl.ds(256 * s, 256), fcols(o)]

    @step
    def cell():
        arrived("st2", "sx2", "st3", "sx3", "st4", "sx4")
        gone = jnp.zeros((2, BLK), F32)
        logs, slots = [], (2 + 2 * c, 0, 3 - c, 1)
        for j, s in enumerate(slots):
            live = (auxin[s, 6:7] == got["first"]) & (sp > j)
            logs.append(jnp.where(live, auxin[s, 0:2] + gone, NEG))
            gone = gone + auxin[s, 2:4]
        came = jnp.maximum(jnp.maximum(logs[0], logs[1]), jnp.maximum(logs[2], logs[3]))
        part = [jnp.where(lg > 0.5 * NEG, jnp.exp(lg - came), 0.0) for lg in logs]
        memx = []
        for h in range(2):
            m, n = jnp.zeros((DH, DH), F32), jnp.zeros((1, BLK), F32)
            for g, s in zip(part, slots):
                m = m + g[h:h + 1] * stin[s, head(h), :].astype(F32)
                n = n + g[h:h + 1] * auxin[s, 4 + h:5 + h]
            memx.append(jnp.concatenate([m, across(n)], axis=1).astype(BF16))
        loads["og"].wait()
        loads["cg"].wait()
        gain = cg[...].astype(F32).reshape(1, HW)
        for a in range(NB):
            squares = jnp.zeros((BLK, DH), F32)
            outs = []
            for h in range(2):
                qm = jnp.dot(q[block(a), head(h)], memx[h], preferred_element_type=F32) * scale
                far = jnp.where(got["dcol"][a] == got["first"], (got["between"](0, a) + came)[h:h + 1], NEG)
                near = top[h, block(a), :]
                m = jnp.maximum(near, far)
                wn, wf = jnp.exp(near - m), jnp.exp(far - m)
                num = wn * nd[h, block(a), :DH] + wf * qm[:, :DH]
                den = wn * nd[h, block(a), DH:] + wf * qm[:, DH:]
                val = num / jnp.maximum(jnp.abs(den), 1.0)
                squares = squares + val * val
                gate = jax.nn.sigmoid(og[block(a), head(h)].astype(F32))
                outs.append((gate * val * gain[:, head(h)]).astype(BF16))
            u[block(a), ucols(0)] = jnp.concatenate(outs, axis=1)
            line1[:, block(a)] = rows_of(squares)
        send("x", "ua-", uview(0, 0), uview(0, 0), xr)
        send("x", "ub+", uview(0, 1), uview(0, 1), xl)
        for r in range(1, NX):
            send("x", "l%d" % r, line1, line1in.at[r - 1], {"x": xi(r)})
        send("x", "ub-", uview(0, 1), uview(0, 1), xr)
        send("x", "ua+", uview(0, 0), uview(0, 0), xl)

    @step
    def ufr():
        arrived("ua-")
        send("x", "uar", uview(-1, 0), uview(-1, 0), xr)

    @step
    def ufl():
        arrived("ub+")
        send("x", "ubl", uview(1, 1), uview(1, 1), xl)

    def project_out(s):
        for a in (2 * s, 2 * s + 1):
            ic = across(got["inv1"][0:1, block(a)])
            acc = jnp.dot(u[block(a), :], wc[...], preferred_element_type=F32)
            squares = jnp.zeros((BLK, BLK), F32)
            outs = []
            for b in range(OWN // BLK):
                f = (res[block(a), block(b)].astype(F32) + acc[:, block(b)] * ic).astype(BF16)
                fw = f.astype(F32)
                squares = squares + fw * fw
                outs.append(f)
            full[block(a), fcols(0)] = jnp.concatenate(outs, axis=1)
            line2[:, block(a)] = rows_of(squares)

    @step
    def outa():
        arrived("l1", "l2", "l3")
        total = line1[...] + line1in[0] + line1in[1] + line1in[2]
        got["inv1"] = lax.rsqrt(total / (DH * 8) + EPS)
        loads["w"].wait()
        loads["res"].wait()
        arrived("wm1", "wm2", "wm3", "ub-", "ua+", "uar", "ubl")
        project_out(0)
        send("x", "fa-", fview(0, 0), fview(0, 0), xr)
        send("x", "fa+", fview(0, 0), fview(0, 0), xl)

    @step
    def outb():
        project_out(1)
        loads["mg"].wait()
        line2[1:2, :] = mg[...].astype(F32).reshape(1, OWN)
        for r in range(1, NX):
            send("x", "m%d" % r, line2, line2in.at[r - 1], {"x": xi(r)})
        send("x", "fb-", fview(0, 1), fview(0, 1), xr)
        send("x", "fb+", fview(0, 1), fview(0, 1), xl)

    @step
    def ffr():
        arrived("fa-")
        send("x", "far", fview(-1, 0), fview(-1, 0), xr)

    @step
    def ffl():
        arrived("fb+")
        send("x", "fbl", fview(1, 1), fview(1, 1), xl)

    @step
    def norm():
        arrived("m1", "m2", "m3")
        total = line2[...] + line2in[0] + line2in[1] + line2in[2]
        inv = lax.rsqrt(total / DM + EPS)
        arrived("fb-", "fa+", "far", "fbl")
        icol = [across(inv[0:1, block(a)]) for a in range(NB)]
        for r in range(NX):
            gain = line2[1:2, :] if r == 0 else line2in[r - 1, 1:2, :]
            for a in range(NB):
                fw = full[block(a), fcols(-r)].astype(F32)
                normed[block(a), fcols(-r)] = jnp.concatenate(
                    [(fw[:, block(b)] * icol[a] * gain[:, block(b)]).astype(BF16) for b in range(OWN // BLK)], axis=1
                )

    def up(t):
        if t == 0:
            arrived("umr0", "umr-1", "umr1", "umr2")
        cols = slice(t * 512, (t + 1) * 512)
        hid = jnp.dot(normed[...], wup[:, :, :, :, cols].reshape(DM, 512), preferred_element_type=F32)
        hid = jnp.maximum(hid, 0.0)
        squared[:, cols] = (hid * hid).astype(BF16)

    for t in range(4):
        steps["up%d" % t] = lambda t=t: up(t)

    @step
    def down():
        arrived(*("dmr%d" % zo for zo in range(-3, 5)))

        def project(r):
            w = wdn[pl.ds(2 * xi(r), 2)].reshape(OWN, DM)
            return lax.dot_general(squared[...], w, (((1,), (1,)), ((), ())), preferred_element_type=F32)

        a, b = slice(0, 256), slice(256, 512)
        terms[2] = project(2).astype(BF16)
        send("x", "p0", terms.at[2, a], parts.at[0], xr)
        send("x", "p1", terms.at[2, b], parts.at[1], xl)
        terms[1] = project(1).astype(BF16)
        send("x", "p2", terms.at[1, b], parts.at[2], xr)
        terms[3] = project(3).astype(BF16)
        send("x", "p3", terms.at[3, a], parts.at[3], xl)
        arrived("p0")
        terms[1, a] = (terms[1, a].astype(F32) + parts[0].astype(F32)).astype(BF16)
        send("x", "p4", terms.at[1, a], parts.at[4], xr)
        arrived("p1")
        terms[3, b] = (terms[3, b].astype(F32) + parts[1].astype(F32)).astype(BF16)
        send("x", "p5", terms.at[3, b], parts.at[5], xl)
        mine = project(0) + full[:, fcols(0)].astype(F32)
        arrived("p2", "p3", "p4", "p5")
        out[a] = (mine[a] + parts[3].astype(F32) + parts[4].astype(F32)).astype(BF16)
        out[b] = (mine[b] + parts[2].astype(F32) + parts[5].astype(F32)).astype(BF16)

    for name in ORDER:
        steps[name]()
    for d in copies.values():
        d.wait_send()


def layer(*arrays):
    dma = pltpu.SemaphoreType.DMA
    return pl.pallas_call(
        kernel,
        out_shape=jax.ShapeDtypeStruct((ROWS, OWN), BF16),
        in_specs=[pl.BlockSpec(memory_space=pltpu.HBM)] * len(arrays),
        out_specs=pl.BlockSpec(memory_space=pltpu.VMEM),
        scratch_shapes=[
            *[pltpu.VMEM(a.shape, a.dtype) for a in arrays[:11]],
            pltpu.VMEM((4 * HW, OWN), BF16),
            pltpu.VMEM((2, ROWS, 2 * DH), F32),
            pltpu.VMEM((2, ROWS, DH), F32),
            pltpu.VMEM((6, 2 * DH, DH), BF16),
            pltpu.VMEM((6, 8, BLK), F32),
            pltpu.VMEM((ROWS, 4 * HW), BF16),
            pltpu.VMEM((8, ROWS), F32),
            pltpu.VMEM((3, 8, ROWS), F32),
            pltpu.VMEM((ROWS, DM), BF16),
            pltpu.VMEM((8, ROWS), F32),
            pltpu.VMEM((3, 8, ROWS), F32),
            pltpu.VMEM((ROWS, DM), BF16),
            pltpu.VMEM((NZ, NY, NC, 32, DM), BF16),
            pltpu.VMEM((NZ, NY, NC, 32, DM), BF16),
            pltpu.VMEM((ROWS, DM), BF16),
            pltpu.VMEM((4, ROWS, OWN), BF16),
            pltpu.VMEM((6, ROWS // 2, OWN), BF16),
            dma((len(LOADS),)), dma((30,)), dma((30,)), dma((10,)), dma((10,)), dma((35,)), dma((35,)),
            dma((40,)), dma((40,)),
        ],
        compiler_params=pltpu.CompilerParams(
            collective_id=0, has_side_effects=True, vmem_limit_bytes=62 * 2**20
        ),
    )(*arrays)


def local(
    queries, keys, values, output_gate_logits, input_gate_log, forget_gate_logits, extra_decay_log,
    document, residual, cell_norm_gain, output_weight, mixer_norm_gain, up_weight, down_weight,
):
    return layer(
        input_gate_log.T, forget_gate_logits.T, extra_decay_log.T, document.reshape(1, ROWS),
        cell_norm_gain, mixer_norm_gain,
        queries, keys, values, output_gate_logits, residual, output_weight, up_weight, down_weight.T,
    )


def solution(mesh):
    split = Mesh(mesh.devices.reshape(NZ, NY, NC, NX), ("z", "y", "c", "x"))
    rows, heads = P(SP, "x"), P("x")
    return jax.shard_map(
        local,
        mesh=split,
        in_specs=(
            rows, rows, rows, rows, rows, rows, rows, P(SP), rows, heads, P("x", None), heads, rows, P("x", SP),
        ),
        out_specs=rows,
        check_vma=False,
    )
```

```python
import jax
import jax.numpy as jnp
from jax import lax
from jax.experimental import pallas as pl
from jax.experimental.pallas import tpu as pltpu
from jax.sharding import Mesh
from jax.sharding import PartitionSpec as P

MESH = pl.DeviceIdType.MESH
SP = ("z", "y", "c")
NZ, NY, NC, NX = 8, 4, 2, 4
ROWS, DH, BLK = 512, 128, 128
HW = 256
DM = 2048
OWN = 512
NB = ROWS // BLK
NEG = -1e30
EPS = 1e-6
F32, BF16 = jnp.float32, jnp.bfloat16
OFFS = (0, -1, 1, 2)
LOADS = ("up", "down", "ig", "fg", "ex", "doc", "k", "v", "q", "cg", "og", "mg", "res", "w")

RIGHT = {"U": (0, -2, 2), "D": (0, -2, 2, -4)}

ORDER = (
    "tell", "begin", "Udy", "Uz0", "Dz0", "Ddy", "Uyz0", "Udz0,0", "intra0",
    "wsend", "intra1", "Uz-1", "Uyz-1", "Uz1", "Dz-1", "Ddo", "Dz1", "Dyz-1",
    "gsend", "st0", "Udz1,0", "Udz0,1", "Uz-2", "Udo", "Udz-1,0", "Uyz-2", "Uz2",
    "Dyz0", "st1", "Dz-2", "Dz2", "Uyz2", "Udz0,-1", "Dyz-2", "comb", "cell0",
    "Ups0", "Uyz1", "Uz-3", "cell1", "Udz1,1", "wpass", "Udz2,0", "Uz3", "Uyz3",
    "Udz-1,1", "Uyz-3", "Udz0,2", "Dz3", "Dz-3", "Udm0", "Udz-1,-1", "Udz1,-1", "Dyz2",
    "Udz-2,0", "ur0", "ul0", "Uz-4", "Uyz-4", "Um0", "Dyz1", "Udz2,1", "Dyz-3",
    "Dyz3", "Udz3,0", "Ups2", "Dps-1", "Ups3", "Udz1,2", "Ups-3", "Udz-1,2", "Udz-2,1",
    "ur1", "Ddz0,1", "Ups-1", "Ups1", "ul1", "Ups-2", "Udm-1", "Udm1", "Dps-2",
    "out0", "Ddz0,0", "Ups-4", "Udz2,-1", "Udz-2,-1", "Dz-4", "Dm0", "Ddz0,-1", "Udz2,2",
    "Ddz0,2", "Udm2", "Dyz-4", "Udz-3,0", "Udz3,1", "Um1", "Dps0", "Ddm0", "Dps1",
    "Ddz1,1", "Udz-2,2", "Dps-3", "out1", "Dps2", "Um-1", "Udm-2", "Udz-3,1", "Udz3,-1",
    "Dps3", "Ddz1,0", "Udz-3,-1", "Ddz-1,0", "fl0", "Udz3,2", "Ddz-1,-1", "Ddz1,2", "Ddz1,-1",
    "fr0", "Ddm1", "Udm3", "Ddz-1,2", "Ddz2,1", "Ddz-1,1", "fl1", "Ddm-1", "Udz4,1",
    "Udz-4,0", "Um2", "fr1", "Udz-3,2", "Udm-3", "Ddz2,0", "Udz-4,-1", "Udz4,2", "Udm4",
    "Dps-4", "Dm-1", "norm0", "Ddz-2,0", "Ddz2,2", "up0,0", "Dm1", "Ddz-2,-1", "Ddz2,-1",
    "up0,1", "Ddm2", "up0,2", "Ddz-2,2", "Ddz3,1", "norm1", "Dm2", "up0,3", "up1,0",
    "Ddz-2,1", "Ddm-2", "up1,1", "s0,0", "Ddz3,2", "up1,2", "Ddz-3,0", "s0,1", "up1,3",
    "Ddz-3,-1", "s1,0", "Ddz-3,2", "Ddz3,-1", "Ddz3,0", "Ddm3", "Ddz-3,1", "Ddm-3", "Ddz4,1",
    "s1,1", "Ddz4,2", "j0,0", "s0,2", "Ddz-4,-1", "Ddz-4,0", "Ddm4", "s1,2", "s0,3",
    "s1,3", "j1,1", "j0,1", "j1,0", "j0,2", "j1,2", "j0,3", "j1,3", "fin0",
    "fin1",
)


def across(row):
    return jnp.transpose(jnp.broadcast_to(row, (BLK, BLK)))


def rows_of(values):
    return lax.dot_general(
        jnp.ones((8, BLK), F32), values, (((1,), (1,)), ((), ())),
        precision=lax.Precision.HIGHEST, preferred_element_type=F32,
    )


def kernel(
    ig_h, fg_h, ex_h, doc_h, cg_h, mg_h, q_h, k_h, v_h, og_h, res_h, wout_h, up_h, down_h,
    out,
    ig, fg, ex, doc, cg, mg, q, k, v, og, res, wc, nd, top, stin, auxin,
    u, line1, line1in, full, line2, line2in, gains, normed, wup, wdn, squared, terms, parts,
    lsem, xss, xrs, sts, strs, uss, urs, dss, drs, pss, prs,
):
    z, y, c, x = (lax.axis_index(a) for a in ("z", "y", "c", "x"))
    chip = z * NY + y

    def at_chip(i):
        i = lax.rem(i + NZ * NY, NZ * NY)
        return {"z": i // NY, "y": lax.rem(i, NY)}

    xi = lambda o: lax.rem(x + NX + o, NX)
    yi = lambda o: lax.rem(y + NY + o, NY)
    zi = lambda o: lax.rem(z + NZ + o, NZ)
    xr, xl, yr, yl, zr, zl = ({a: f(o)} for a, f in (("x", xi), ("y", yi), ("z", zi)) for o in (1, -1))
    mate = {"c": 1 - c}
    ahead, behind, two_ahead, two_behind = (at_chip(chip + o) for o in (1, -1, 2, -2))
    sp = chip * NC + c

    own_cols = pl.ds(pl.multiple_of(x * OWN, OWN), OWN)
    sources = dict(
        up=(up_h, wup.at[z, y, c]), down=(down_h, wdn.at[z, y, c]), ig=(ig_h, ig), fg=(fg_h, fg), ex=(ex_h, ex),
        doc=(doc_h, doc), k=(k_h, k), v=(v_h, v), q=(q_h, q), cg=(cg_h, cg), og=(og_h, og), mg=(mg_h, mg),
        res=(res_h, res), w=(wout_h.at[:, own_cols], wc.at[pl.ds(pl.multiple_of(x * HW, HW), HW), :]),
    )
    loads = {}
    for i, name in enumerate(LOADS):
        loads[name] = pltpu.make_async_copy(*sources[name], lsem.at[i])
        loads[name].start()

    barrier = pltpu.get_barrier_semaphore()
    peers = [xr, xl, {"x": xi(2)}, mate, yr, yl, zr, zl, ahead, behind, two_ahead, two_behind]
    for peer in peers:
        pl.semaphore_signal(barrier, inc=1, device_id=peer, device_id_type=MESH)
    pools = {"x": [xss, xrs, 0], "s": [sts, strs, 0], "u": [uss, urs, 0], "d": [dss, drs, 0]}
    copies = {}

    def send(pool, name, src, dst, dev):
        p = pools[pool]
        d = pltpu.make_async_remote_copy(
            src_ref=src, dst_ref=dst, send_sem=p[0].at[p[2]], recv_sem=p[1].at[p[2]],
            device_id=dev, device_id_type=MESH,
        )
        p[2] += 1
        d.start()
        copies[name] = d

    def arrived(*names):
        for name in names:
            copies[name].wait_recv()

    got = {}
    steps = {}

    def step(f):
        steps[f.__name__] = f
        return f

    @step
    def begin():
        loads["up"].wait()
        loads["down"].wait()

    def weight(w, pool, buf):
        lo, hi = pl.ds(0, 16), pl.ds(16, 16)
        at_lo = lambda zo, yo: buf.at[zi(zo), yi(yo), c, lo]
        at_hi = lambda zo, yo: buf.at[zi(zo), yi(yo), c, hi]

        def put(name, ref, dev):
            send(pool, w + name, ref, ref, dev)

        def come(*names):
            arrived(*(w + name for name in names))

        def along_z(zo):
            if zo:
                come("z%d" % zo)
            if -4 < zo <= 0:
                put("z%d" % (zo - 1), at_lo(zo, 0), zr)
            if 0 <= zo < 3:
                put("z%d" % (zo + 1), at_lo(zo, 0), zl)

        def along_y(zo):
            put("y%d,-1" % zo, at_lo(zo, 0), yr)
            put("y%d,1" % zo, at_lo(zo, 0), yl)

        def opposite(zo):
            side = -1 if zo in RIGHT[w] else 1
            come("y%d,%d" % (zo, side))
            put("o%d" % zo, at_lo(zo, side), yr if side < 0 else yl)

        def hand_y(yo):
            if yo in (-1, 1):
                come(*("y%d,%d" % (zo, yo) for zo in range(-4, 4) if (zo in RIGHT[w]) != (yo == -1)))
            elif yo == 2:
                come(*("o%d" % zo for zo in range(-4, 4)))
            put("mr%d" % yo, buf.at[:, yi(yo), c, lo], mate)

        def first_y():
            put("dy-1", at_hi(0, 0), yr)
            put("dy1", at_hi(0, 0), yl)

        over = -1 if w == "U" else 1

        def second_y():
            come("dy%d" % over)
            put("do", at_hi(0, over), yr if over < 0 else yl)

        def then_z(zo, yo):
            if zo:
                come("dz%d,%d" % (zo, yo))
            elif yo == -over:
                come("dy%d" % yo)
            elif yo == 2:
                come("do")
            for side, dev, last in ((-1, zr, (0, -1)), (1, zl, (1, 2))):
                if zo * side < 0 or abs(zo) == 4 or (abs(zo) == 3 and yo not in last):
                    continue
                put("dz%d,%d" % (zo + side, yo), at_hi(zo, yo), dev)

        def hand_z(zo):
            put("dmr%d" % zo, buf.at[zi(zo), :, c, hi], mate)

        for zo in range(-4, 4):
            steps[w + "z%d" % zo] = lambda zo=zo: along_z(zo)
            steps[w + "yz%d" % zo] = lambda zo=zo: along_y(zo)
            steps[w + "ps%d" % zo] = lambda zo=zo: opposite(zo)
        for o in OFFS:
            steps[w + "m%d" % o] = lambda o=o: hand_y(o)
        steps[w + "dy"] = first_y
        steps[w + "do"] = second_y
        for zo in range(-4, 5):
            steps[w + "dm%d" % zo] = lambda zo=zo: hand_z(zo)
            for yo in OFFS:
                steps[w + "dz%d,%d" % (zo, yo)] = lambda zo=zo, yo=yo: then_z(zo, yo)

    weight("U", "u", wup)
    weight("D", "d", wdn)

    @step
    def gsend():
        loads["mg"].wait()
        gains[0] = jnp.broadcast_to(mg[...].astype(F32).reshape(1, OWN), (8, OWN))
        for r in range(1, NX):
            send("x", "g%d" % r, gains.at[0], gains.at[r], {"x": xi(r)})

    half = pl.multiple_of(c * 128, 128)
    wrows = lambda o: wc.at[pl.ds(pl.multiple_of(xi(o) * HW + half, 128), 128), :]

    @step
    def wsend():
        for r in range(1, NX):
            cols = pl.ds(pl.multiple_of(xi(r) * OWN, OWN), OWN)
            send("x", "w%d" % r, wout_h.at[pl.ds(half, 128), cols], wrows(0), {"x": xi(r)})

    @step
    def wpass():
        for r in range(1, NX):
            arrived("w%d" % r)
            send("x", "wm%d" % r, wrows(-r), wrows(-r), mate)

    ri = lax.broadcasted_iota(jnp.int32, (BLK, BLK), 0)
    ci = lax.broadcasted_iota(jnp.int32, (BLK, BLK), 1)
    scale = DH ** (-0.5)
    block = lambda a: slice(a * BLK, (a + 1) * BLK)
    head = lambda h: slice(h * DH, (h + 1) * DH)

    @step
    def gates():
        for name in ("ig", "fg", "ex", "doc"):
            loads[name].wait()
        f = fg[...]
        lf = jnp.minimum(f, 0.0) - jnp.log1p(jnp.exp(-jnp.abs(f))) + ex[...]
        docs = doc[...].astype(F32)
        dr = [docs[:, block(a)] for a in range(NB)]
        ga = [ig[:, block(a)] for a in range(NB)]
        cum = jnp.dot(
            jnp.concatenate([lf[:, block(a)] for a in range(NB)], axis=0), (ri <= ci).astype(F32),
            precision=lax.Precision.HIGHEST, preferred_element_type=F32,
        )
        cm = [cum[2 * a:2 * a + 2] for a in range(NB)]
        tot = [jnp.broadcast_to(cm[a][:, BLK - 1:BLK], (2, BLK)) for a in range(NB)]

        def between(b, a):
            s = jnp.zeros((2, BLK), F32)
            for i in range(b, a):
                s = s + tot[i]
            return s

        got.update(
            between=between, dr=dr,
            ex=[[ga[b] - cm[b] if a == b else ga[b] + ((tot[b] - cm[b]) + between(b + 1, a))
                 for b in range(min(a + 1, NB))] for a in range(NB + 1)],
            first=jnp.broadcast_to(dr[0][:, 0:1], (1, BLK)), last=jnp.broadcast_to(dr[NB - 1][:, BLK - 1:BLK], (1, BLK)),
        )
        got["dcol"] = [across(d) for d in dr]

    @step
    def state():
        e = got["ex"][NB]
        kept = [jnp.where(got["dr"][b] == got["last"], e[b], NEG) for b in range(NB)]
        peak = jnp.maximum(jnp.maximum(kept[0], kept[1]), jnp.maximum(kept[2], kept[3]))
        peak = jnp.broadcast_to(jnp.max(peak, axis=1, keepdims=True), (2, BLK))
        wt = [jnp.exp(kept[b] - peak) for b in range(NB)]
        wrow = jnp.concatenate(wt, axis=1)
        loads["k"].wait()
        loads["v"].wait()
        for h in range(2):
            kh = k[:, head(h)]
            scaled = jnp.concatenate(
                [v[block(b), head(h)].astype(F32) * across(wt[b][h:h + 1]) for b in range(NB)], axis=0
            ).astype(BF16)
            stin[5, head(h), :] = lax.dot_general(
                kh, scaled, (((0,), (0,)), ((), ())), preferred_element_type=F32
            ).astype(BF16)
            w8 = jnp.broadcast_to(wrow[h:h + 1], (8, ROWS)).astype(BF16)
            auxin[5, 4 + h:5 + h] = jnp.dot(w8, kh, preferred_element_type=F32)[0:1]
        auxin[5, 0:2] = peak
        auxin[5, 2:4] = got["between"](0, NB)
        auxin[5, 6:7] = got["last"]
        auxin[5, 7:8] = got["last"]

    @step
    def tell():
        pass_state(5, 0, ahead)
        pass_state(5, 1, two_ahead)
        pass_state(5, 4, mate)

    def pass_state(slot, to, dev):
        send("s", "st%d" % to, stin.at[slot], stin.at[to], dev)
        send("s", "sx%d" % to, auxin.at[slot], auxin.at[to], dev)

    @step
    def st0():
        arrived("st0", "sx0")
        pass_state(0, 2, mate)

    @step
    def st1():
        arrived("st1", "sx1")
        pass_state(1, 3, mate)

    def intra(h):
        if loads["q"] is not None:
            loads["q"].wait()
            loads["q"] = None
        vx = jnp.concatenate([v[:, head(h)], jnp.ones((ROWS, DH), BF16)], axis=1)
        for a in range(NB):
            n = (a + 1) * BLK
            sc = lax.dot_general(
                q[block(a), head(h)], k[:n, head(h)], (((1,), (1,)), ((), ())), preferred_element_type=F32
            )
            es = []
            for b in range(a + 1):
                ok = got["dcol"][a] == got["dr"][b]
                if b == a:
                    ok = ok & (ci <= ri)
                es.append(jnp.where(ok, got["ex"][a][b][h:h + 1], NEG))
            best = es[0]
            for e in es[1:]:
                best = jnp.maximum(best, e)
            best = jnp.max(best, axis=1, keepdims=True)
            p = jnp.concatenate(
                [(jnp.exp(es[b] - best) * (sc[:, block(b)] * scale)).astype(BF16) for b in range(a + 1)], axis=1
            )
            nd[h, block(a), :] = jnp.dot(p, vx[:n], preferred_element_type=F32)
            top[h, block(a), :] = jnp.broadcast_to(best, (BLK, BLK))

    steps["intra0"] = lambda: intra(0)
    steps["intra1"] = lambda: intra(1)

    ucols = lambda o: pl.ds(pl.multiple_of(xi(o) * HW, HW), HW)
    def uview(o, s, part=None):
        rows = pl.ds(256 * s, 256) if part is None else pl.ds(256 * s + 128 * part, 128)
        return u.at[rows, ucols(o)]

    fcols = lambda o: pl.ds(pl.multiple_of(xi(o) * OWN, OWN), OWN)

    def fview(o, s, part=None):
        rows = pl.ds(256 * s, 256) if part is None else pl.ds(256 * s + 128 * part, 128)
        return full.at[rows, fcols(o)]

    def spread(view, tag, s):
        send("x", tag + "%d-" % s, view(0, s), view(0, s), xr)
        send("x", tag + "%d+" % s, view(0, s), view(0, s), xl)

    def onward(view, tag, s, side):
        if side < 0:
            arrived(tag + "%d-" % s)
            send("x", tag + "%dr" % s, view(-1, s, 0), view(-1, s, 0), xr)
        else:
            arrived(tag + "%d+" % s)
            send("x", tag + "%dl" % s, view(1, s, 1), view(1, s, 1), xl)

    for s in (0, 1):
        steps["ur%d" % s] = lambda s=s: onward(uview, "u", s, -1)
        steps["ul%d" % s] = lambda s=s: onward(uview, "u", s, 1)
        steps["fr%d" % s] = lambda s=s: onward(fview, "f", s, -1)
        steps["fl%d" % s] = lambda s=s: onward(fview, "f", s, 1)

    @step
    def comb():
        arrived("st2", "sx2", "st3", "sx3", "st4", "sx4")
        gone = jnp.zeros((2, BLK), F32)
        logs, slots = [], (2 + 2 * c, 0, 3 - c, 1)
        for j, s in enumerate(slots):
            live = (auxin[s, 6:7] == got["first"]) & (sp > j)
            logs.append(jnp.where(live, auxin[s, 0:2] + gone, NEG))
            gone = gone + auxin[s, 2:4]
        came = jnp.maximum(jnp.maximum(logs[0], logs[1]), jnp.maximum(logs[2], logs[3]))
        part = [jnp.where(lg > 0.5 * NEG, jnp.exp(lg - came), 0.0) for lg in logs]
        memx = []
        for h in range(2):
            m, n = jnp.zeros((DH, DH), F32), jnp.zeros((1, BLK), F32)
            for g, s in zip(part, slots):
                m = m + g[h:h + 1] * stin[s, head(h), :].astype(F32)
                n = n + g[h:h + 1] * auxin[s, 4 + h:5 + h]
            memx.append(jnp.concatenate([m, across(n)], axis=1).astype(BF16))
        loads["og"].wait()
        loads["cg"].wait()
        got.update(memx=memx, came=came, gain=cg[...].astype(F32).reshape(1, HW))

    def cell(s):
        memx, came, gain = got["memx"], got["came"], got["gain"]
        for a in (2 * s, 2 * s + 1):
            squares = jnp.zeros((BLK, DH), F32)
            outs = []
            for h in range(2):
                qm = jnp.dot(q[block(a), head(h)], memx[h], preferred_element_type=F32) * scale
                far = jnp.where(got["dcol"][a] == got["first"], (got["between"](0, a) + came)[h:h + 1], NEG)
                near = top[h, block(a), :]
                m = jnp.maximum(near, far)
                wn, wf = jnp.exp(near - m), jnp.exp(far - m)
                num = wn * nd[h, block(a), :DH] + wf * qm[:, :DH]
                den = wn * nd[h, block(a), DH:] + wf * qm[:, DH:]
                val = num / jnp.maximum(jnp.abs(den), 1.0)
                squares = squares + val * val
                gate = jax.nn.sigmoid(og[block(a), head(h)].astype(F32))
                outs.append((gate * val * gain[:, head(h)]).astype(BF16))
            u[block(a), ucols(0)] = jnp.concatenate(outs, axis=1)
            line1[:, block(a)] = rows_of(squares)
        cols = slice(256 * s, 256 * s + 256)
        spread(uview, "u", s)
        for r in range(1, NX):
            send("x", "l%d,%d" % (s, r), line1.at[:, cols], line1in.at[r - 1, :, cols], {"x": xi(r)})

    steps["cell0"] = lambda: cell(0)
    steps["cell1"] = lambda: cell(1)

    def head_out(s):
        arrived(*("l%d,%d" % (s, r) for r in range(1, NX)))
        cols = slice(256 * s, 256 * s + 256)
        total = line1[:, cols] + line1in[0, :, cols] + line1in[1, :, cols] + line1in[2, :, cols]
        inv = lax.rsqrt(total / (DH * 8) + EPS)
        if s == 0:
            loads["w"].wait()
            loads["res"].wait()
            arrived("wm1", "wm2", "wm3")
        arrived("u%dr" % s, "u%dl" % s)
        for a in (2 * s, 2 * s + 1):
            ic = across(inv[0:1, block(a - 2 * s)])
            acc = jnp.dot(u[block(a), :], wc[...], preferred_element_type=F32)
            squares = jnp.zeros((BLK, BLK), F32)
            outs = []
            for b in range(OWN // BLK):
                f = (res[block(a), block(b)].astype(F32) + acc[:, block(b)] * ic).astype(BF16)
                fw = f.astype(F32)
                squares = squares + fw * fw
                outs.append(f)
            full[block(a), fcols(0)] = jnp.concatenate(outs, axis=1)
            line2[:, block(a)] = rows_of(squares)

        spread(fview, "f", s)
        for r in range(1, NX):
            send("x", "m%d,%d" % (s, r), line2.at[:, cols], line2in.at[r - 1, :, cols], {"x": xi(r)})

    steps["out0"] = lambda: head_out(0)
    steps["out1"] = lambda: head_out(1)

    def norm(s):
        arrived(*("m%d,%d" % (s, r) for r in range(1, NX)))
        cols = slice(256 * s, 256 * s + 256)
        total = line2[:, cols] + line2in[0, :, cols] + line2in[1, :, cols] + line2in[2, :, cols]
        inv = lax.rsqrt(total / DM + EPS)
        if s == 0:
            arrived("g1", "g2", "g3")
        arrived("f%dr" % s, "f%dl" % s)
        for a in (2 * s, 2 * s + 1):
            ic = across(inv[0:1, block(a - 2 * s)])
            for r in range(NX):
                fw = full[block(a), fcols(-r)].astype(F32)
                gain = gains[0, 0:1] if r == 0 else gains[r, 0:1]
                normed[block(a), fcols(-r)] = jnp.concatenate(
                    [(fw[:, block(b)] * ic * gain[:, block(b)]).astype(BF16) for b in range(OWN // BLK)], axis=1
                )

    steps["norm0"] = lambda: norm(0)
    steps["norm1"] = lambda: norm(1)

    def up(s, t):
        if s == t == 0:
            arrived(*("Umr%d" % o for o in OFFS), *("Udmr%d" % zo for zo in range(-3, 5)))
        rows, cols = slice(256 * s, 256 * s + 256), slice(t * 512, (t + 1) * 512)
        hid = jnp.dot(normed[rows, :], wup[:, :, :, :, cols].reshape(DM, 512), preferred_element_type=F32)
        hid = jnp.maximum(hid, 0.0)
        squared[rows, cols] = (hid * hid).astype(BF16)

    for t in range(4):
        steps["up0,%d" % t] = lambda t=t: up(0, t)
        steps["up1,%d" % t] = lambda t=t: up(1, t)

    zb = lax.rem(z, 2)
    owner = [lax.rem(z // 2 + d + NX, NX) for d in (0, 2 * zb - 1, 1 - 2 * zb, 2)]
    ahead_by = [lax.rem(o - x + NX, NX) for o in owner]
    ways = ((0, xr), (1, xl), (1, xr), (0, xl), (0, xr), (1, xl))
    quarter = lambda s, h: slice(256 * s + 128 * h, 256 * s + 128 * h + 128)

    def part(s, i, k):
        h, dev = ways[i]
        return pltpu.make_async_remote_copy(
            src_ref=terms.at[k, quarter(s, h)], dst_ref=parts.at[s, i], send_sem=pss.at[6 * s + i],
            recv_sem=prs.at[6 * s + i], device_id=dev, device_id_type=MESH,
        )

    def stage(s, k):
        if s == 0:
            if k == 0:
                arrived(*("Dmr%d" % o for o in OFFS))
            arrived(*("Ddmr%d" % zo for zo in ((0, 1, -1), (2, -2), (3, -3), (4,))[k]))
        w = wdn[pl.ds(2 * owner[k], 2)].reshape(OWN, DM)
        rows = slice(256 * s, 256 * s + 256)
        terms[k, rows] = lax.dot_general(
            squared[rows, :], w, (((1,), (1,)), ((), ())), preferred_element_type=F32
        ).astype(BF16)

        @pl.when(ahead_by[k] == 2)
        def _():
            part(s, 0, k).start()
            part(s, 1, k).start()

        @pl.when(ahead_by[k] == 1)
        def _():
            part(s, 2, k).start()

        @pl.when(ahead_by[k] == 3)
        def _():
            part(s, 3, k).start()

    def join(s, k):
        for side, h, i in ((1, 0, 0), (3, 1, 1)):
            @pl.when(ahead_by[k] == side)
            def _():
                part(s, i, 0).wait_recv()
                rows = quarter(s, h)
                terms[k, rows] = (terms[k, rows].astype(F32) + parts[s, i].astype(F32)).astype(BF16)
                part(s, i + 4, k).start()

    def final(s):
        d = lax.rem(x - z // 2 + NX, NX)
        d = lax.rem(d * (2 * zb - 1) + NX, NX)
        mine = terms.at[d + d // 2 - 2 * (d // 3)]
        for h, i, n in ((0, 3, 4), (1, 2, 5)):
            part(s, i, 0).wait_recv()
            part(s, n, 0).wait_recv()
            rows = quarter(s, h)
            out[rows] = (
                full[rows, fcols(0)].astype(F32) + mine[rows].astype(F32)
                + parts[s, i].astype(F32) + parts[s, n].astype(F32)
            ).astype(BF16)
        for i in range(6):
            part(s, i, 0).wait_send()

    for s in (0, 1):
        for n in range(4):
            steps["s%d,%d" % (s, n)] = lambda s=s, n=n: stage(s, n)
            steps["j%d,%d" % (s, n)] = lambda s=s, n=n: join(s, n)
        steps["fin%d" % s] = lambda s=s: final(s)

    steps["gates"]()
    steps["state"]()
    pl.semaphore_wait(barrier, len(peers))
    for name in ORDER:
        steps[name]()
    for d in copies.values():
        d.wait_send()


def layer(*arrays):
    dma = pltpu.SemaphoreType.DMA
    return pl.pallas_call(
        kernel,
        out_shape=jax.ShapeDtypeStruct((ROWS, OWN), BF16),
        in_specs=[pl.BlockSpec(memory_space=pltpu.HBM)] * len(arrays),
        out_specs=pl.BlockSpec(memory_space=pltpu.VMEM),
        scratch_shapes=[
            *[pltpu.VMEM(a.shape, a.dtype) for a in arrays[:11]],
            pltpu.VMEM((4 * HW, OWN), BF16),
            pltpu.VMEM((2, ROWS, 2 * DH), F32),
            pltpu.VMEM((2, ROWS, DH), F32),
            pltpu.VMEM((6, 2 * DH, DH), BF16),
            pltpu.VMEM((6, 8, BLK), F32),
            pltpu.VMEM((ROWS, 4 * HW), BF16),
            pltpu.VMEM((8, ROWS), F32),
            pltpu.VMEM((3, 8, ROWS), F32),
            pltpu.VMEM((ROWS, DM), BF16),
            pltpu.VMEM((8, ROWS), F32),
            pltpu.VMEM((3, 8, ROWS), F32),
            pltpu.VMEM((4, 8, OWN), F32),
            pltpu.VMEM((ROWS, DM), BF16),
            pltpu.VMEM((NZ, NY, NC, 32, DM), BF16),
            pltpu.VMEM((NZ, NY, NC, 32, DM), BF16),
            pltpu.VMEM((ROWS, DM), BF16),
            pltpu.VMEM((4, ROWS, OWN), BF16),
            pltpu.VMEM((2, 6, ROWS // 4, OWN), BF16),
            dma((len(LOADS),)), dma((37,)), dma((37,)), dma((10,)), dma((10,)), dma((75,)), dma((75,)),
            dma((75,)), dma((75,)), dma((12,)), dma((12,)),
        ],
        compiler_params=pltpu.CompilerParams(
            collective_id=0, has_side_effects=True, vmem_limit_bytes=62 * 2**20
        ),
    )(*arrays)


def local(
    queries, keys, values, output_gate_logits, input_gate_log, forget_gate_logits, extra_decay_log,
    document, residual, cell_norm_gain, output_weight, mixer_norm_gain, up_weight, down_weight,
):
    return layer(
        input_gate_log.T, forget_gate_logits.T, extra_decay_log.T, document.reshape(1, ROWS),
        cell_norm_gain, mixer_norm_gain,
        queries, keys, values, output_gate_logits, residual, output_weight, up_weight, down_weight.T,
    )


def solution(mesh):
    split = Mesh(mesh.devices.reshape(NZ, NY, NC, NX), ("z", "y", "c", "x"))
    rows, heads = P(SP, "x"), P("x")
    return jax.shard_map(
        local,
        mesh=split,
        in_specs=(
            rows, rows, rows, rows, rows, rows, rows, P(SP), rows, heads, P("x", None), heads, rows, P("x", SP),
        ),
        out_specs=rows,
        check_vma=False,
    )
```

```python
import jax
import jax.numpy as jnp
from jax import lax
from jax.experimental import pallas as pl
from jax.experimental.pallas import tpu as pltpu
from jax.sharding import Mesh
from jax.sharding import PartitionSpec as P

MESH = pl.DeviceIdType.MESH
SP = ("z", "y", "c")
NZ, NY, NC, NX = 8, 4, 2, 4
ROWS, DH, BLK = 512, 128, 128
HW = 256
DM = 2048
OWN = 512
NB = ROWS // BLK
NEG = -1e30
EPS = 1e-6
F32, BF16 = jnp.float32, jnp.bfloat16
OFFS = (0, -1, 1, 2)
LOADS = ("up", "down", "ig", "fg", "ex", "doc", "k", "v", "q", "cg", "og", "mg", "res", "w")

RIGHT = {"U": (0, -2, 2, -4), "D": (0, -2, 2)}
SPLIT = {"U": 16, "D": 24}

RECEIVES = 164

ORDER = (
    "tell", "begin", "Uz0", "Ddz0,0", "wsend", "Udy", "Ddy", "Dz0", "gsend",
    "intra0", "Dyz0", "Uz-1", "Uz1", "Uyz1", "Ddo", "Uyz-1", "Udz0,0", "st0",
    "intra1", "Dz1", "Dz-1", "Uz-2", "Ups1", "Udo", "Uz2", "Udz0,1", "st1",
    "Ddz0,1", "Udz1,0", "Dyz-1", "Uyz-2", "comb", "Ddz0,2", "cell0", "Dyz1", "Udz0,-1",
    "Uz-3", "Udz-1,0", "Um1", "cell1", "Uz3", "wpass", "Udz0,2", "Udz-1,1", "Udm0",
    "Udz1,1", "Ups-1", "Uyz3", "Dps-1", "Dz-2", "Udz-1,-1", "Ddz0,-1", "Uyz-3", "Ddm0",
    "ul0", "Udz2,0", "Ddz1,0", "Ddz1,1", "ur0", "Uyz0", "Uyz2", "Uz-4", "Udz-2,0",
    "Udz1,2", "ul1", "ur1", "Udz1,-1", "Udz-1,2", "Ddz1,2", "Udm-1", "Dps1", "out0",
    "Ups3", "Udz3,0", "Uyz-4", "Ddz1,-1", "Udz2,1", "Dyz-2", "out1", "Udz-2,-1", "Ups2",
    "Udz-2,1", "Dm-1", "Udz2,2", "Ups-3", "Ups0", "Udz2,-1", "Udz-3,0", "Dz2", "Udz-2,2",
    "Dyz2", "Udz3,1", "Ups-4", "Udz3,2", "Ups-2", "Ddz2,1", "Udm-2", "Ddz2,-1", "Dps0",
    "Ddz2,2", "fl0", "Dm1", "Udz-3,-1", "Dz-3", "Ddz-1,-1", "Ddz-1,0", "fr0", "Ddz2,0",
    "Ddz-1,2", "Ddz-1,1", "Udm2", "Um0", "Udz3,-1", "Um-1", "Udm3", "Um3", "Udz-3,1",
    "Ddm2", "Dps-2", "Udm1", "Um2", "Ddm1", "Dps2", "Dyz-3", "Um-3", "Um-4",
    "Udz-3,2", "Ddm-1", "Udz-4,0", "Udz-4,-1", "Dz3", "Udm-3", "Dyz3", "fl1", "Udz4,1",
    "Um-2", "Udz4,2", "Udm4", "Ddz3,1", "fr1", "Dz-4", "Dyz-4", "Ddz3,-1", "Dps-3",
    "norm0", "Ddz-2,0", "up0,0", "Ddz-2,2", "Ddz-2,-1", "Dm0", "Ddz3,0", "up0,1", "Ddz3,2",
    "Ddm3", "Dps3", "Ddz-2,1", "up0,2", "Ddm-2", "Dm-2", "up0,3", "Ddz4,1", "s0,0",
    "Dm2", "Ddz-3,0", "Dps-4", "norm1", "up1,0", "up1,1", "Ddz4,2", "Ddz-3,-1", "Ddz-3,2",
    "s0,1", "Dm-3", "Ddz-3,1", "up1,2", "Ddm-3", "up1,3", "Ddz-4,0", "Dm3", "s1,0",
    "Ddz-4,-1", "Ddm4", "Dm-4", "s1,1", "s0,2", "j0,1", "s1,2", "s0,3", "j0,0",
    "s1,3", "j1,0", "j0,2", "j1,2", "j1,1", "j0,3", "j1,3", "sent", "fin0",
    "fin1", "rest",
)


def across(row):
    return jnp.transpose(jnp.broadcast_to(row, (BLK, BLK)))


def rows_of(values):
    return lax.dot_general(
        jnp.ones((8, BLK), F32), values, (((1,), (1,)), ((), ())),
        precision=lax.Precision.HIGHEST, preferred_element_type=F32,
    )


def kernel(
    ig_h, fg_h, ex_h, doc_h, cg_h, mg_h, q_h, k_h, v_h, og_h, res_h, wout_h, up_h, down_h,
    out_h,
    ig, fg, ex, doc, cg, mg, q, k, v, og, res, wc, nd, top, stin, auxin,
    u, line1, line1in, full, line2, line2in, gains, normed, wup, wdn, squared, terms, parts, out,
    lsem, ssem, rsem, prs, osem,
):
    z, y, c, x = (lax.axis_index(a) for a in ("z", "y", "c", "x"))
    chip = z * NY + y

    def at_chip(i):
        i = lax.rem(i + NZ * NY, NZ * NY)
        return {"z": i // NY, "y": lax.rem(i, NY)}

    xi = lambda o: lax.rem(x + NX + o, NX)
    yi = lambda o: lax.rem(y + NY + o, NY)
    zi = lambda o: lax.rem(z + NZ + o, NZ)
    xr, xl, yr, yl, zr, zl = ({a: f(o)} for a, f in (("x", xi), ("y", yi), ("z", zi)) for o in (1, -1))
    mate = {"c": 1 - c}
    ahead, behind, two_ahead, two_behind = (at_chip(chip + o) for o in (1, -1, 2, -2))
    sp = chip * NC + c

    own_cols = pl.ds(pl.multiple_of(x * OWN, OWN), OWN)
    sources = dict(
        up=(up_h, wup.at[z, y, c]), down=(down_h, wdn.at[z, y, c]), ig=(ig_h, ig), fg=(fg_h, fg), ex=(ex_h, ex),
        doc=(doc_h, doc), k=(k_h, k), v=(v_h, v), q=(q_h, q), cg=(cg_h, cg), og=(og_h, og), mg=(mg_h, mg),
        res=(res_h, res), w=(wout_h.at[:, own_cols], wc.at[pl.ds(pl.multiple_of(x * HW, HW), HW), :]),
    )
    loads = {}
    for i, name in enumerate(LOADS):
        loads[name] = pltpu.make_async_copy(*sources[name], lsem.at[i])
        loads[name].start()

    barrier = pltpu.get_barrier_semaphore()
    peers = [xr, xl, {"x": xi(2)}, mate, yr, yl, zr, zl, ahead, behind, two_ahead, two_behind]
    for peer in peers:
        pl.semaphore_signal(barrier, inc=1, device_id=peer, device_id_type=MESH)
    copies, shared = {}, {}
    sizes = {
        "U1": wup.at[0:7, 0, 0], "U2": wup.at[0:7], "D1": wdn.at[0:7, 0, 0], "D2": wdn.at[0:7],
        "u": u.at[0:384], "f": full.at[0:384], "l": line1in, "m": line2in, "g": gains.at[0:3],
        "w": wc.at[0:384], "wm": wc.at[0:384], "st": stin.at[0:5], "sx": auxin.at[0:5], "p": parts,
    }
    groups = list(sizes)
    counts = [0]

    def receive(key=None):
        if key in shared:
            return shared[key]
        counts[0] += 1
        if key is not None:
            shared[key] = counts[0] - 1
        return counts[0] - 1

    def send(group, name, src, dst, dev, key=None):
        d = pltpu.make_async_remote_copy(
            src_ref=src, dst_ref=dst, send_sem=ssem.at[groups.index(group)], recv_sem=rsem.at[receive(key)],
            device_id=dev, device_id_type=MESH,
        )
        d.start()
        copies[name] = d

    def arrived(*names):
        for name in names:
            copies[name].wait_recv()

    def all_arrived(key, ref):
        pltpu.make_async_copy(ref, ref, rsem.at[shared[key]]).wait()

    def all_sent(group):
        pltpu.make_async_copy(sizes[group], sizes[group], ssem.at[groups.index(group)]).wait()

    got = {}
    steps = {}

    def step(f):
        steps[f.__name__] = f
        return f

    @step
    def begin():
        loads["up"].wait()
        loads["down"].wait()

    def weight(w, buf):
        lo, hi = pl.ds(0, SPLIT[w]), pl.ds(SPLIT[w], 32 - SPLIT[w])
        at_lo = lambda zo, yo: buf.at[zi(zo), yi(yo), c, lo]
        at_hi = lambda zo, yo: buf.at[zi(zo), yi(yo), c, hi]

        early = ["dz%d,%d" % (zo, yo) for zo in (-1, 1, -2, 2, -3, 3, -4, 4) for yo in OFFS][:14 if w == "U" else 32]

        def put(name, ref, dev, key=None):
            send(w + ("1" if name in early else "2"), w + name, ref, ref, dev, key)

        def come(*names):
            arrived(*(w + name for name in names))

        mates = lambda zo: "U" if w == "U" else "D%d" % max(abs(zo) - 1, 0)

        def along_z(zo):
            if zo:
                come("z%d" % zo)
            if -4 < zo <= 0:
                put("z%d" % (zo - 1), at_lo(zo, 0), zr)
            if 0 <= zo < 3:
                put("z%d" % (zo + 1), at_lo(zo, 0), zl)

        def along_y(zo):
            put("y%d,-1" % zo, at_lo(zo, 0), yr)
            put("y%d,1" % zo, at_lo(zo, 0), yl)

        def opposite(zo):
            side = -1 if zo in RIGHT[w] else 1
            come("y%d,%d" % (zo, side))
            put("o%d" % zo, at_lo(zo, side), yr if side < 0 else yl)

        def hand_y(zo):
            come("y%d,%d" % (zo, 1 if zo in RIGHT[w] else -1), "o%d" % zo)
            put("mr%d" % zo, buf.at[zi(zo), :, c, lo], mate, mates(zo))

        def first_y():
            put("dy-1", at_hi(0, 0), yr)
            put("dy1", at_hi(0, 0), yl)

        over = -1 if w == "U" else 1

        def second_y():
            come("dy%d" % over)
            put("do", at_hi(0, over), yr if over < 0 else yl)

        def then_z(zo, yo):
            if zo:
                come("dz%d,%d" % (zo, yo))
            elif yo == -over:
                come("dy%d" % yo)
            elif yo == 2:
                come("do")
            for side, dev, last in ((-1, zr, (0, -1)), (1, zl, (1, 2))):
                if zo * side < 0 or abs(zo) == 4 or (abs(zo) == 3 and yo not in last):
                    continue
                put("dz%d,%d" % (zo + side, yo), at_hi(zo, yo), dev)

        def hand_z(zo):
            put("dmr%d" % zo, buf.at[zi(zo), :, c, hi], mate, mates(zo))

        for zo in range(-4, 4):
            steps[w + "z%d" % zo] = lambda zo=zo: along_z(zo)
            steps[w + "yz%d" % zo] = lambda zo=zo: along_y(zo)
            steps[w + "ps%d" % zo] = lambda zo=zo: opposite(zo)
            steps[w + "m%d" % zo] = lambda zo=zo: hand_y(zo)
        steps[w + "dy"] = first_y
        steps[w + "do"] = second_y
        for zo in range(-4, 5):
            steps[w + "dm%d" % zo] = lambda zo=zo: hand_z(zo)
            for yo in OFFS:
                steps[w + "dz%d,%d" % (zo, yo)] = lambda zo=zo, yo=yo: then_z(zo, yo)

    weight("U", wup)
    weight("D", wdn)

    @step
    def gsend():
        loads["mg"].wait()
        gains[0] = jnp.broadcast_to(mg[...].astype(F32).reshape(1, OWN), (8, OWN))
        for r in range(1, NX):
            send("g", "g%d" % r, gains.at[0], gains.at[r], {"x": xi(r)}, "g")

    half = pl.multiple_of(c * 128, 128)
    wrows = lambda o: wc.at[pl.ds(pl.multiple_of(xi(o) * HW + half, 128), 128), :]

    @step
    def wsend():
        for r in range(1, NX):
            cols = pl.ds(pl.multiple_of(xi(r) * OWN, OWN), OWN)
            send("w", "w%d" % r, wout_h.at[pl.ds(half, 128), cols], wrows(0), {"x": xi(r)})

    @step
    def wpass():
        for r in range(1, NX):
            arrived("w%d" % r)
            send("wm", "wm%d" % r, wrows(-r), wrows(-r), mate, "wm")

    ri = lax.broadcasted_iota(jnp.int32, (BLK, BLK), 0)
    ci = lax.broadcasted_iota(jnp.int32, (BLK, BLK), 1)
    scale = DH ** (-0.5)
    block = lambda a: slice(a * BLK, (a + 1) * BLK)
    head = lambda h: slice(h * DH, (h + 1) * DH)

    @step
    def gates():
        for name in ("ig", "fg", "ex", "doc"):
            loads[name].wait()
        f = fg[...]
        lf = jnp.minimum(f, 0.0) - jnp.log1p(jnp.exp(-jnp.abs(f))) + ex[...]
        docs = doc[...].astype(F32)
        dr = [docs[:, block(a)] for a in range(NB)]
        ga = [ig[:, block(a)] for a in range(NB)]
        cum = jnp.dot(
            jnp.concatenate([lf[:, block(a)] for a in range(NB)], axis=0), (ri <= ci).astype(F32),
            precision=lax.Precision.HIGHEST, preferred_element_type=F32,
        )
        cm = [cum[2 * a:2 * a + 2] for a in range(NB)]
        tot = [jnp.broadcast_to(cm[a][:, BLK - 1:BLK], (2, BLK)) for a in range(NB)]

        def between(b, a):
            s = jnp.zeros((2, BLK), F32)
            for i in range(b, a):
                s = s + tot[i]
            return s

        got.update(
            between=between, dr=dr,
            ex=[[ga[b] - cm[b] if a == b else ga[b] + ((tot[b] - cm[b]) + between(b + 1, a))
                 for b in range(min(a + 1, NB))] for a in range(NB + 1)],
            first=jnp.broadcast_to(dr[0][:, 0:1], (1, BLK)), last=jnp.broadcast_to(dr[NB - 1][:, BLK - 1:BLK], (1, BLK)),
        )
        got["dcol"] = [across(d) for d in dr]

    @step
    def state():
        e = got["ex"][NB]
        kept = [jnp.where(got["dr"][b] == got["last"], e[b], NEG) for b in range(NB)]
        peak = jnp.maximum(jnp.maximum(kept[0], kept[1]), jnp.maximum(kept[2], kept[3]))
        peak = jnp.broadcast_to(jnp.max(peak, axis=1, keepdims=True), (2, BLK))
        wt = [jnp.exp(kept[b] - peak) for b in range(NB)]
        wrow = jnp.concatenate(wt, axis=1)
        loads["k"].wait()
        loads["v"].wait()
        for h in range(2):
            kh = k[:, head(h)]
            scaled = jnp.concatenate(
                [v[block(b), head(h)].astype(F32) * across(wt[b][h:h + 1]) for b in range(NB)], axis=0
            ).astype(BF16)
            stin[5, head(h), :] = lax.dot_general(
                kh, scaled, (((0,), (0,)), ((), ())), preferred_element_type=F32
            ).astype(BF16)
            w8 = jnp.broadcast_to(wrow[h:h + 1], (8, ROWS)).astype(BF16)
            auxin[5, 4 + h:5 + h] = jnp.dot(w8, kh, preferred_element_type=F32)[0:1]
        auxin[5, 0:2] = peak
        auxin[5, 2:4] = got["between"](0, NB)
        auxin[5, 6:7] = got["last"]
        auxin[5, 7:8] = got["last"]

    @step
    def tell():
        pass_state(5, 0, ahead)
        pass_state(5, 1, two_ahead)
        pass_state(5, 4, mate)

    def pass_state(slot, to, dev):
        send("st", "st%d" % to, stin.at[slot], stin.at[to], dev)
        send("sx", "sx%d" % to, auxin.at[slot], auxin.at[to], dev)

    @step
    def st0():
        arrived("st0", "sx0")
        pass_state(0, 2, mate)

    @step
    def st1():
        arrived("st1", "sx1")
        pass_state(1, 3, mate)

    def intra(h):
        if loads["q"] is not None:
            loads["q"].wait()
            loads["q"] = None
        vx = jnp.concatenate([v[:, head(h)], jnp.ones((ROWS, DH), BF16)], axis=1)
        for a in range(NB):
            n = (a + 1) * BLK
            sc = lax.dot_general(
                q[block(a), head(h)], k[:n, head(h)], (((1,), (1,)), ((), ())), preferred_element_type=F32
            )
            es = []
            for b in range(a + 1):
                ok = got["dcol"][a] == got["dr"][b]
                if b == a:
                    ok = ok & (ci <= ri)
                es.append(jnp.where(ok, got["ex"][a][b][h:h + 1], NEG))
            best = es[0]
            for e in es[1:]:
                best = jnp.maximum(best, e)
            best = jnp.max(best, axis=1, keepdims=True)
            p = jnp.concatenate(
                [(jnp.exp(es[b] - best) * (sc[:, block(b)] * scale)).astype(BF16) for b in range(a + 1)], axis=1
            )
            nd[h, block(a), :] = jnp.dot(p, vx[:n], preferred_element_type=F32)
            top[h, block(a), :] = jnp.broadcast_to(best, (BLK, BLK))

    steps["intra0"] = lambda: intra(0)
    steps["intra1"] = lambda: intra(1)

    ucols = lambda o: pl.ds(pl.multiple_of(xi(o) * HW, HW), HW)
    def uview(o, s, part=None):
        rows = pl.ds(256 * s, 256) if part is None else pl.ds(256 * s + 128 * part, 128)
        return u.at[rows, ucols(o)]

    fcols = lambda o: pl.ds(pl.multiple_of(xi(o) * OWN, OWN), OWN)

    def fview(o, s, part=None):
        rows = pl.ds(256 * s, 256) if part is None else pl.ds(256 * s + 128 * part, 128)
        return full.at[rows, fcols(o)]

    def spread(view, tag, s):
        send(tag, tag + "%d-" % s, view(0, s), view(0, s), xr)
        send(tag, tag + "%d+" % s, view(0, s), view(0, s), xl)

    def onward(view, tag, s, side):
        if side < 0:
            arrived(tag + "%d-" % s)
            send(tag, tag + "%dr" % s, view(-1, s, 0), view(-1, s, 0), xr)
        else:
            arrived(tag + "%d+" % s)
            send(tag, tag + "%dl" % s, view(1, s, 1), view(1, s, 1), xl)

    for s in (0, 1):
        steps["ur%d" % s] = lambda s=s: onward(uview, "u", s, -1)
        steps["ul%d" % s] = lambda s=s: onward(uview, "u", s, 1)
        steps["fr%d" % s] = lambda s=s: onward(fview, "f", s, -1)
        steps["fl%d" % s] = lambda s=s: onward(fview, "f", s, 1)

    @step
    def comb():
        arrived("st2", "sx2", "st3", "sx3", "st4", "sx4")
        gone = jnp.zeros((2, BLK), F32)
        logs, slots = [], (2 + 2 * c, 0, 3 - c, 1)
        for j, s in enumerate(slots):
            live = (auxin[s, 6:7] == got["first"]) & (sp > j)
            logs.append(jnp.where(live, auxin[s, 0:2] + gone, NEG))
            gone = gone + auxin[s, 2:4]
        came = jnp.maximum(jnp.maximum(logs[0], logs[1]), jnp.maximum(logs[2], logs[3]))
        part = [jnp.where(lg > 0.5 * NEG, jnp.exp(lg - came), 0.0) for lg in logs]
        memx = []
        for h in range(2):
            m, n = jnp.zeros((DH, DH), F32), jnp.zeros((1, BLK), F32)
            for g, s in zip(part, slots):
                m = m + g[h:h + 1] * stin[s, head(h), :].astype(F32)
                n = n + g[h:h + 1] * auxin[s, 4 + h:5 + h]
            memx.append(jnp.concatenate([m, across(n)], axis=1).astype(BF16))
        loads["og"].wait()
        loads["cg"].wait()
        got.update(memx=memx, came=came, gain=cg[...].astype(F32).reshape(1, HW))

    def cell(s):
        memx, came, gain = got["memx"], got["came"], got["gain"]
        for a in (2 * s, 2 * s + 1):
            squares = jnp.zeros((BLK, DH), F32)
            outs = []
            for h in range(2):
                qm = jnp.dot(q[block(a), head(h)], memx[h], preferred_element_type=F32) * scale
                far = jnp.where(got["dcol"][a] == got["first"], (got["between"](0, a) + came)[h:h + 1], NEG)
                near = top[h, block(a), :]
                m = jnp.maximum(near, far)
                wn, wf = jnp.exp(near - m), jnp.exp(far - m)
                num = wn * nd[h, block(a), :DH] + wf * qm[:, :DH]
                den = wn * nd[h, block(a), DH:] + wf * qm[:, DH:]
                val = num / jnp.maximum(jnp.abs(den), 1.0)
                squares = squares + val * val
                gate = jax.nn.sigmoid(og[block(a), head(h)].astype(F32))
                outs.append((gate * val * gain[:, head(h)]).astype(BF16))
            u[block(a), ucols(0)] = jnp.concatenate(outs, axis=1)
            line1[:, block(a)] = rows_of(squares)
        cols = slice(256 * s, 256 * s + 256)
        spread(uview, "u", s)
        for r in range(1, NX):
            send("l", "l%d,%d" % (s, r), line1.at[:, cols], line1in.at[r - 1, :, cols], {"x": xi(r)}, "l%d" % s)

    steps["cell0"] = lambda: cell(0)
    steps["cell1"] = lambda: cell(1)

    def head_out(s):
        cols = slice(256 * s, 256 * s + 256)
        all_arrived("l%d" % s, line1in.at[:, :, cols])
        total = line1[:, cols] + line1in[0, :, cols] + line1in[1, :, cols] + line1in[2, :, cols]
        inv = lax.rsqrt(total / (DH * 8) + EPS)
        if s == 0:
            loads["w"].wait()
            loads["res"].wait()
            all_arrived("wm", wc.at[0:384])
        arrived("u%dr" % s, "u%dl" % s)
        for a in (2 * s, 2 * s + 1):
            ic = across(inv[0:1, block(a - 2 * s)])
            acc = jnp.dot(u[block(a), :], wc[...], preferred_element_type=F32)
            squares = jnp.zeros((BLK, BLK), F32)
            outs = []
            for b in range(OWN // BLK):
                f = (res[block(a), block(b)].astype(F32) + acc[:, block(b)] * ic).astype(BF16)
                fw = f.astype(F32)
                squares = squares + fw * fw
                outs.append(f)
            full[block(a), fcols(0)] = jnp.concatenate(outs, axis=1)
            line2[:, block(a)] = rows_of(squares)

        spread(fview, "f", s)
        for r in range(1, NX):
            send("m", "m%d,%d" % (s, r), line2.at[:, cols], line2in.at[r - 1, :, cols], {"x": xi(r)}, "m%d" % s)

    steps["out0"] = lambda: head_out(0)
    steps["out1"] = lambda: head_out(1)

    def norm(s):
        cols = slice(256 * s, 256 * s + 256)
        all_arrived("m%d" % s, line2in.at[:, :, cols])
        total = line2[:, cols] + line2in[0, :, cols] + line2in[1, :, cols] + line2in[2, :, cols]
        inv = lax.rsqrt(total / DM + EPS)
        if s == 0:
            all_arrived("g", gains.at[0:3])
        arrived("f%dr" % s, "f%dl" % s)
        for a in (2 * s, 2 * s + 1):
            ic = across(inv[0:1, block(a - 2 * s)])
            for r in range(NX):
                fw = full[block(a), fcols(-r)].astype(F32)
                gain = gains[0, 0:1] if r == 0 else gains[r, 0:1]
                normed[block(a), fcols(-r)] = jnp.concatenate(
                    [(fw[:, block(b)] * ic * gain[:, block(b)]).astype(BF16) for b in range(OWN // BLK)], axis=1
                )

    steps["norm0"] = lambda: norm(0)
    steps["norm1"] = lambda: norm(1)

    def up(s, t):
        if s == t == 0:
            all_arrived("U", wup.at[0:4])
        rows, cols = slice(256 * s, 256 * s + 256), slice(t * 512, (t + 1) * 512)
        hid = jnp.dot(normed[rows, :], wup[:, :, :, :, cols].reshape(DM, 512), preferred_element_type=F32)
        hid = jnp.maximum(hid, 0.0)
        squared[rows, cols] = (hid * hid).astype(BF16)

    for t in range(4):
        steps["up0,%d" % t] = lambda t=t: up(0, t)
        steps["up1,%d" % t] = lambda t=t: up(1, t)

    zb = lax.rem(z, 2)
    owner = [lax.rem(z // 2 + d + NX, NX) for d in (0, 2 * zb - 1, 1 - 2 * zb, 2)]
    ahead_by = [lax.rem(o - x + NX, NX) for o in owner]
    ways = ((0, xr), (1, xl), (1, xr), (0, xl), (0, xr), (1, xl))
    quarter = lambda s, h: slice(256 * s + 128 * h, 256 * s + 128 * h + 128)

    def part(s, i, k):
        h, dev = ways[i]
        return pltpu.make_async_remote_copy(
            src_ref=terms.at[k, quarter(s, h)], dst_ref=parts.at[s, i], send_sem=ssem.at[groups.index("p")],
            recv_sem=prs.at[6 * s + i], device_id=dev, device_id_type=MESH,
        )

    def stage(s, k):
        if s == 0:
            all_arrived("D%d" % k, (wdn.at[0:3, :, 0], wdn.at[0], wdn.at[0], wdn.at[0, :, 0])[k])
        w = wdn[pl.ds(2 * owner[k], 2)].reshape(OWN, DM)
        rows = slice(256 * s, 256 * s + 256)
        terms[k, rows] = lax.dot_general(
            squared[rows, :], w, (((1,), (1,)), ((), ())), preferred_element_type=F32
        ).astype(BF16)

        @pl.when(ahead_by[k] == 2)
        def _():
            part(s, 0, k).start()
            part(s, 1, k).start()

        @pl.when(ahead_by[k] == 1)
        def _():
            part(s, 2, k).start()

        @pl.when(ahead_by[k] == 3)
        def _():
            part(s, 3, k).start()

    def join(s, k):
        for side, h, i in ((1, 0, 0), (3, 1, 1)):
            @pl.when(ahead_by[k] == side)
            def _():
                part(s, i, 0).wait_recv()
                rows = quarter(s, h)
                terms[k, rows] = (terms[k, rows].astype(F32) + parts[s, i].astype(F32)).astype(BF16)
                part(s, i + 4, k).start()

    @step
    def sent():
        for group in groups:
            if group != "p":
                all_sent(group)

    def final(s):
        d = lax.rem(x - z // 2 + NX, NX)
        d = lax.rem(d * (2 * zb - 1) + NX, NX)
        mine = terms.at[d + d // 2 - 2 * (d // 3)]
        for h, i, n in ((0, 3, 4), (1, 2, 5)):
            part(s, i, 0).wait_recv()
            part(s, n, 0).wait_recv()
            rows = quarter(s, h)
            out[rows] = (
                full[rows, fcols(0)].astype(F32) + mine[rows].astype(F32)
                + parts[s, i].astype(F32) + parts[s, n].astype(F32)
            ).astype(BF16)
        half = slice(256 * s, 256 * s + 256)
        d = pltpu.make_async_copy(out.at[half], out_h.at[half], osem.at[s])
        d.start()
        kept.append(d)

    kept = []

    @step
    def rest():
        for d in kept:
            d.wait()
        all_sent("p")

    for s in (0, 1):
        for n in range(4):
            steps["s%d,%d" % (s, n)] = lambda s=s, n=n: stage(s, n)
            steps["j%d,%d" % (s, n)] = lambda s=s, n=n: join(s, n)
        steps["fin%d" % s] = lambda s=s: final(s)

    steps["gates"]()
    steps["state"]()
    pl.semaphore_wait(barrier, len(peers))
    for name in ORDER:
        steps[name]()


def layer(*arrays):
    dma = pltpu.SemaphoreType.DMA
    return pl.pallas_call(
        kernel,
        out_shape=jax.ShapeDtypeStruct((ROWS, OWN), BF16),
        in_specs=[pl.BlockSpec(memory_space=pltpu.HBM)] * len(arrays),
        out_specs=pl.BlockSpec(memory_space=pltpu.HBM),
        scratch_shapes=[
            *[pltpu.VMEM(a.shape, a.dtype) for a in arrays[:11]],
            pltpu.VMEM((4 * HW, OWN), BF16),
            pltpu.VMEM((2, ROWS, 2 * DH), F32),
            pltpu.VMEM((2, ROWS, DH), F32),
            pltpu.VMEM((6, 2 * DH, DH), BF16),
            pltpu.VMEM((6, 8, BLK), F32),
            pltpu.VMEM((ROWS, 4 * HW), BF16),
            pltpu.VMEM((8, ROWS), F32),
            pltpu.VMEM((3, 8, ROWS), F32),
            pltpu.VMEM((ROWS, DM), BF16),
            pltpu.VMEM((8, ROWS), F32),
            pltpu.VMEM((3, 8, ROWS), F32),
            pltpu.VMEM((4, 8, OWN), F32),
            pltpu.VMEM((ROWS, DM), BF16),
            pltpu.VMEM((NZ, NY, NC, 32, DM), BF16),
            pltpu.VMEM((NZ, NY, NC, 32, DM), BF16),
            pltpu.VMEM((ROWS, DM), BF16),
            pltpu.VMEM((4, ROWS, OWN), BF16),
            pltpu.VMEM((2, 6, ROWS // 4, OWN), BF16),
            pltpu.VMEM((ROWS, OWN), BF16),
            dma((len(LOADS),)), dma((14,)), dma((RECEIVES,)), dma((12,)), dma((2,)),
        ],
        compiler_params=pltpu.CompilerParams(
            collective_id=0, has_side_effects=True, vmem_limit_bytes=62 * 2**20
        ),
    )(*arrays)


def local(
    queries, keys, values, output_gate_logits, input_gate_log, forget_gate_logits, extra_decay_log,
    document, residual, cell_norm_gain, output_weight, mixer_norm_gain, up_weight, down_weight,
):
    return layer(
        input_gate_log.T, forget_gate_logits.T, extra_decay_log.T, document.reshape(1, ROWS),
        cell_norm_gain, mixer_norm_gain,
        queries, keys, values, output_gate_logits, residual, output_weight, up_weight, down_weight.T,
    )


def solution(mesh):
    split = Mesh(mesh.devices.reshape(NZ, NY, NC, NX), ("z", "y", "c", "x"))
    rows, heads = P(SP, "x"), P("x")
    return jax.shard_map(
        local,
        mesh=split,
        in_specs=(
            rows, rows, rows, rows, rows, rows, rows, P(SP), rows, heads, P("x", None), heads, rows, P("x", SP),
        ),
        out_specs=rows,
        check_vma=False,
    )
```

```python
import jax
import jax.numpy as jnp
from jax import lax
from jax.experimental import pallas as pl
from jax.experimental.pallas import tpu as pltpu
from jax.sharding import Mesh
from jax.sharding import PartitionSpec as P

MESH = pl.DeviceIdType.MESH
SP = ("z", "y", "c")
NZ, NY, NC, NX = 8, 4, 2, 4
ROWS, DH, BLK = 512, 128, 128
HW = 256
DM = 2048
OWN = 512
NB = ROWS // BLK
NEG = -1e30
EPS = 1e-6
F32, BF16 = jnp.float32, jnp.bfloat16
OFFS = (0, -1, 1, 2)
LOADS = ("up", "down", "ig", "fg", "ex", "doc", "k", "v", "q", "cg", "og", "mg", "res", "w")

RIGHT = {"U": (0, -2, 2, -4), "D": (0, -2, 2)}
SPLIT = {"U": 16, "D": 24}

RECEIVES = 164

ORDER = (
    "tell", "begin", "Uz0", "Udy", "Uyz0", "Ddz0,0", "intra0", "wsend", "Ddy",
    "Dz0", "Uz-1", "Uz1", "Uyz-1", "Dyz0", "Uyz1", "Udz0,1", "Udz0,0", "Ddz1,0",
    "st0", "intra1", "Ups-1", "gsend", "Uz2", "Uz-2", "Dz-1", "st1", "Udo",
    "Ddo", "Udz0,-1", "Dz1", "Uyz-2", "comb", "cell0", "Uyz2", "wpass", "Dyz-1",
    "Uz-3", "Udz1,0", "Um-1", "Ddz0,-1", "Ups1", "Ddz0,1", "cell1", "Udz1,1", "Udz-1,-1",
    "Udz-1,0", "Udz0,2", "Dz2", "Uz3", "ur0", "Ups0", "Udz-1,1", "Ddz0,2", "ul0",
    "Uz-4", "Uyz-4", "Dyz2", "ul1", "Dps-1", "ur1", "Dz-2", "Ddz1,-1", "Uyz3",
    "Udz1,-1", "Uyz-3", "Ddz1,1", "Udm0", "Ups2", "Udz-2,-1", "Ddz-1,-1", "Ups-2", "out0",
    "Ddm0", "Udz1,2", "Udz2,1", "Dyz-2", "out1", "Udz2,0", "Um1", "Um0", "Udz-1,2",
    "Dz3", "Ups-4", "Udm-1", "Dm-1", "Udz-2,0", "Dyz1", "Udm1", "Dps0", "Ups-3",
    "Udz2,2", "Udz-2,1", "Udz-3,-1", "fr0", "Dps2", "Um2", "Udz-2,2", "Ups3", "Udz2,-1",
    "Udz3,1", "Dps1", "Um-3", "Udz-3,0", "fl0", "Udz3,2", "Ddz-1,0", "Dz-3", "Ddz-1,1",
    "Udm2", "Ddz-1,2", "Ddz1,2", "Dps-2", "Ddz2,1", "Udz3,-1", "Udz3,0", "Udm-2", "Udm3",
    "Udz-3,1", "Dyz3", "Um3", "Ddz2,-1", "Um-2", "Ddz2,0", "Udz-4,-1", "Udz-3,2", "Udm-3",
    "fr1", "fl1", "Ddm1", "Dyz-3", "Um-4", "Udz-4,0", "Ddz-2,-1", "Udz4,2", "Udz4,1",
    "Udm4", "Ddz-2,0", "Ddz2,2", "Ddm2", "norm0", "Dps3", "Ddm-1", "up0,0", "Dm0",
    "up0,1", "Ddz-2,1", "Ddz3,0", "Ddz3,1", "Dz-4", "Dyz-4", "Ddz3,-1", "norm1", "Dm1",
    "up0,2", "Dm2", "Dps-3", "Ddz-2,2", "Ddm-2", "Ddz3,2", "up0,3", "s0,0", "Ddz-3,0",
    "Ddz-3,-1", "Ddz4,1", "Ddz-3,1", "Dm-2", "up1,0", "up1,1", "Dps-4", "Ddz4,2", "Ddz-3,2",
    "s0,1", "Ddm3", "Ddm-3", "up1,2", "Ddz-4,-1", "Ddz-4,0", "Dm3", "up1,3", "Dm-3",
    "Ddm4", "s1,0", "Dm-4", "s1,1", "s0,2", "j0,1", "s1,2", "s0,3", "j0,0",
    "s1,3", "j1,0", "j0,2", "j1,2", "j1,1", "j0,3", "j1,3", "sent", "fin0",
    "fin1", "rest",
)


def across(row):
    return jnp.transpose(jnp.broadcast_to(row, (BLK, BLK)))


def rows_of(values):
    return lax.dot_general(
        jnp.ones((8, BLK), F32), values, (((1,), (1,)), ((), ())),
        precision=lax.Precision.HIGHEST, preferred_element_type=F32,
    )


def kernel(
    ig_h, fg_h, ex_h, doc_h, cg_h, mg_h, q_h, k_h, v_h, og_h, res_h, wout_h, up_h, down_h,
    out_h,
    ig, fg, ex, doc, cg, mg, q, k, v, og, res, wc, nd, top, stin, auxin,
    u, line1, line1in, full, line2, line2in, gains, normed, wup, wdn, squared, terms, parts, out,
    lsem, ssem, rsem, prs, osem,
):
    z, y, c, x = (lax.axis_index(a) for a in ("z", "y", "c", "x"))
    chip = z * NY + y

    def at_chip(i):
        i = lax.rem(i + NZ * NY, NZ * NY)
        return {"z": i // NY, "y": lax.rem(i, NY)}

    xi = lambda o: lax.rem(x + NX + o, NX)
    yi = lambda o: lax.rem(y + NY + o, NY)
    zi = lambda o: lax.rem(z + NZ + o, NZ)
    xr, xl, yr, yl, zr, zl = ({a: f(o)} for a, f in (("x", xi), ("y", yi), ("z", zi)) for o in (1, -1))
    mate = {"c": 1 - c}
    ahead, behind, two_ahead, two_behind = (at_chip(chip + o) for o in (1, -1, 2, -2))
    sp = chip * NC + c

    own_cols = pl.ds(pl.multiple_of(x * OWN, OWN), OWN)
    sources = dict(
        up=(up_h, wup.at[z, y, c]), down=(down_h, wdn.at[z, y, c]), ig=(ig_h, ig), fg=(fg_h, fg), ex=(ex_h, ex),
        doc=(doc_h, doc), k=(k_h, k), v=(v_h, v), q=(q_h, q), cg=(cg_h, cg), og=(og_h, og), mg=(mg_h, mg),
        res=(res_h, res), w=(wout_h.at[:, own_cols], wc.at[pl.ds(pl.multiple_of(x * HW, HW), HW), :]),
    )
    loads = {}
    for i, name in enumerate(LOADS):
        loads[name] = pltpu.make_async_copy(*sources[name], lsem.at[i])
        loads[name].start()

    barrier = pltpu.get_barrier_semaphore()
    peers = [xr, xl, {"x": xi(2)}, mate, yr, yl, zr, zl, ahead, behind, two_ahead, two_behind]
    for peer in peers:
        pl.semaphore_signal(barrier, inc=1, device_id=peer, device_id_type=MESH)
    copies, shared = {}, {}
    sizes = {
        "U1": wup.at[0:7, 0, 0], "U2": wup.at[0:7], "D1": wdn.at[0:7, 0, 0], "D2": wdn.at[0:7],
        "u": u.at[0:384], "f": full.at[0:384], "l": line1in, "m": line2in, "g": gains.at[0:3],
        "w": wc.at[0:384], "wm": wc.at[0:384], "st": stin.at[0:5], "sx": auxin.at[0:5], "p": parts,
    }
    groups = list(sizes)
    counts = [0]

    def receive(key=None):
        if key in shared:
            return shared[key]
        counts[0] += 1
        if key is not None:
            shared[key] = counts[0] - 1
        return counts[0] - 1

    def send(group, name, src, dst, dev, key=None):
        d = pltpu.make_async_remote_copy(
            src_ref=src, dst_ref=dst, send_sem=ssem.at[groups.index(group)], recv_sem=rsem.at[receive(key)],
            device_id=dev, device_id_type=MESH,
        )
        d.start()
        copies[name] = d

    def arrived(*names):
        for name in names:
            copies[name].wait_recv()

    def all_arrived(key, ref):
        pltpu.make_async_copy(ref, ref, rsem.at[shared[key]]).wait()

    def all_sent(group):
        pltpu.make_async_copy(sizes[group], sizes[group], ssem.at[groups.index(group)]).wait()

    got = {}
    steps = {}

    def step(f):
        steps[f.__name__] = f
        return f

    @step
    def begin():
        loads["up"].wait()
        loads["down"].wait()

    def weight(w, buf):
        lo, hi = pl.ds(0, SPLIT[w]), pl.ds(SPLIT[w], 32 - SPLIT[w])
        at_lo = lambda zo, yo: buf.at[zi(zo), yi(yo), c, lo]
        at_hi = lambda zo, yo: buf.at[zi(zo), yi(yo), c, hi]

        early = ["dz%d,%d" % (zo, yo) for zo in (-1, 1, -2, 2, -3, 3, -4, 4) for yo in OFFS][:14 if w == "U" else 32]

        def put(name, ref, dev, key=None):
            send(w + ("1" if name in early else "2"), w + name, ref, ref, dev, key)

        def come(*names):
            arrived(*(w + name for name in names))

        mates = lambda zo: "U" if w == "U" else "D%d" % max(abs(zo) - 1, 0)

        def along_z(zo):
            if zo:
                come("z%d" % zo)
            if -4 < zo <= 0:
                put("z%d" % (zo - 1), at_lo(zo, 0), zr)
            if 0 <= zo < 3:
                put("z%d" % (zo + 1), at_lo(zo, 0), zl)

        def along_y(zo):
            put("y%d,-1" % zo, at_lo(zo, 0), yr)
            put("y%d,1" % zo, at_lo(zo, 0), yl)

        def opposite(zo):
            side = -1 if zo in RIGHT[w] else 1
            come("y%d,%d" % (zo, side))
            put("o%d" % zo, at_lo(zo, side), yr if side < 0 else yl)

        def hand_y(zo):
            come("y%d,%d" % (zo, 1 if zo in RIGHT[w] else -1), "o%d" % zo)
            put("mr%d" % zo, buf.at[zi(zo), :, c, lo], mate, mates(zo))

        def first_y():
            put("dy-1", at_hi(0, 0), yr)
            put("dy1", at_hi(0, 0), yl)

        over = -1 if w == "U" else 1

        def second_y():
            come("dy%d" % over)
            put("do", at_hi(0, over), yr if over < 0 else yl)

        def then_z(zo, yo):
            if zo:
                come("dz%d,%d" % (zo, yo))
            elif yo == -over:
                come("dy%d" % yo)
            elif yo == 2:
                come("do")
            for side, dev, last in ((-1, zr, (0, -1)), (1, zl, (1, 2))):
                if zo * side < 0 or abs(zo) == 4 or (abs(zo) == 3 and yo not in last):
                    continue
                put("dz%d,%d" % (zo + side, yo), at_hi(zo, yo), dev)

        def hand_z(zo):
            put("dmr%d" % zo, buf.at[zi(zo), :, c, hi], mate, mates(zo))

        for zo in range(-4, 4):
            steps[w + "z%d" % zo] = lambda zo=zo: along_z(zo)
            steps[w + "yz%d" % zo] = lambda zo=zo: along_y(zo)
            steps[w + "ps%d" % zo] = lambda zo=zo: opposite(zo)
            steps[w + "m%d" % zo] = lambda zo=zo: hand_y(zo)
        steps[w + "dy"] = first_y
        steps[w + "do"] = second_y
        for zo in range(-4, 5):
            steps[w + "dm%d" % zo] = lambda zo=zo: hand_z(zo)
            for yo in OFFS:
                steps[w + "dz%d,%d" % (zo, yo)] = lambda zo=zo, yo=yo: then_z(zo, yo)

    weight("U", wup)
    weight("D", wdn)

    @step
    def gsend():
        loads["mg"].wait()
        gains[0] = jnp.broadcast_to(mg[...].astype(F32).reshape(1, OWN), (8, OWN))
        for r in range(1, NX):
            send("g", "g%d" % r, gains.at[0], gains.at[r], {"x": xi(r)}, "g")

    half = pl.multiple_of(c * 128, 128)
    wrows = lambda o: wc.at[pl.ds(pl.multiple_of(xi(o) * HW + half, 128), 128), :]

    @step
    def wsend():
        for r in range(1, NX):
            cols = pl.ds(pl.multiple_of(xi(r) * OWN, OWN), OWN)
            send("w", "w%d" % r, wout_h.at[pl.ds(half, 128), cols], wrows(0), {"x": xi(r)})

    @step
    def wpass():
        for r in range(1, NX):
            arrived("w%d" % r)
            send("wm", "wm%d" % r, wrows(-r), wrows(-r), mate, "wm")

    ri = lax.broadcasted_iota(jnp.int32, (BLK, BLK), 0)
    ci = lax.broadcasted_iota(jnp.int32, (BLK, BLK), 1)
    scale = DH ** (-0.5)
    block = lambda a: slice(a * BLK, (a + 1) * BLK)
    head = lambda h: slice(h * DH, (h + 1) * DH)

    @step
    def gates():
        for name in ("ig", "fg", "ex", "doc"):
            loads[name].wait()
        f = fg[...]
        lf = jnp.minimum(f, 0.0) - jnp.log1p(jnp.exp(-jnp.abs(f))) + ex[...]
        docs = doc[...].astype(F32)
        dr = [docs[:, block(a)] for a in range(NB)]
        ga = [ig[:, block(a)] for a in range(NB)]
        cum = jnp.dot(
            jnp.concatenate([lf[:, block(a)] for a in range(NB)], axis=0), (ri <= ci).astype(F32),
            precision=lax.Precision.HIGHEST, preferred_element_type=F32,
        )
        cm = [cum[2 * a:2 * a + 2] for a in range(NB)]
        tot = [jnp.broadcast_to(cm[a][:, BLK - 1:BLK], (2, BLK)) for a in range(NB)]

        def between(b, a):
            s = jnp.zeros((2, BLK), F32)
            for i in range(b, a):
                s = s + tot[i]
            return s

        got.update(
            between=between, dr=dr,
            ex=[[ga[b] - cm[b] if a == b else ga[b] + ((tot[b] - cm[b]) + between(b + 1, a))
                 for b in range(min(a + 1, NB))] for a in range(NB + 1)],
            first=jnp.broadcast_to(dr[0][:, 0:1], (1, BLK)), last=jnp.broadcast_to(dr[NB - 1][:, BLK - 1:BLK], (1, BLK)),
        )
        got["dcol"] = [across(d) for d in dr]

    @step
    def state():
        e = got["ex"][NB]
        kept = [jnp.where(got["dr"][b] == got["last"], e[b], NEG) for b in range(NB)]
        peak = jnp.maximum(jnp.maximum(kept[0], kept[1]), jnp.maximum(kept[2], kept[3]))
        peak = jnp.broadcast_to(jnp.max(peak, axis=1, keepdims=True), (2, BLK))
        wt = [jnp.exp(kept[b] - peak) for b in range(NB)]
        wrow = jnp.concatenate(wt, axis=1)
        loads["k"].wait()
        loads["v"].wait()
        for h in range(2):
            kh = k[:, head(h)]
            scaled = jnp.concatenate(
                [v[block(b), head(h)].astype(F32) * across(wt[b][h:h + 1]) for b in range(NB)], axis=0
            ).astype(BF16)
            stin[5, head(h), :] = lax.dot_general(
                kh, scaled, (((0,), (0,)), ((), ())), preferred_element_type=F32
            ).astype(BF16)
            w8 = jnp.broadcast_to(wrow[h:h + 1], (8, ROWS)).astype(BF16)
            auxin[5, 4 + h:5 + h] = jnp.dot(w8, kh, preferred_element_type=F32)[0:1]
        auxin[5, 0:2] = peak
        auxin[5, 2:4] = got["between"](0, NB)
        auxin[5, 6:7] = got["last"]
        auxin[5, 7:8] = got["last"]

    @step
    def tell():
        pass_state(5, 0, ahead)
        pass_state(5, 1, two_ahead)
        pass_state(5, 4, mate)

    def pass_state(slot, to, dev):
        send("st", "st%d" % to, stin.at[slot], stin.at[to], dev)
        send("sx", "sx%d" % to, auxin.at[slot], auxin.at[to], dev)

    @step
    def st0():
        arrived("st0", "sx0")
        pass_state(0, 2, mate)

    @step
    def st1():
        arrived("st1", "sx1")
        pass_state(1, 3, mate)

    def intra(h):
        if loads["q"] is not None:
            loads["q"].wait()
            loads["q"] = None
        vx = jnp.concatenate([v[:, head(h)], jnp.ones((ROWS, DH), BF16)], axis=1)
        for a in range(NB):
            n = (a + 1) * BLK
            sc = lax.dot_general(
                q[block(a), head(h)], k[:n, head(h)], (((1,), (1,)), ((), ())), preferred_element_type=F32
            )
            es = []
            for b in range(a + 1):
                ok = got["dcol"][a] == got["dr"][b]
                if b == a:
                    ok = ok & (ci <= ri)
                es.append(jnp.where(ok, got["ex"][a][b][h:h + 1], NEG))
            best = es[0]
            for e in es[1:]:
                best = jnp.maximum(best, e)
            best = jnp.max(best, axis=1, keepdims=True)
            p = jnp.concatenate(
                [(jnp.exp(es[b] - best) * (sc[:, block(b)] * scale)).astype(BF16) for b in range(a + 1)], axis=1
            )
            nd[h, block(a), :] = jnp.dot(p, vx[:n], preferred_element_type=F32)
            top[h, block(a), :] = jnp.broadcast_to(best, (BLK, BLK))

    steps["intra0"] = lambda: intra(0)
    steps["intra1"] = lambda: intra(1)

    ucols = lambda o: pl.ds(pl.multiple_of(xi(o) * HW, HW), HW)
    def uview(o, s, part=None):
        rows = pl.ds(256 * s, 256) if part is None else pl.ds(256 * s + 128 * part, 128)
        return u.at[rows, ucols(o)]

    fcols = lambda o: pl.ds(pl.multiple_of(xi(o) * OWN, OWN), OWN)

    def fview(o, s, part=None):
        rows = pl.ds(256 * s, 256) if part is None else pl.ds(256 * s + 128 * part, 128)
        return full.at[rows, fcols(o)]

    def spread(view, tag, s):
        send(tag, tag + "%d-" % s, view(0, s), view(0, s), xr)
        send(tag, tag + "%d+" % s, view(0, s), view(0, s), xl)

    def onward(view, tag, s, side):
        if side < 0:
            arrived(tag + "%d-" % s)
            send(tag, tag + "%dr" % s, view(-1, s, 0), view(-1, s, 0), xr)
        else:
            arrived(tag + "%d+" % s)
            send(tag, tag + "%dl" % s, view(1, s, 1), view(1, s, 1), xl)

    for s in (0, 1):
        steps["ur%d" % s] = lambda s=s: onward(uview, "u", s, -1)
        steps["ul%d" % s] = lambda s=s: onward(uview, "u", s, 1)
        steps["fr%d" % s] = lambda s=s: onward(fview, "f", s, -1)
        steps["fl%d" % s] = lambda s=s: onward(fview, "f", s, 1)

    @step
    def comb():
        arrived("st2", "sx2", "st3", "sx3", "st4", "sx4")
        gone = jnp.zeros((2, BLK), F32)
        logs, slots = [], (2 + 2 * c, 0, 3 - c, 1)
        for j, s in enumerate(slots):
            live = (auxin[s, 6:7] == got["first"]) & (sp > j)
            logs.append(jnp.where(live, auxin[s, 0:2] + gone, NEG))
            gone = gone + auxin[s, 2:4]
        came = jnp.maximum(jnp.maximum(logs[0], logs[1]), jnp.maximum(logs[2], logs[3]))
        part = [jnp.where(lg > 0.5 * NEG, jnp.exp(lg - came), 0.0) for lg in logs]
        memx = []
        for h in range(2):
            m, n = jnp.zeros((DH, DH), F32), jnp.zeros((1, BLK), F32)
            for g, s in zip(part, slots):
                m = m + g[h:h + 1] * stin[s, head(h), :].astype(F32)
                n = n + g[h:h + 1] * auxin[s, 4 + h:5 + h]
            memx.append(jnp.concatenate([m, across(n)], axis=1).astype(BF16))
        loads["og"].wait()
        loads["cg"].wait()
        got.update(memx=memx, came=came, gain=cg[...].astype(F32).reshape(1, HW))

    def cell(s):
        memx, came, gain = got["memx"], got["came"], got["gain"]
        for a in (2 * s, 2 * s + 1):
            squares = jnp.zeros((BLK, DH), F32)
            outs = []
            for h in range(2):
                qm = jnp.dot(q[block(a), head(h)], memx[h], preferred_element_type=F32) * scale
                far = jnp.where(got["dcol"][a] == got["first"], (got["between"](0, a) + came)[h:h + 1], NEG)
                near = top[h, block(a), :]
                m = jnp.maximum(near, far)
                wn, wf = jnp.exp(near - m), jnp.exp(far - m)
                num = wn * nd[h, block(a), :DH] + wf * qm[:, :DH]
                den = wn * nd[h, block(a), DH:] + wf * qm[:, DH:]
                val = num / jnp.maximum(jnp.abs(den), 1.0)
                squares = squares + val * val
                gate = jax.nn.sigmoid(og[block(a), head(h)].astype(F32))
                outs.append((gate * val * gain[:, head(h)]).astype(BF16))
            u[block(a), ucols(0)] = jnp.concatenate(outs, axis=1)
            line1[:, block(a)] = rows_of(squares)
        cols = slice(256 * s, 256 * s + 256)
        spread(uview, "u", s)
        for r in range(1, NX):
            send("l", "l%d,%d" % (s, r), line1.at[:, cols], line1in.at[r - 1, :, cols], {"x": xi(r)}, "l%d" % s)

    steps["cell0"] = lambda: cell(0)
    steps["cell1"] = lambda: cell(1)

    def head_out(s):
        cols = slice(256 * s, 256 * s + 256)
        all_arrived("l%d" % s, line1in.at[:, :, cols])
        total = line1[:, cols] + line1in[0, :, cols] + line1in[1, :, cols] + line1in[2, :, cols]
        inv = lax.rsqrt(total / (DH * 8) + EPS)
        if s == 0:
            loads["w"].wait()
            loads["res"].wait()
            all_arrived("wm", wc.at[0:384])
        arrived("u%dr" % s, "u%dl" % s)
        for a in (2 * s, 2 * s + 1):
            ic = across(inv[0:1, block(a - 2 * s)])
            acc = jnp.dot(u[block(a), :], wc[...], preferred_element_type=F32)
            squares = jnp.zeros((BLK, BLK), F32)
            outs = []
            for b in range(OWN // BLK):
                f = (res[block(a), block(b)].astype(F32) + acc[:, block(b)] * ic).astype(BF16)
                fw = f.astype(F32)
                squares = squares + fw * fw
                outs.append(f)
            full[block(a), fcols(0)] = jnp.concatenate(outs, axis=1)
            line2[:, block(a)] = rows_of(squares)

        spread(fview, "f", s)
        for r in range(1, NX):
            send("m", "m%d,%d" % (s, r), line2.at[:, cols], line2in.at[r - 1, :, cols], {"x": xi(r)}, "m%d" % s)

    steps["out0"] = lambda: head_out(0)
    steps["out1"] = lambda: head_out(1)

    def norm(s):
        cols = slice(256 * s, 256 * s + 256)
        all_arrived("m%d" % s, line2in.at[:, :, cols])
        total = line2[:, cols] + line2in[0, :, cols] + line2in[1, :, cols] + line2in[2, :, cols]
        inv = lax.rsqrt(total / DM + EPS)
        if s == 0:
            all_arrived("g", gains.at[0:3])
        arrived("f%dr" % s, "f%dl" % s)
        for a in (2 * s, 2 * s + 1):
            ic = across(inv[0:1, block(a - 2 * s)])
            for r in range(NX):
                fw = full[block(a), fcols(-r)].astype(F32)
                gain = gains[0, 0:1] if r == 0 else gains[r, 0:1]
                normed[block(a), fcols(-r)] = jnp.concatenate(
                    [(fw[:, block(b)] * ic * gain[:, block(b)]).astype(BF16) for b in range(OWN // BLK)], axis=1
                )

    steps["norm0"] = lambda: norm(0)
    steps["norm1"] = lambda: norm(1)

    def up(s, t):
        if s == t == 0:
            all_arrived("U", wup.at[0:4])
        rows, cols = slice(256 * s, 256 * s + 256), slice(t * 512, (t + 1) * 512)
        hid = jnp.dot(normed[rows, :], wup[:, :, :, :, cols].reshape(DM, 512), preferred_element_type=F32)
        hid = jnp.maximum(hid, 0.0)
        squared[rows, cols] = (hid * hid).astype(BF16)

    for t in range(4):
        steps["up0,%d" % t] = lambda t=t: up(0, t)
        steps["up1,%d" % t] = lambda t=t: up(1, t)

    zb = lax.rem(z, 2)
    owner = [lax.rem(z // 2 + d + NX, NX) for d in (0, 2 * zb - 1, 1 - 2 * zb, 2)]
    ahead_by = [lax.rem(o - x + NX, NX) for o in owner]
    ways = ((0, xr), (1, xl), (1, xr), (0, xl), (0, xr), (1, xl))
    quarter = lambda s, h: slice(256 * s + 128 * h, 256 * s + 128 * h + 128)

    def part(s, i, k):
        h, dev = ways[i]
        return pltpu.make_async_remote_copy(
            src_ref=terms.at[k, quarter(s, h)], dst_ref=parts.at[s, i], send_sem=ssem.at[groups.index("p")],
            recv_sem=prs.at[6 * s + i], device_id=dev, device_id_type=MESH,
        )

    def stage(s, k):
        if s == 0:
            all_arrived("D%d" % k, (wdn.at[0:3, :, 0], wdn.at[0], wdn.at[0], wdn.at[0, :, 0])[k])
        w = wdn[pl.ds(2 * owner[k], 2)].reshape(OWN, DM)
        rows = slice(256 * s, 256 * s + 256)
        terms[k, rows] = lax.dot_general(
            squared[rows, :], w, (((1,), (1,)), ((), ())), preferred_element_type=F32
        ).astype(BF16)

        @pl.when(ahead_by[k] == 2)
        def _():
            part(s, 0, k).start()
            part(s, 1, k).start()

        @pl.when(ahead_by[k] == 1)
        def _():
            part(s, 2, k).start()

        @pl.when(ahead_by[k] == 3)
        def _():
            part(s, 3, k).start()

    def join(s, k):
        for side, h, i in ((1, 0, 0), (3, 1, 1)):
            @pl.when(ahead_by[k] == side)
            def _():
                part(s, i, 0).wait_recv()
                rows = quarter(s, h)
                terms[k, rows] = (terms[k, rows].astype(F32) + parts[s, i].astype(F32)).astype(BF16)
                part(s, i + 4, k).start()

    @step
    def sent():
        for group in groups:
            if group != "p":
                all_sent(group)

    def final(s):
        d = lax.rem(x - z // 2 + NX, NX)
        d = lax.rem(d * (2 * zb - 1) + NX, NX)
        mine = terms.at[d + d // 2 - 2 * (d // 3)]
        for h, i, n in ((0, 3, 4), (1, 2, 5)):
            part(s, i, 0).wait_recv()
            part(s, n, 0).wait_recv()
            rows = quarter(s, h)
            out[rows] = (
                full[rows, fcols(0)].astype(F32) + mine[rows].astype(F32)
                + parts[s, i].astype(F32) + parts[s, n].astype(F32)
            ).astype(BF16)
        half = slice(256 * s, 256 * s + 256)
        d = pltpu.make_async_copy(out.at[half], out_h.at[half], osem.at[s])
        d.start()
        kept.append(d)

    kept = []

    @step
    def rest():
        for d in kept:
            d.wait()
        all_sent("p")

    for s in (0, 1):
        for n in range(4):
            steps["s%d,%d" % (s, n)] = lambda s=s, n=n: stage(s, n)
            steps["j%d,%d" % (s, n)] = lambda s=s, n=n: join(s, n)
        steps["fin%d" % s] = lambda s=s: final(s)

    steps["gates"]()
    steps["state"]()
    pl.semaphore_wait(barrier, len(peers))
    for name in ORDER:
        steps[name]()


def layer(*arrays):
    dma = pltpu.SemaphoreType.DMA
    return pl.pallas_call(
        kernel,
        out_shape=jax.ShapeDtypeStruct((ROWS, OWN), BF16),
        in_specs=[pl.BlockSpec(memory_space=pltpu.HBM)] * len(arrays),
        out_specs=pl.BlockSpec(memory_space=pltpu.HBM),
        scratch_shapes=[
            *[pltpu.VMEM(a.shape, a.dtype) for a in arrays[:11]],
            pltpu.VMEM((4 * HW, OWN), BF16),
            pltpu.VMEM((2, ROWS, 2 * DH), F32),
            pltpu.VMEM((2, ROWS, DH), F32),
            pltpu.VMEM((6, 2 * DH, DH), BF16),
            pltpu.VMEM((6, 8, BLK), F32),
            pltpu.VMEM((ROWS, 4 * HW), BF16),
            pltpu.VMEM((8, ROWS), F32),
            pltpu.VMEM((3, 8, ROWS), F32),
            pltpu.VMEM((ROWS, DM), BF16),
            pltpu.VMEM((8, ROWS), F32),
            pltpu.VMEM((3, 8, ROWS), F32),
            pltpu.VMEM((4, 8, OWN), F32),
            pltpu.VMEM((ROWS, DM), BF16),
            pltpu.VMEM((NZ, NY, NC, 32, DM), BF16),
            pltpu.VMEM((NZ, NY, NC, 32, DM), BF16),
            pltpu.VMEM((ROWS, DM), BF16),
            pltpu.VMEM((4, ROWS, OWN), BF16),
            pltpu.VMEM((2, 6, ROWS // 4, OWN), BF16),
            pltpu.VMEM((ROWS, OWN), BF16),
            dma((len(LOADS),)), dma((14,)), dma((RECEIVES,)), dma((12,)), dma((2,)),
        ],
        compiler_params=pltpu.CompilerParams(
            collective_id=0, has_side_effects=True, vmem_limit_bytes=62 * 2**20
        ),
    )(*arrays)


def local(
    queries, keys, values, output_gate_logits, input_gate_log, forget_gate_logits, extra_decay_log,
    document, residual, cell_norm_gain, output_weight, mixer_norm_gain, up_weight, down_weight,
):
    return layer(
        input_gate_log.T, forget_gate_logits.T, extra_decay_log.T, document.reshape(1, ROWS),
        cell_norm_gain, mixer_norm_gain,
        queries, keys, values, output_gate_logits, residual, output_weight, up_weight, down_weight.T,
    )


def solution(mesh):
    split = Mesh(mesh.devices.reshape(NZ, NY, NC, NX), ("z", "y", "c", "x"))
    rows, heads = P(SP, "x"), P("x")
    return jax.shard_map(
        local,
        mesh=split,
        in_specs=(
            rows, rows, rows, rows, rows, rows, rows, P(SP), rows, heads, P("x", None), heads, rows, P("x", SP),
        ),
        out_specs=rows,
        check_vma=False,
    )
```

```python
import jax
import jax.numpy as jnp
from jax import lax
from jax.experimental import pallas as pl
from jax.experimental.pallas import tpu as pltpu
from jax.sharding import Mesh
from jax.sharding import PartitionSpec as P

MESH = pl.DeviceIdType.MESH
SP = ("z", "y", "c")
NZ, NY, NC, NX = 8, 4, 2, 4
ROWS, DH, BLK = 512, 128, 128
HW = 256
DM = 2048
OWN = 512
NB = ROWS // BLK
NEG = -1e30
EPS = 1e-6
F32, BF16 = jnp.float32, jnp.bfloat16
OFFS = (0, -1, 1, 2)
LOADS = ("up", "down", "ig", "fg", "ex", "doc", "k", "v", "q", "cg", "og", "mg", "res", "w")

RIGHT = {"U": (0, -2, 2, -4), "D": (0, -2, 2)}
SPLIT = {"U": 16, "D": 24}

RECEIVES = 163

ORDER = (
    "tell", "begin", "Uz0", "Udy", "Ddy", "Dyz0", "intra0", "Ddz0,0", "intra1",
    "Uyz0", "Dz0", "wsend", "Uz1", "Uz-1", "Ddo", "Uyz1", "Uyz-1", "Ddz1,0",
    "gsend", "Udz0,1", "st0", "Dz1", "Dz-1", "Uz-2", "Ddz0,1", "Ddz-1,0", "Uz2",
    "Udo", "Dyz1", "st1", "comb", "Udz1,1", "Ups1", "cell0", "Ddz0,-1", "Uyz2",
    "Dyz-1", "cell1", "Dz-2", "Ddz2,0", "Ddz0,2", "Uz-3", "Dps1", "Ddz1,1", "Ddm0",
    "Um1", "Udz0,-1", "Ups-1", "Uyz-2", "Ddz-1,-1", "Uyz-3", "ul0", "ur0", "Uz3",
    "Udz0,2", "Ddz1,-1", "Udz0,0", "Dz-3", "ul1", "Uz-4", "Dps-1", "Uyz-4", "Uyz3",
    "Dz2", "ur1", "Udm0", "wpass", "Udz1,-1", "out0", "Ups0", "Ddz3,0", "Ups2",
    "Udz1,2", "Udz-1,-1", "Dps0", "Udz1,0", "Dm1", "Udz-1,0", "Ups-2", "Ddz1,2", "Dyz-3",
    "Udz-1,2", "Udm1", "Udz-1,1", "Dz3", "out1", "Dz-4", "Udz2,1", "Ups-3", "Ups-4",
    "Udz-2,-1", "Dm-1", "Udz2,2", "Um-1", "Um0", "Udz2,0", "Dyz-4", "Ups3", "Udz-2,0",
    "Ddz2,-1", "Dyz3", "Udz2,-1", "Ddm1", "fr0", "fl0", "Ddz2,2", "Um2", "Udz-2,2",
    "Udz-2,1", "Udz3,1", "Udz-3,-1", "Udz3,2", "Ddz2,1", "Udz-3,0", "Ddz-1,1", "Udm-1", "Udz3,0",
    "Ddz-1,2", "Udm2", "Udm-2", "Ddm2", "Um-3", "Udz-3,2", "fr1", "Dps-4", "fl1",
    "Ddz-2,-1", "Dm0", "Ddm-1", "Dps-3", "Um-2", "Um3", "Ddz3,-1", "Udz3,-1", "Udm3",
    "Udz4,1", "Dps3", "Udz-4,-1", "Um-4", "Ddz-2,0", "Dyz-2", "Udz-3,1", "Dyz2", "Udm-3",
    "Ddz3,2", "Udz4,2", "Udz-4,0", "Udm4", "norm0", "Ddz-2,1", "Ddz-2,2", "up0,0", "Ddz-3,-1",
    "norm1", "Ddz3,1", "Ddm3", "Ddz-3,0", "up1,0", "Dm-3", "Dm-4", "Dps-2", "Ddz4,2",
    "up0,1", "Ddz-3,1", "Ddm-2", "up0,2", "Dm3", "Ddz-3,2", "Ddm-3", "up0,3", "Dps2",
    "Ddz-4,-1", "Ddz-4,0", "Ddz4,1", "Ddm4", "up1,1", "s0,0", "up1,2", "Dm-2", "s0,1",
    "Dm2", "up1,3", "s1,0", "s1,1", "s0,2", "s0,3", "s1,2", "s1,3", "j0,0",
    "j0,2", "j0,3", "j1,0", "j1,2", "j0,1", "j1,1", "j1,3", "sent", "fin0",
    "fin1", "rest",
)


def across(row):
    return jnp.transpose(jnp.broadcast_to(row, (BLK, BLK)))


def rows_of(values):
    return lax.dot_general(
        jnp.ones((8, BLK), F32), values, (((1,), (1,)), ((), ())),
        precision=lax.Precision.HIGHEST, preferred_element_type=F32,
    )


def kernel(
    ig_h, fg_h, ex_h, doc_h, cg_h, mg_h, q_h, k_h, v_h, og_h, res_h, wout_h, up_h, down_h,
    out_h,
    ig, fg, ex, doc, cg, mg, q, k, v, og, res, wc, nd, top, stin, auxin,
    u, line1, line1in, full, line2, line2in, gains, normed, wup, wdn, squared, terms, parts, out,
    lsem, ssem, rsem, prs, osem,
):
    z, y, c, x = (lax.axis_index(a) for a in ("z", "y", "c", "x"))
    chip = z * NY + y

    def at_chip(i):
        i = lax.rem(i + NZ * NY, NZ * NY)
        return {"z": i // NY, "y": lax.rem(i, NY)}

    xi = lambda o: lax.rem(x + NX + o, NX)
    yi = lambda o: lax.rem(y + NY + o, NY)
    zi = lambda o: lax.rem(z + NZ + o, NZ)
    xr, xl, yr, yl, zr, zl = ({a: f(o)} for a, f in (("x", xi), ("y", yi), ("z", zi)) for o in (1, -1))
    mate = {"c": 1 - c}
    ahead, behind, two_ahead, two_behind = (at_chip(chip + o) for o in (1, -1, 2, -2))
    sp = chip * NC + c

    own_cols = pl.ds(pl.multiple_of(x * OWN, OWN), OWN)
    sources = dict(
        up=(up_h, wup.at[z, y, c]), down=(down_h, wdn.at[z, y, c]), ig=(ig_h, ig), fg=(fg_h, fg), ex=(ex_h, ex),
        doc=(doc_h, doc), k=(k_h, k), v=(v_h, v), q=(q_h, q), cg=(cg_h, cg), og=(og_h, og), mg=(mg_h, mg),
        res=(res_h, res), w=(wout_h.at[:, own_cols], wc.at[pl.ds(pl.multiple_of(x * HW, HW), HW), :]),
    )
    loads = {}
    for i, name in enumerate(LOADS):
        loads[name] = pltpu.make_async_copy(*sources[name], lsem.at[i])
        loads[name].start()

    barrier = pltpu.get_barrier_semaphore()
    peers = [xr, xl, {"x": xi(2)}, mate, yr, yl, zr, zl, ahead, behind, two_ahead, two_behind]
    for peer in peers:
        pl.semaphore_signal(barrier, inc=1, device_id=peer, device_id_type=MESH)
    copies, shared = {}, {}
    sizes = {
        "U1": wup.at[0:7, 0, 0], "U2": wup.at[0:7], "D1": wdn.at[0:7, 0, 0], "D2": wdn.at[0:7],
        "u": u.at[0:384], "f": full.at[0:384], "l": line1in, "m": line2in, "g": gains.at[0:3],
        "w": wc.at[0:384], "wm": wc.at[0:384], "st": stin.at[0:5], "sx": auxin.at[0:5], "p": parts,
    }
    groups = list(sizes)
    counts = [0]

    def receive(key=None):
        if key in shared:
            return shared[key]
        counts[0] += 1
        if key is not None:
            shared[key] = counts[0] - 1
        return counts[0] - 1

    def send(group, name, src, dst, dev, key=None):
        d = pltpu.make_async_remote_copy(
            src_ref=src, dst_ref=dst, send_sem=ssem.at[groups.index(group)], recv_sem=rsem.at[receive(key)],
            device_id=dev, device_id_type=MESH,
        )
        d.start()
        copies[name] = d

    def arrived(*names):
        for name in names:
            copies[name].wait_recv()

    def all_arrived(key, ref):
        pltpu.make_async_copy(ref, ref, rsem.at[shared[key]]).wait()

    def all_sent(group):
        pltpu.make_async_copy(sizes[group], sizes[group], ssem.at[groups.index(group)]).wait()

    got = {}
    steps = {}

    def step(f):
        steps[f.__name__] = f
        return f

    @step
    def begin():
        loads["up"].wait()
        loads["down"].wait()

    def weight(w, buf):
        lo, hi = pl.ds(0, SPLIT[w]), pl.ds(SPLIT[w], 32 - SPLIT[w])
        at_lo = lambda zo, yo: buf.at[zi(zo), yi(yo), c, lo]
        at_hi = lambda zo, yo: buf.at[zi(zo), yi(yo), c, hi]

        early = ["dz%d,%d" % (zo, yo) for zo in (-1, 1, -2, 2, -3, 3, -4, 4) for yo in OFFS][:14 if w == "U" else 32]

        def put(name, ref, dev, key=None):
            send(w + ("1" if name in early else "2"), w + name, ref, ref, dev, key)

        def come(*names):
            arrived(*(w + name for name in names))

        mates = lambda zo: "U" if w == "U" else "D%d" % (0, 0, 2, 1, 1)[abs(zo)]

        def along_z(zo):
            if zo:
                come("z%d" % zo)
            if -4 < zo <= 0:
                put("z%d" % (zo - 1), at_lo(zo, 0), zr)
            if 0 <= zo < 3:
                put("z%d" % (zo + 1), at_lo(zo, 0), zl)

        def along_y(zo):
            put("y%d,-1" % zo, at_lo(zo, 0), yr)
            put("y%d,1" % zo, at_lo(zo, 0), yl)

        def opposite(zo):
            side = -1 if zo in RIGHT[w] else 1
            come("y%d,%d" % (zo, side))
            put("o%d" % zo, at_lo(zo, side), yr if side < 0 else yl)

        def hand_y(zo):
            come("y%d,%d" % (zo, 1 if zo in RIGHT[w] else -1), "o%d" % zo)
            put("mr%d" % zo, buf.at[zi(zo), :, c, lo], mate, mates(zo))

        def first_y():
            put("dy-1", at_hi(0, 0), yr)
            put("dy1", at_hi(0, 0), yl)

        over = -1 if w == "U" else 1

        def second_y():
            come("dy%d" % over)
            put("do", at_hi(0, over), yr if over < 0 else yl)

        def then_z(zo, yo):
            if zo:
                come("dz%d,%d" % (zo, yo))
            elif yo == -over:
                come("dy%d" % yo)
            elif yo == 2:
                come("do")
            for side, dev, last in ((-1, zr, (0, -1)), (1, zl, (1, 2))):
                if zo * side < 0 or abs(zo) == 4 or (abs(zo) == 3 and yo not in last):
                    continue
                put("dz%d,%d" % (zo + side, yo), at_hi(zo, yo), dev)

        def hand_z(zo):
            put("dmr%d" % zo, buf.at[zi(zo), :, c, hi], mate, mates(zo))

        for zo in range(-4, 4):
            steps[w + "z%d" % zo] = lambda zo=zo: along_z(zo)
            steps[w + "yz%d" % zo] = lambda zo=zo: along_y(zo)
            steps[w + "ps%d" % zo] = lambda zo=zo: opposite(zo)
            steps[w + "m%d" % zo] = lambda zo=zo: hand_y(zo)
        steps[w + "dy"] = first_y
        steps[w + "do"] = second_y
        for zo in range(-4, 5):
            steps[w + "dm%d" % zo] = lambda zo=zo: hand_z(zo)
            for yo in OFFS:
                steps[w + "dz%d,%d" % (zo, yo)] = lambda zo=zo, yo=yo: then_z(zo, yo)

    weight("U", wup)
    weight("D", wdn)

    @step
    def gsend():
        loads["mg"].wait()
        gains[0] = jnp.broadcast_to(mg[...].astype(F32).reshape(1, OWN), (8, OWN))
        for r in range(1, NX):
            send("g", "g%d" % r, gains.at[0], gains.at[r], {"x": xi(r)}, "g")

    half = pl.multiple_of(c * 128, 128)
    wrows = lambda o: wc.at[pl.ds(pl.multiple_of(xi(o) * HW + half, 128), 128), :]

    @step
    def wsend():
        for r in range(1, NX):
            cols = pl.ds(pl.multiple_of(xi(r) * OWN, OWN), OWN)
            send("w", "w%d" % r, wout_h.at[pl.ds(half, 128), cols], wrows(0), {"x": xi(r)})

    @step
    def wpass():
        for r in range(1, NX):
            arrived("w%d" % r)
            send("wm", "wm%d" % r, wrows(-r), wrows(-r), mate, "wm")

    ri = lax.broadcasted_iota(jnp.int32, (BLK, BLK), 0)
    ci = lax.broadcasted_iota(jnp.int32, (BLK, BLK), 1)
    scale = DH ** (-0.5)
    block = lambda a: slice(a * BLK, (a + 1) * BLK)
    head = lambda h: slice(h * DH, (h + 1) * DH)

    @step
    def gates():
        for name in ("ig", "fg", "ex", "doc"):
            loads[name].wait()
        f = fg[...]
        lf = jnp.minimum(f, 0.0) - jnp.log1p(jnp.exp(-jnp.abs(f))) + ex[...]
        docs = doc[...].astype(F32)
        dr = [docs[:, block(a)] for a in range(NB)]
        ga = [ig[:, block(a)] for a in range(NB)]
        cum = jnp.dot(
            jnp.concatenate([lf[:, block(a)] for a in range(NB)], axis=0), (ri <= ci).astype(F32),
            precision=lax.Precision.HIGHEST, preferred_element_type=F32,
        )
        cm = [cum[2 * a:2 * a + 2] for a in range(NB)]
        tot = [jnp.broadcast_to(cm[a][:, BLK - 1:BLK], (2, BLK)) for a in range(NB)]

        def between(b, a):
            s = jnp.zeros((2, BLK), F32)
            for i in range(b, a):
                s = s + tot[i]
            return s

        got.update(
            between=between, dr=dr,
            ex=[[ga[b] - cm[b] if a == b else ga[b] + ((tot[b] - cm[b]) + between(b + 1, a))
                 for b in range(min(a + 1, NB))] for a in range(NB + 1)],
            first=jnp.broadcast_to(dr[0][:, 0:1], (1, BLK)), last=jnp.broadcast_to(dr[NB - 1][:, BLK - 1:BLK], (1, BLK)),
        )
        got["dcol"] = [across(d) for d in dr]

    @step
    def state():
        e = got["ex"][NB]
        kept = [jnp.where(got["dr"][b] == got["last"], e[b], NEG) for b in range(NB)]
        peak = jnp.maximum(jnp.maximum(kept[0], kept[1]), jnp.maximum(kept[2], kept[3]))
        peak = jnp.broadcast_to(jnp.max(peak, axis=1, keepdims=True), (2, BLK))
        wt = [jnp.exp(kept[b] - peak) for b in range(NB)]
        wrow = jnp.concatenate(wt, axis=1)
        loads["k"].wait()
        loads["v"].wait()
        for h in range(2):
            kh = k[:, head(h)]
            scaled = jnp.concatenate(
                [v[block(b), head(h)].astype(F32) * across(wt[b][h:h + 1]) for b in range(NB)], axis=0
            ).astype(BF16)
            stin[5, head(h), :] = lax.dot_general(
                kh, scaled, (((0,), (0,)), ((), ())), preferred_element_type=F32
            ).astype(BF16)
            w8 = jnp.broadcast_to(wrow[h:h + 1], (8, ROWS)).astype(BF16)
            auxin[5, 4 + h:5 + h] = jnp.dot(w8, kh, preferred_element_type=F32)[0:1]
        auxin[5, 0:2] = peak
        auxin[5, 2:4] = got["between"](0, NB)
        auxin[5, 6:7] = got["last"]
        auxin[5, 7:8] = got["last"]

    @step
    def tell():
        pass_state(5, 0, ahead)
        pass_state(5, 1, two_ahead)
        pass_state(5, 4, mate)

    def pass_state(slot, to, dev):
        send("st", "st%d" % to, stin.at[slot], stin.at[to], dev)
        send("sx", "sx%d" % to, auxin.at[slot], auxin.at[to], dev)

    @step
    def st0():
        arrived("st0", "sx0")
        pass_state(0, 2, mate)

    @step
    def st1():
        arrived("st1", "sx1")
        pass_state(1, 3, mate)

    def intra(h):
        if loads["q"] is not None:
            loads["q"].wait()
            loads["q"] = None
        vx = jnp.concatenate([v[:, head(h)], jnp.ones((ROWS, DH), BF16)], axis=1)
        for a in range(NB):
            n = (a + 1) * BLK
            sc = lax.dot_general(
                q[block(a), head(h)], k[:n, head(h)], (((1,), (1,)), ((), ())), preferred_element_type=F32
            )
            es = []
            for b in range(a + 1):
                ok = got["dcol"][a] == got["dr"][b]
                if b == a:
                    ok = ok & (ci <= ri)
                es.append(jnp.where(ok, got["ex"][a][b][h:h + 1], NEG))
            best = es[0]
            for e in es[1:]:
                best = jnp.maximum(best, e)
            best = jnp.max(best, axis=1, keepdims=True)
            p = jnp.concatenate(
                [(jnp.exp(es[b] - best) * (sc[:, block(b)] * scale)).astype(BF16) for b in range(a + 1)], axis=1
            )
            nd[h, block(a), :] = jnp.dot(p, vx[:n], preferred_element_type=F32)
            top[h, block(a), :] = jnp.broadcast_to(best, (BLK, BLK))

    steps["intra0"] = lambda: intra(0)
    steps["intra1"] = lambda: intra(1)

    ucols = lambda o: pl.ds(pl.multiple_of(xi(o) * HW, HW), HW)
    def uview(o, s, part=None):
        rows = pl.ds(256 * s, 256) if part is None else pl.ds(256 * s + 128 * part, 128)
        return u.at[rows, ucols(o)]

    fcols = lambda o: pl.ds(pl.multiple_of(xi(o) * OWN, OWN), OWN)

    def fview(o, s, part=None):
        rows = pl.ds(256 * s, 256) if part is None else pl.ds(256 * s + 128 * part, 128)
        return full.at[rows, fcols(o)]

    def spread(view, tag, s):
        send(tag, tag + "%d-" % s, view(0, s), view(0, s), xr)
        send(tag, tag + "%d+" % s, view(0, s), view(0, s), xl)

    def onward(view, tag, s, side):
        if side < 0:
            arrived(tag + "%d-" % s)
            send(tag, tag + "%dr" % s, view(-1, s, 0), view(-1, s, 0), xr)
        else:
            arrived(tag + "%d+" % s)
            send(tag, tag + "%dl" % s, view(1, s, 1), view(1, s, 1), xl)

    for s in (0, 1):
        steps["ur%d" % s] = lambda s=s: onward(uview, "u", s, -1)
        steps["ul%d" % s] = lambda s=s: onward(uview, "u", s, 1)
        steps["fr%d" % s] = lambda s=s: onward(fview, "f", s, -1)
        steps["fl%d" % s] = lambda s=s: onward(fview, "f", s, 1)

    @step
    def comb():
        arrived("st2", "sx2", "st3", "sx3", "st4", "sx4")
        gone = jnp.zeros((2, BLK), F32)
        logs, slots = [], (2 + 2 * c, 0, 3 - c, 1)
        for j, s in enumerate(slots):
            live = (auxin[s, 6:7] == got["first"]) & (sp > j)
            logs.append(jnp.where(live, auxin[s, 0:2] + gone, NEG))
            gone = gone + auxin[s, 2:4]
        came = jnp.maximum(jnp.maximum(logs[0], logs[1]), jnp.maximum(logs[2], logs[3]))
        part = [jnp.where(lg > 0.5 * NEG, jnp.exp(lg - came), 0.0) for lg in logs]
        memx = []
        for h in range(2):
            m, n = jnp.zeros((DH, DH), F32), jnp.zeros((1, BLK), F32)
            for g, s in zip(part, slots):
                m = m + g[h:h + 1] * stin[s, head(h), :].astype(F32)
                n = n + g[h:h + 1] * auxin[s, 4 + h:5 + h]
            memx.append(jnp.concatenate([m, across(n)], axis=1).astype(BF16))
        loads["og"].wait()
        loads["cg"].wait()
        got.update(memx=memx, came=came, gain=cg[...].astype(F32).reshape(1, HW))

    def cell(s):
        memx, came, gain = got["memx"], got["came"], got["gain"]
        for a in (2 * s, 2 * s + 1):
            squares = jnp.zeros((BLK, DH), F32)
            outs = []
            for h in range(2):
                qm = jnp.dot(q[block(a), head(h)], memx[h], preferred_element_type=F32) * scale
                far = jnp.where(got["dcol"][a] == got["first"], (got["between"](0, a) + came)[h:h + 1], NEG)
                near = top[h, block(a), :]
                m = jnp.maximum(near, far)
                wn, wf = jnp.exp(near - m), jnp.exp(far - m)
                num = wn * nd[h, block(a), :DH] + wf * qm[:, :DH]
                den = wn * nd[h, block(a), DH:] + wf * qm[:, DH:]
                val = num / jnp.maximum(jnp.abs(den), 1.0)
                squares = squares + val * val
                gate = jax.nn.sigmoid(og[block(a), head(h)].astype(F32))
                outs.append((gate * val * gain[:, head(h)]).astype(BF16))
            u[block(a), ucols(0)] = jnp.concatenate(outs, axis=1)
            line1[:, block(a)] = rows_of(squares)
        cols = slice(256 * s, 256 * s + 256)
        spread(uview, "u", s)
        for r in range(1, NX):
            send("l", "l%d,%d" % (s, r), line1.at[:, cols], line1in.at[r - 1, :, cols], {"x": xi(r)}, "l%d" % s)

    steps["cell0"] = lambda: cell(0)
    steps["cell1"] = lambda: cell(1)

    def head_out(s):
        cols = slice(256 * s, 256 * s + 256)
        all_arrived("l%d" % s, line1in.at[:, :, cols])
        total = line1[:, cols] + line1in[0, :, cols] + line1in[1, :, cols] + line1in[2, :, cols]
        inv = lax.rsqrt(total / (DH * 8) + EPS)
        if s == 0:
            loads["w"].wait()
            loads["res"].wait()
            all_arrived("wm", wc.at[0:384])
        arrived("u%dr" % s, "u%dl" % s)
        for a in (2 * s, 2 * s + 1):
            ic = across(inv[0:1, block(a - 2 * s)])
            acc = jnp.dot(u[block(a), :], wc[...], preferred_element_type=F32)
            squares = jnp.zeros((BLK, BLK), F32)
            outs = []
            for b in range(OWN // BLK):
                f = (res[block(a), block(b)].astype(F32) + acc[:, block(b)] * ic).astype(BF16)
                fw = f.astype(F32)
                squares = squares + fw * fw
                outs.append(f)
            full[block(a), fcols(0)] = jnp.concatenate(outs, axis=1)
            line2[:, block(a)] = rows_of(squares)

        spread(fview, "f", s)
        for r in range(1, NX):
            send("m", "m%d,%d" % (s, r), line2.at[:, cols], line2in.at[r - 1, :, cols], {"x": xi(r)}, "m%d" % s)

    steps["out0"] = lambda: head_out(0)
    steps["out1"] = lambda: head_out(1)

    def norm(s):
        cols = slice(256 * s, 256 * s + 256)
        all_arrived("m%d" % s, line2in.at[:, :, cols])
        total = line2[:, cols] + line2in[0, :, cols] + line2in[1, :, cols] + line2in[2, :, cols]
        inv = lax.rsqrt(total / DM + EPS)
        if s == 0:
            all_arrived("g", gains.at[0:3])
        arrived("f%dr" % s, "f%dl" % s)
        for a in (2 * s, 2 * s + 1):
            ic = across(inv[0:1, block(a - 2 * s)])
            for r in range(NX):
                fw = full[block(a), fcols(-r)].astype(F32)
                gain = gains[0, 0:1] if r == 0 else gains[r, 0:1]
                normed[block(a), fcols(-r)] = jnp.concatenate(
                    [(fw[:, block(b)] * ic * gain[:, block(b)]).astype(BF16) for b in range(OWN // BLK)], axis=1
                )

    steps["norm0"] = lambda: norm(0)
    steps["norm1"] = lambda: norm(1)

    def up(s, t):
        if s == t == 0:
            all_arrived("U", wup.at[0:4])
        rows, cols = slice(256 * s, 256 * s + 256), slice(t * 512, (t + 1) * 512)
        hid = jnp.dot(normed[rows, :], wup[:, :, :, :, cols].reshape(DM, 512), preferred_element_type=F32)
        hid = jnp.maximum(hid, 0.0)
        squared[rows, cols] = (hid * hid).astype(BF16)

    for t in range(4):
        steps["up0,%d" % t] = lambda t=t: up(0, t)
        steps["up1,%d" % t] = lambda t=t: up(1, t)

    zb = lax.rem(z, 2)
    owner = [lax.rem(z // 2 + d + NX, NX) for d in (0, 2, 2 * zb - 1, 1 - 2 * zb)]
    ahead_by = [lax.rem(o - x + NX, NX) for o in owner]
    ways = ((0, xr), (1, xl), (1, xr), (0, xl), (0, xr), (1, xl))
    quarter = lambda s, h: slice(256 * s + 128 * h, 256 * s + 128 * h + 128)

    def part(s, i, k):
        h, dev = ways[i]
        return pltpu.make_async_remote_copy(
            src_ref=terms.at[k, quarter(s, h)], dst_ref=parts.at[s, i], send_sem=ssem.at[groups.index("p")],
            recv_sem=prs.at[6 * s + i], device_id=dev, device_id_type=MESH,
        )

    def stage(s, k):
        if s == 0:
            if k < 3:
                all_arrived("D%d" % k, (wdn.at[0:3, :, 0], wdn.at[0:3, :, 0], wdn.at[0])[k])
        w = wdn[pl.ds(2 * owner[k], 2)].reshape(OWN, DM)
        rows = slice(256 * s, 256 * s + 256)
        terms[k, rows] = lax.dot_general(
            squared[rows, :], w, (((1,), (1,)), ((), ())), preferred_element_type=F32
        ).astype(BF16)

        @pl.when(ahead_by[k] == 2)
        def _():
            part(s, 0, k).start()
            part(s, 1, k).start()

        @pl.when(ahead_by[k] == 1)
        def _():
            part(s, 2, k).start()

        @pl.when(ahead_by[k] == 3)
        def _():
            part(s, 3, k).start()

    def join(s, k):
        for side, h, i in ((1, 0, 0), (3, 1, 1)):
            @pl.when(ahead_by[k] == side)
            def _():
                part(s, i, 0).wait_recv()
                rows = quarter(s, h)
                terms[k, rows] = (terms[k, rows].astype(F32) + parts[s, i].astype(F32)).astype(BF16)
                part(s, i + 4, k).start()

    @step
    def sent():
        for group in groups:
            if group != "p":
                all_sent(group)

    def final(s):
        d = lax.rem(x - z // 2 + NX, NX)
        d = lax.rem(d * (2 * zb - 1) + NX, NX)
        mine = terms.at[2 * lax.rem(d, 2) + d // 2]
        for h, i, n in ((0, 3, 4), (1, 2, 5)):
            part(s, i, 0).wait_recv()
            part(s, n, 0).wait_recv()
            rows = quarter(s, h)
            out[rows] = (
                full[rows, fcols(0)].astype(F32) + mine[rows].astype(F32)
                + parts[s, i].astype(F32) + parts[s, n].astype(F32)
            ).astype(BF16)
        half = slice(256 * s, 256 * s + 256)
        d = pltpu.make_async_copy(out.at[half], out_h.at[half], osem.at[s])
        d.start()
        kept.append(d)

    kept = []

    @step
    def rest():
        for d in kept:
            d.wait()
        all_sent("p")

    for s in (0, 1):
        for n in range(4):
            steps["s%d,%d" % (s, n)] = lambda s=s, n=n: stage(s, n)
            steps["j%d,%d" % (s, n)] = lambda s=s, n=n: join(s, n)
        steps["fin%d" % s] = lambda s=s: final(s)

    steps["gates"]()
    steps["state"]()
    pl.semaphore_wait(barrier, len(peers))
    for name in ORDER:
        steps[name]()


def layer(*arrays):
    dma = pltpu.SemaphoreType.DMA
    return pl.pallas_call(
        kernel,
        out_shape=jax.ShapeDtypeStruct((ROWS, OWN), BF16),
        in_specs=[pl.BlockSpec(memory_space=pltpu.HBM)] * len(arrays),
        out_specs=pl.BlockSpec(memory_space=pltpu.HBM),
        scratch_shapes=[
            *[pltpu.VMEM(a.shape, a.dtype) for a in arrays[:11]],
            pltpu.VMEM((4 * HW, OWN), BF16),
            pltpu.VMEM((2, ROWS, 2 * DH), F32),
            pltpu.VMEM((2, ROWS, DH), F32),
            pltpu.VMEM((6, 2 * DH, DH), BF16),
            pltpu.VMEM((6, 8, BLK), F32),
            pltpu.VMEM((ROWS, 4 * HW), BF16),
            pltpu.VMEM((8, ROWS), F32),
            pltpu.VMEM((3, 8, ROWS), F32),
            pltpu.VMEM((ROWS, DM), BF16),
            pltpu.VMEM((8, ROWS), F32),
            pltpu.VMEM((3, 8, ROWS), F32),
            pltpu.VMEM((4, 8, OWN), F32),
            pltpu.VMEM((ROWS, DM), BF16),
            pltpu.VMEM((NZ, NY, NC, 32, DM), BF16),
            pltpu.VMEM((NZ, NY, NC, 32, DM), BF16),
            pltpu.VMEM((ROWS, DM), BF16),
            pltpu.VMEM((4, ROWS, OWN), BF16),
            pltpu.VMEM((2, 6, ROWS // 4, OWN), BF16),
            pltpu.VMEM((ROWS, OWN), BF16),
            dma((len(LOADS),)), dma((14,)), dma((RECEIVES,)), dma((12,)), dma((2,)),
        ],
        compiler_params=pltpu.CompilerParams(
            collective_id=0, has_side_effects=True, vmem_limit_bytes=62 * 2**20
        ),
    )(*arrays)


def local(
    queries, keys, values, output_gate_logits, input_gate_log, forget_gate_logits, extra_decay_log,
    document, residual, cell_norm_gain, output_weight, mixer_norm_gain, up_weight, down_weight,
):
    return layer(
        input_gate_log.T, forget_gate_logits.T, extra_decay_log.T, document.reshape(1, ROWS),
        cell_norm_gain, mixer_norm_gain,
        queries, keys, values, output_gate_logits, residual, output_weight, up_weight, down_weight.T,
    )


def solution(mesh):
    split = Mesh(mesh.devices.reshape(NZ, NY, NC, NX), ("z", "y", "c", "x"))
    rows, heads = P(SP, "x"), P("x")
    return jax.shard_map(
        local,
        mesh=split,
        in_specs=(
            rows, rows, rows, rows, rows, rows, rows, P(SP), rows, heads, P("x", None), heads, rows, P("x", SP),
        ),
        out_specs=rows,
        check_vma=False,
    )
```
